32 devices in a mesh: grp: 2 (over y), sp: 4 (over z), tp: 4 (over x, core).
Axes of the slice: x: 2, y: 2, z: 4, core: 2. Of those that a mesh axis runs over, the one named last changes fastest.
Arguments:
- query_latent: bfloat16 [1024, 768], P(('grp', 'sp')), parts along dimension 0, may hold values from -6 to 6
- key_latent: bfloat16 [1024, 256], P(('grp', 'sp', 'tp')), parts along dimension 0, may hold values from -20 to 20
- rotary_key: bfloat16 [1024, 64], P(('grp', 'sp', 'tp')), parts along dimension 0, may hold values from -1000 to 1000
- query_gain: float32 [768], replicated, may hold values from 0.1 to 1.9
- latent_gain: float32 [256], replicated, may hold values from 0.1 to 1.9
- query_up: bfloat16 [768, 3072], P(None, 'tp'), may hold values from -0.21875 to 0.21875
- key_up: bfloat16 [256, 2048], P(None, 'tp'), may hold values from -0.375 to 0.375
- value_up: bfloat16 [256, 2048], P(None, 'tp'), may hold values from -0.375 to 0.375
- out_gain: float32 [2048], P('tp'), may hold values from 0.1 to 1.9
- out_weight: bfloat16 [2048, 4096], P('sp', 'tp'), may hold values from -0.125 to 0.125
Outputs:
- mixed: bfloat16 [1024, 4096], P(('grp', 'sp'), 'tp'), parts along dimension 0
The draws below stay inside these ranges and needn't reach their ends.
There are 2 independent parts, one for each index of `grp`. The reference program is written for one: setup_inputs(seed, part) draws one part's arguments, and reference() takes and returns one part's arrays. A program takes and returns all parts, laid end to end along the dimension named above; an argument that names none is the same for every part. Nothing has to cross between parts.
All inputs are finite; a program needn't handle non-finite values.
Results may differ from the reference program's by a relative error of at most 0.02.
The reference program's roundings to bfloat16 on the way count: a program that leaves them out, or rounds other values in their place, can miss the bound.
Values may be sent and summed in bfloat16 or wider, within the bound.
A program may use at most 128 MiB of HBM per device.

```python
import jax
import jax.numpy as jnp
from jax import lax

D_MODEL = 4096
HEADS = 16
NOPE_DIM = 128
ROPE_DIM = 64
VALUE_DIM = 128
QRANK = 768
KVRANK = 256
TOK_DEV = 128
TOKENS = 512
N_SP = 4


def draw_key_latent(key, part):
    first_key, second_key = jax.random.split(jax.random.fold_in(key, 11), 2)
    blocks = TOKENS // TOK_DEV
    offsets = jax.random.normal(second_key, (blocks, KVRANK), jnp.float32)
    noise = jax.random.normal(first_key, (TOKENS, KVRANK), jnp.float32)
    offset_rows = jnp.repeat(offsets, TOK_DEV, axis=0)
    return jnp.clip(noise + offset_rows, -20.0, 20.0).astype(jnp.bfloat16)


def draw_rotary_key(key, part):
    first_key = jax.random.fold_in(jax.random.fold_in(key, 23), 0)
    values = jax.random.normal(first_key, (TOKENS, ROPE_DIM), jnp.float32)
    return jnp.clip(values, -1000.0, 1000.0).astype(jnp.bfloat16)


def shard_levels(rng, extent, cuts, smallest, top_value):
    def one(dim, shards_of):
        heights = jax.random.uniform(jax.random.fold_in(jax.random.fold_in(rng, 6), dim), (shards_of,), jnp.float32, smallest / len(cuts), top_value / len(cuts))
        return jnp.repeat(jnp.exp(heights), extent[dim] // shards_of).reshape((-1,) + (1,) * (len(extent) - dim - 1))

    factor_of = one(*cuts[0])
    for cut in cuts[1:]:
        factor_of = factor_of * one(*cut)
    return factor_of


def scatter_about(own_key, extent, scale, reach, pieces=(), kind=jnp.bfloat16):
    result = jax.random.normal(own_key, extent, jnp.float32) * scale
    if len(pieces) > 0:
        result = shard_levels(own_key, extent, pieces, -0.22, 0.18) * result
    return jnp.clip(result, min=-reach, max=reach).astype(kind)


def setup_inputs(seed: int = 0, part: int = 0) -> dict:
    keys = jax.random.split(jax.random.key(seed), 11)
    own_keys = jax.random.split(jax.random.fold_in(keys[10], part), 11)
    return {
        "query_latent": scatter_about(own_keys[0], (TOKENS, QRANK), 1.0, 6.0, ((0, 4),)),
        "key_latent": draw_key_latent(jax.random.fold_in(jax.random.fold_in(keys[10], part), 71), part),
        "rotary_key": draw_rotary_key(jax.random.fold_in(jax.random.fold_in(keys[10], part), 71), part),
        "query_gain": jnp.clip(1.0 + 0.18 * jax.random.normal(keys[3], (QRANK,), jnp.float32), 0.1, 1.9),
        "latent_gain": jnp.clip(1.0 + 0.18 * jax.random.normal(keys[4], (KVRANK,), jnp.float32), 0.1, 1.9),
        "query_up": scatter_about(keys[5], (QRANK, HEADS * (NOPE_DIM + ROPE_DIM)), QRANK ** -0.5, 0.21875, ((1, 4),)),
        "key_up": scatter_about(keys[6], (KVRANK, HEADS * NOPE_DIM), KVRANK ** -0.5, 0.375, ((1, 4),)),
        "value_up": scatter_about(keys[7], (KVRANK, HEADS * VALUE_DIM), KVRANK ** -0.5, 0.375, ((1, 4),)),
        "out_gain": jnp.clip(1.0 + 0.18 * jax.random.normal(keys[8], (HEADS * VALUE_DIM,), jnp.float32), 0.1, 1.9),
        "out_weight": scatter_about(keys[9], (HEADS * VALUE_DIM, D_MODEL), (HEADS * VALUE_DIM) ** -0.5, 0.125, ((0, 4), (1, 4))),
    }


norm_eps = 1e-06
rope_theta = 10000.0

def rms_scaled(inputs, gain_vec):
    widened = inputs.astype(jnp.float32)
    return widened * lax.rsqrt(lax.optimization_barrier(jnp.mean(widened * widened, axis=-1, keepdims=True)) + norm_eps) * gain_vec

def rotate_half(inputs, positions):
    half_width = inputs.shape[-1] // 2
    inverse = rope_theta ** (-jnp.arange(half_width, dtype=jnp.float32) / half_width)
    angles = positions[:, None] * inverse[None, :]
    if inputs.ndim == 3:
        angles = angles[:, None, :]
    cosine = jnp.cos(angles)
    sine = jnp.sin(angles)
    widened = inputs.astype(jnp.float32)
    first = widened[..., :half_width]
    second = widened[..., half_width:]
    return jnp.concatenate([first * cosine - second * sine, second * cosine + first * sine], axis=-1)

def reference(query_latent, key_latent, rotary_key, query_gain, latent_gain, query_up, key_up, value_up, out_gain, out_weight):
    positions = jnp.arange(TOKENS, dtype=jnp.float32)
    score_scale = (NOPE_DIM + ROPE_DIM) ** (-0.5)
    query_normed = rms_scaled(query_latent, query_gain).astype(jnp.bfloat16)
    query_full = jnp.dot(query_normed, query_up, preferred_element_type=jnp.float32).astype(jnp.bfloat16)
    query_full = query_full.reshape(TOKENS, HEADS, NOPE_DIM + ROPE_DIM)
    query_plain = query_full[..., :NOPE_DIM]
    query_turned = rotate_half(query_full[..., NOPE_DIM:], positions).astype(jnp.bfloat16)
    latent_normed = rms_scaled(key_latent, latent_gain).astype(jnp.bfloat16)
    key_turned = rotate_half(rotary_key, positions).astype(jnp.bfloat16)
    key_plain = jnp.dot(latent_normed, key_up, preferred_element_type=jnp.float32).astype(jnp.bfloat16)
    key_wide = key_plain.reshape(TOKENS, HEADS, NOPE_DIM).astype(jnp.float32)
    turned_wide = key_turned.astype(jnp.float32)
    latent_wide = latent_normed.astype(jnp.float32)
    value_heads = value_up.astype(jnp.float32).reshape(KVRANK, HEADS, VALUE_DIM)

    def one_block(block_index):
        begin = (block_index * TOK_DEV).astype(jnp.int32)
        plain = lax.dynamic_slice_in_dim(query_plain, begin, TOK_DEV, 0).astype(jnp.float32)
        turned = lax.dynamic_slice_in_dim(query_turned, begin, TOK_DEV, 0).astype(jnp.float32)
        scores = jnp.einsum('qhd,khd->qhk', plain, key_wide) + jnp.einsum('qhd,kd->qhk', turned, turned_wide)
        scores = scores * score_scale
        row_top = lax.optimization_barrier(jnp.max(scores, axis=-1, keepdims=True))
        expo = jnp.exp(scores - row_top)
        total = lax.optimization_barrier(jnp.sum(expo, axis=-1))
        weights = lax.optimization_barrier(expo.astype(jnp.bfloat16)).astype(jnp.float32)
        latent_mix = jnp.einsum('qhk,kc->qhc', weights, latent_wide) / total[..., None]
        latent_mix = lax.optimization_barrier(latent_mix.astype(jnp.bfloat16)).astype(jnp.float32)
        head_out = jnp.einsum('qhc,chd->qhd', latent_mix, value_heads).astype(jnp.bfloat16)
        return head_out.reshape(TOK_DEV, HEADS * VALUE_DIM)
    head_out = lax.map(one_block, jnp.arange(N_SP, dtype=jnp.int32)).reshape(TOKENS, HEADS * VALUE_DIM)
    widened = head_out.astype(jnp.float32)
    mean_square = lax.optimization_barrier(jnp.mean(widened * widened, axis=1))
    gained = (widened * out_gain).astype(jnp.bfloat16)
    projected = jnp.dot(gained, out_weight, preferred_element_type=jnp.float32)
    return (projected * lax.rsqrt(mean_square + norm_eps)[:, None]).astype(jnp.bfloat16)
```

```python
import functools

import jax
import jax.numpy as jnp
import numpy as np
from jax import lax
from jax.experimental import pallas as pl
from jax.experimental.pallas import tpu as pltpu
from jax.sharding import PartitionSpec as P

HEADS = 16
NOPE_DIM = 128
ROPE_DIM = 64
VALUE_DIM = 128
KVRANK = 256


norm_eps = 1e-06
rope_theta = 10000.0


def rms_scaled(inputs, gain_vec):
    widened = inputs.astype(jnp.float32)
    return (
        widened
        * lax.rsqrt(jnp.mean(widened * widened, axis=-1, keepdims=True) + norm_eps)
        * gain_vec
    )


def rotate_half(inputs, positions):
    half_width = inputs.shape[-1] // 2
    inverse = rope_theta ** (-jnp.arange(half_width, dtype=jnp.float32) / half_width)
    angles = positions[:, None] * inverse[None, :]
    if inputs.ndim == 3:
        angles = angles[:, None, :]
    cosine = jnp.cos(angles)
    sine = jnp.sin(angles)
    widened = inputs.astype(jnp.float32)
    first = widened[..., :half_width]
    second = widened[..., half_width:]
    return jnp.concatenate(
        [first * cosine - second * sine, second * cosine + first * sine], axis=-1
    )


def on_device(
    query_latent,
    key_latent,
    rotary_key,
    query_gain,
    latent_gain,
    query_up,
    key_up,
    value_up,
    out_gain,
    out_weight,
):
    block_rows = query_latent.shape[0]
    row_count = key_latent.shape[0]
    head_local = key_up.shape[1] // NOPE_DIM
    block_start = lax.axis_index("sp") * block_rows
    own_start = block_start + lax.axis_index("tp") * row_count
    score_scale = (NOPE_DIM + ROPE_DIM) ** (-0.5)
    normed = rms_scaled(query_latent, query_gain).astype(jnp.bfloat16)
    query_full = jnp.dot(normed, query_up, preferred_element_type=jnp.float32).astype(jnp.bfloat16)
    query_full = query_full.reshape(block_rows, head_local, NOPE_DIM + ROPE_DIM)
    query_positions = (block_start + jnp.arange(block_rows, dtype=jnp.int32)).astype(jnp.float32)
    query_plain = query_full[..., :NOPE_DIM]
    query_turned = rotate_half(query_full[..., NOPE_DIM:], query_positions).astype(jnp.bfloat16)
    latent_normed = rms_scaled(key_latent, latent_gain).astype(jnp.bfloat16)
    own_positions = (own_start + jnp.arange(row_count, dtype=jnp.int32)).astype(jnp.float32)
    key_turned = rotate_half(rotary_key, own_positions).astype(jnp.bfloat16)
    running_max = jnp.full((block_rows, head_local), -1e30, jnp.float32)
    running_sum = jnp.zeros((block_rows, head_local), jnp.float32)
    weighted = jnp.zeros((block_rows, head_local, KVRANK), jnp.float32)
    latents = lax.all_gather(latent_normed, ("sp", "tp"), axis=0, tiled=True)
    turned_keys = lax.all_gather(key_turned, ("sp", "tp"), axis=0, tiled=True)
    portion_rows = latents.shape[0]
    step_rows = min(portion_rows, 2048)
    for begin in range(0, portion_rows, step_rows):
        latent_part = latents[begin : begin + step_rows]
        turned_part = turned_keys[begin : begin + step_rows]
        key_plain = jnp.dot(latent_part, key_up, preferred_element_type=jnp.float32).astype(
            jnp.bfloat16
        )
        key_plain = key_plain.reshape(latent_part.shape[0], head_local, NOPE_DIM)
        scores = jnp.einsum(
            "qhd,khd->qhk", query_plain, key_plain, preferred_element_type=jnp.float32
        )
        scores = scores + jnp.einsum(
            "qhd,kd->qhk", query_turned, turned_part, preferred_element_type=jnp.float32
        )
        scores = scores * score_scale
        new_max = jnp.maximum(running_max, jnp.max(scores, axis=-1))
        rescale = jnp.exp(running_max - new_max)
        expo = jnp.exp(scores - new_max[..., None])
        running_sum = running_sum * rescale + jnp.sum(expo, axis=-1)
        weighted = weighted * rescale[..., None] + jnp.einsum(
            "qhk,kc->qhc",
            expo.astype(jnp.bfloat16),
            latent_part,
            preferred_element_type=jnp.float32,
        )
        running_max = new_max
    final_state = (running_max, running_sum, weighted)
    running_max, running_sum, weighted = final_state
    latent_mix = (weighted / running_sum[..., None]).astype(jnp.bfloat16)
    value_heads = value_up.reshape(KVRANK, head_local, VALUE_DIM)
    head_out = jnp.einsum(
        "qhc,chd->qhd", latent_mix, value_heads, preferred_element_type=jnp.float32
    ).astype(jnp.bfloat16)
    head_out = head_out.reshape(block_rows, head_local * VALUE_DIM)
    widened = head_out.astype(jnp.float32)
    square_part = jnp.sum(widened * widened, axis=1)
    gained = (widened * out_gain).astype(jnp.bfloat16)
    all_gained, square_parts = (
        lax.all_gather(gained, "tp", axis=1, tiled=True),
        lax.all_gather(square_part[:, None].astype(jnp.bfloat16), "tp", axis=1, tiled=True).astype(
            jnp.float32
        ),
    )
    all_squares = jnp.sum(square_parts, axis=1)
    own_sums = jnp.dot(
        all_gained,
        lax.all_gather(out_weight, "sp", axis=0, tiled=True),
        preferred_element_type=jnp.float32,
    )
    mean_square = all_squares / (HEADS * VALUE_DIM)
    return (own_sums * lax.rsqrt(mean_square + norm_eps)[:, None]).astype(jnp.bfloat16)


LANES = 128
LINE = 4
TILES = 4
SPLIT = 2
CHUNKS = TILES * SPLIT


def rope_table(tokens, width):
    half = width // 2
    inverse = np.float32(rope_theta) ** (-np.arange(half, dtype=np.float32) / np.float32(half))
    angles = np.arange(tokens, dtype=np.float32)[:, None] * inverse.astype(np.float32)[None, :]
    wide = angles.astype(np.float32).astype(np.float64)
    cosine, sine = np.cos(wide), np.sin(wide)
    return np.concatenate([cosine, cosine, -sine, sine], axis=1).astype(np.float32)


def turned(wide, table):
    width = wide.shape[-1]
    half = width // 2
    swapped = jnp.concatenate([wide[:, half:], wide[:, :half]], axis=1)
    return wide * table[:, :width] + swapped * table[:, width:]


def kernel(
    n_sp, n_tp,
    ql_hbm, kl, rk, qg_hbm, lg_hbm, og_hbm, table_hbm, qup, kup, vup, ow, out_hbm,
    ql, qg, lg, og, table,
    lat, wbuf, qbuf, kbuf, vbuf, latn, kturn, qfull, qnorm, gall, squares, acc, far_acc,
    asked, far_out, far_in, out,
    local, w_local, o_local, l_send, l_recv, g_send, g_recv,
    w_send, w_recv, q_send, q_recv, f_send, f_recv,
):
    z, t, g = lax.axis_index("sp"), lax.axis_index("tp"), lax.axis_index("grp")
    parity = lax.rem(g, 2)
    partner = g + 1 - 2 * parity
    core = lax.rem(t, 2)
    sibling = t + 1 - 2 * core
    block_rows = ql.shape[0]
    depth = ow.shape[0]
    half = depth // 2
    piece = half // SPLIT
    tile = wbuf.shape[3]
    heads = kup.shape[1] // NOPE_DIM
    cols = heads * VALUE_DIM
    head_width = NOPE_DIM + ROPE_DIM
    rank = kl.shape[1]
    width = rk.shape[1]
    keys = n_sp * n_tp * kl.shape[0]

    lower = z < n_sp // 2
    toward = jnp.where(lower, 1, -1)
    centre = z + toward
    outer = z - toward
    beyond = centre + toward
    has_up, has_down = z < n_sp - 1, z > 0
    edge = jnp.logical_or(z == 0, z == n_sp - 1)
    inner = jnp.logical_not(edge)
    far_base = jnp.where(lower, n_tp // 2, 0)

    loads = [
        pltpu.make_async_copy(src, dst, local.at[i])
        for i, (src, dst) in enumerate((
            (kl, lat.at[z, t, :, pl.ds(0, rank)]),
            (rk, lat.at[z, t, :, pl.ds(rank, width)]),
            (ql_hbm, ql),
            (qg_hbm, qg),
            (qup, qbuf),
            (lg_hbm, lg),
            (table_hbm, table),
            (kup, kbuf),
            (vup, vbuf),
            (og_hbm, og),
        ))
    ]
    w_loads = [
        pltpu.make_async_copy(ow.at[:, pl.ds(f * tile, tile)], wbuf.at[z, f], w_local.at[f])
        for f in range(TILES)
    ]
    for load in loads[:2] + w_loads[:1] + loads[2:5] + w_loads[1:] + loads[5:]:
        load.start()

    barrier = pltpu.get_barrier_semaphore()

    @pl.when(has_up)
    def _():
        pl.semaphore_signal(barrier, inc=1, device_id={"sp": z + 1}, device_id_type=MESH)

    @pl.when(has_down)
    def _():
        pl.semaphore_signal(barrier, inc=1, device_id={"sp": z - 1}, device_id_type=MESH)

    pl.semaphore_signal(barrier, inc=1, device_id={"grp": partner}, device_id_type=MESH)
    for d in range(1, n_tp):
        pl.semaphore_signal(barrier, inc=1, device_id={"tp": lax.rem(t + d, n_tp)}, device_id_type=MESH)
    pl.semaphore_wait(barrier, n_tp + jnp.where(edge, 1, 2))

    def remote(src, dst, send, recv, target):
        return pltpu.make_async_remote_copy(
            src_ref=src, dst_ref=dst, send_sem=send, recv_sem=recv,
            device_id=target, device_id_type=MESH,
        )

    def part_along(b, up):
        return remote(
            lat.at[b, t], lat.at[b, t], l_send.at[b, up], l_recv.at[b, t], {"sp": z + 1 if up else z - 1}
        )

    def part_across(b, d):
        return remote(
            lat.at[b, t], lat.at[b, t], l_send.at[b, 1 + d], l_recv.at[b, t], {"tp": lax.rem(t + d, n_tp)}
        )

    def spread(b):
        for d in range(1, n_tp):
            part_across(b, d).start()

    def arrive(d):
        @pl.when(z >= d)
        def _():
            part_along(z - d, 1).wait_recv()

            @pl.when(has_up)
            def _():
                part_along(z - d, 1).start()

            spread(z - d)

        @pl.when(z + d < n_sp)
        def _():
            part_along(z + d, 0).wait_recv()

            @pl.when(has_down)
            def _():
                part_along(z + d, 0).start()

            spread(z + d)

    def rows_of(b, p, i):
        start = pl.multiple_of(p * half + (i % SPLIT) * piece, piece)
        return wbuf.at[b, i // SPLIT, pl.ds(start, piece)]

    def moved(kind, b, p, i, target):
        return remote(rows_of(b, p, i), rows_of(b, p, i), w_send.at[kind, i], w_recv.at[b, p, i], target)

    def inward(i):
        return moved(0, z, parity, i, {"sp": centre})

    def outward(i):
        return moved(1, z, parity, i, {"sp": outer})

    def passed(i):
        return moved(2, outer, parity, i, {"sp": centre})

    def inward_far(i):
        return moved(3, z, 1 - parity, i, {"sp": centre})

    def across(b, i):
        return moved(4, b, parity, i, {"grp": partner})

    def across_beyond(i):
        return moved(5, beyond, parity, i, {"grp": partner})

    def landed(b, p, i):
        moved(0, b, p, i, {"sp": centre}).wait_recv()

    def near(i):
        if i % SPLIT == 0:
            w_loads[i // SPLIT].wait()
        inward(i).start()

        @pl.when(inner)
        def _():
            outward(i).start()

    def near_far(i):
        @pl.when(edge)
        def _():
            inward_far(i).start()

    def first_hop(i):
        @pl.when(inner)
        def _():
            landed(outer, parity, i)
            passed(i).start()

        landed(centre, parity, i)
        across(centre, i).start()

    def second_hop(i):
        landed(beyond, parity, i)
        across_beyond(i).start()

    def queries():
        for load in loads[2:5]:
            load.wait()
        wide = ql[...].astype(jnp.float32)
        mean = jnp.mean(wide * wide, axis=-1, keepdims=True)
        gain = jnp.concatenate([qg[i : i + 1] for i in range(qg.shape[0])], axis=1)
        qnorm[...] = (wide * lax.rsqrt(mean + norm_eps) * gain).astype(jnp.bfloat16)
        qfull[...] = jnp.dot(qnorm[...], qbuf[...], preferred_element_type=jnp.float32).astype(
            jnp.bfloat16
        )

    def latents():
        for load in loads[5:]:
            load.wait()
        for b in range(n_sp):
            for d in range(1, n_tp):
                p = lax.rem(t + d, n_tp)
                remote(lat.at[b, p], lat.at[b, p], l_send.at[b, 1 + d], l_recv.at[b, p], {"tp": p}).wait_recv()
        whole = lat[...].reshape(keys, rank + width)
        wide = whole[:, :rank].astype(jnp.float32)
        mean = jnp.mean(wide * wide, axis=-1, keepdims=True)
        latn[...] = (wide * lax.rsqrt(mean + norm_eps) * lg[...]).astype(jnp.bfloat16)
        spun = whole[:, rank:].astype(jnp.float32)
        kturn[...] = turned(spun, table[...]).astype(jnp.bfloat16)

    transposed = (((1,), (1,)), ((), ()))

    def attend(h):
        start = h * head_width
        plain = qfull[:, start : start + NOPE_DIM]
        spun = qfull[:, start + NOPE_DIM : start + head_width].astype(jnp.float32)
        own = table[pl.ds(pl.multiple_of(z * block_rows, block_rows), block_rows), :]
        spun = turned(spun, own).astype(jnp.bfloat16)
        key_plain = jnp.dot(
            latn[...], kbuf[:, h * NOPE_DIM : (h + 1) * NOPE_DIM], preferred_element_type=jnp.float32
        ).astype(jnp.bfloat16)
        scores = lax.dot_general(plain, key_plain, transposed, preferred_element_type=jnp.float32)
        scores = scores + lax.dot_general(
            spun, kturn[...], transposed, preferred_element_type=jnp.float32
        )
        scores = scores * (head_width ** (-0.5))
        expo = jnp.exp(scores - jnp.max(scores, axis=-1, keepdims=True))
        total = jnp.sum(expo, axis=-1, keepdims=True)
        mix = jnp.dot(expo.astype(jnp.bfloat16), latn[...], preferred_element_type=jnp.float32)
        mix = (mix / total).astype(jnp.bfloat16)
        head_out = jnp.dot(
            mix, vbuf[:, h * VALUE_DIM : (h + 1) * VALUE_DIM], preferred_element_type=jnp.float32
        ).astype(jnp.bfloat16)
        wide = head_out.astype(jnp.float32)
        gained = wide * og[:, h * VALUE_DIM : (h + 1) * VALUE_DIM]
        gall[t, :, h * VALUE_DIM : (h + 1) * VALUE_DIM] = gained.astype(jnp.bfloat16)
        square = jnp.sum(wide * wide, axis=-1, keepdims=True)
        if h:
            square = square + squares[:, :1]
        squares[...] = jnp.broadcast_to(square, squares.shape)
        if h == heads - 1:
            gall[t, :, cols:] = squares[...].astype(jnp.bfloat16)

    def head_part(h):
        span = VALUE_DIM if h < heads - 1 else 2 * VALUE_DIM
        return gall.at[t, :, pl.ds(h * VALUE_DIM, span)]

    shares = [
        [
            remote(head_part(h), head_part(h), g_send.at[h, d], g_recv.at[h, d], {"tp": lax.rem(t + d, n_tp)})
            for d in range(1, n_tp)
        ]
        for h in range(heads)
    ]

    def share(h):
        for copy in shares[h]:
            copy.start()

    def gather(h):
        for copy in shares[h]:
            copy.wait_recv()

    ask_width = cols // 2

    def question(a):
        return pl.ds(a * ask_width, ask_width)

    def ask(a):
        return remote(
            gall.at[far_base + core, :, question(a)], asked.at[core, :, question(a)],
            q_send.at[0, a], q_recv.at[core, a], {"sp": centre},
        )

    def hand(a):
        return remote(
            asked.at[core, :, question(a)], asked.at[core, :, question(a)],
            q_send.at[1, a], q_recv.at[core, a], {"tp": sibling},
        )

    def heard(c, a):
        remote(
            asked.at[c, :, question(a)], asked.at[c, :, question(a)],
            q_send.at[1, a], q_recv.at[c, a], {"tp": sibling},
        ).wait_recv()

    def hand_on(a):
        heard(core, a)
        hand(a).start()

    def answer(f):
        return remote(far_out.at[f], far_in.at[f], f_send.at[f], f_recv.at[f], {"sp": outer})

    def part_of(p):
        return pl.ds(pl.multiple_of(p * half, half), half)

    def whole_dot(lhs, b, f):
        return jnp.dot(lhs, wbuf[b, f], preferred_element_type=jnp.float32)

    def gained_half(b, p, f):
        return jnp.dot(gall[b, :, part_of(p)], wbuf[b, f, part_of(p)], preferred_element_type=jnp.float32)

    def asked_half(b, p, f):
        return jnp.dot(
            asked[b - far_base, :, part_of(p)], wbuf[b, f, part_of(p)], preferred_element_type=jnp.float32
        )

    def stored(f):
        return pltpu.make_async_copy(out.at[f], out_hbm.at[:, pl.ds(f * tile, tile)], o_local.at[f])

    def put(f, total):
        square = gall[0, :, cols : cols + 1].astype(jnp.float32)
        for p in range(1, n_tp):
            square = square + gall[p, :, cols : cols + 1].astype(jnp.float32)
        scale = lax.rsqrt(square / (n_tp * cols) + norm_eps)
        out[f] = (total * scale).astype(out.dtype)
        stored(f).start()

    loads[0].wait()
    loads[1].wait()

    @pl.when(has_up)
    def _():
        part_along(z, 1).start()

    @pl.when(has_down)
    def _():
        part_along(z, 0).start()

    spread(z)
    near(0)
    near(1)
    queries()
    arrive(1)
    near(2)
    near(3)
    arrive(2)
    for i in range(4, CHUNKS):
        near(i)
    first_hop(0)
    first_hop(1)
    arrive(3)
    first_hop(2)
    latents()
    first_hop(3)
    attend(0)
    first_hop(4)
    near_far(0)
    attend(1)
    share(0)
    first_hop(5)
    first_hop(6)
    near_far(1)
    attend(2)
    share(1)
    first_hop(7)
    near_far(2)
    attend(3)
    share(2)

    @pl.when(inner)
    def _():
        second_hop(0)
        second_hop(1)

    share(3)
    gather(0)
    gather(1)

    @pl.when(edge)
    def _():
        ask(0).start()
        gather(2)
        gather(3)
        ask(1).start()
        for i in range(3, CHUNKS):
            inward_far(i).start()
        for f in range(TILES):
            acc[f] = whole_dot(gall[z, :, :cols], z, f)
        for f in range(TILES):
            for i in range(f * SPLIT, (f + 1) * SPLIT):
                landed(centre, 1 - parity, i)
            acc[f] += whole_dot(gall[centre, :, :cols], centre, f)
        for f in range(TILES):
            answer(f).wait_recv()
            put(f, acc[f] + far_in[f].astype(jnp.float32))

    @pl.when(inner)
    def _():
        second_hop(2)
        gather(2)
        gather(3)
        second_hop(3)
        hand_on(0)
        for f in range(TILES):
            acc[f] = whole_dot(gall[z, :, :cols], z, f)
        second_hop(4)
        for f in range(TILES):
            acc[f] += gained_half(outer, parity, f)
        second_hop(5)
        for i in range(CHUNKS):
            landed(centre, 1 - parity, i)
        for f in range(TILES):
            acc[f] += whole_dot(gall[centre, :, :cols], centre, f)
        hand_on(1)
        second_hop(6)
        for a in range(2):
            heard(1 - core, a)
        for f in range(TILES):
            far_acc[f] = whole_dot(asked[centre - far_base], centre, f)
        second_hop(7)
        for f in range(TILES):
            acc[f] += gained_half(beyond, parity, f)
            far_acc[f] += asked_half(beyond, parity, f)
            for i in range(f * SPLIT, (f + 1) * SPLIT):
                landed(beyond, 1 - parity, i)
            far_out[f] = (far_acc[f] + asked_half(beyond, 1 - parity, f)).astype(far_out.dtype)
            acc[f] += gained_half(beyond, 1 - parity, f)
            answer(f).start()
        for f in range(TILES):
            for i in range(f * SPLIT, (f + 1) * SPLIT):
                landed(outer, 1 - parity, i)
            put(f, acc[f] + gained_half(outer, 1 - parity, f))

    for b in range(n_sp):
        for d in range(1, n_tp):
            part_across(b, d).wait_send()

        @pl.when(jnp.logical_and(z >= b, has_up))
        def _():
            part_along(b, 1).wait_send()

        @pl.when(jnp.logical_and(z <= b, has_down))
        def _():
            part_along(b, 0).wait_send()

    for copy in sum(shares, []):
        copy.wait_send()
    for i in range(CHUNKS):
        inward(i).wait_send()
        across(centre, i).wait_send()

    @pl.when(edge)
    def _():
        for i in range(CHUNKS):
            inward_far(i).wait_send()
        for a in range(2):
            ask(a).wait_send()

    @pl.when(inner)
    def _():
        for i in range(CHUNKS):
            outward(i).wait_send()
            passed(i).wait_send()
            across_beyond(i).wait_send()
        for a in range(2):
            hand(a).wait_send()
        for f in range(TILES):
            answer(f).wait_send()

    for f in range(TILES):
        stored(f).wait()


MESH = pl.DeviceIdType.MESH


def on_device_fused(
    n_sp, n_tp,
    query_latent, key_latent, rotary_key, query_gain, latent_gain,
    query_up, key_up, value_up, out_gain, out_weight,
):
    block_rows, row_count = query_latent.shape[0], key_latent.shape[0]
    rank, width = key_latent.shape[1], rotary_key.shape[1]
    keys = n_sp * n_tp * row_count
    depth, features = out_weight.shape
    cols = value_up.shape[1]
    vmem, bf16, dma = pltpu.VMEM, jnp.bfloat16, pltpu.SemaphoreType.DMA
    table = jnp.asarray(rope_table(keys, width))
    tiled = (TILES, block_rows, features // TILES)
    in_hbm = pl.BlockSpec(memory_space=pl.ANY)
    return pl.pallas_call(
        functools.partial(kernel, n_sp, n_tp),
        out_shape=jax.ShapeDtypeStruct((block_rows, features), bf16),
        in_specs=[in_hbm] * 11,
        out_specs=in_hbm,
        scratch_shapes=[
            vmem(query_latent.shape, bf16),
            vmem((query_gain.shape[0] // LANES, LANES), jnp.float32),
            vmem((1, rank), jnp.float32),
            vmem((1, cols), jnp.float32),
            vmem(table.shape, jnp.float32),
            vmem((n_sp, n_tp, row_count, rank + width), bf16),
            vmem((n_sp, TILES, depth, features // TILES), bf16),
            vmem(query_up.shape, bf16),
            vmem(key_up.shape, bf16),
            vmem(value_up.shape, bf16),
            vmem((keys, rank), bf16),
            vmem((keys, width), bf16),
            vmem((block_rows, query_up.shape[1]), bf16),
            vmem(query_latent.shape, bf16),
            vmem((n_tp, block_rows, cols + VALUE_DIM), bf16),
            vmem((block_rows, VALUE_DIM), jnp.float32),
            vmem(tiled, jnp.float32),
            vmem(tiled, jnp.float32),
            vmem((n_tp // 2, block_rows, cols), bf16),
            vmem(tiled, bf16),
            vmem(tiled, bf16),
            vmem(tiled, bf16),
            dma((10,)),
            dma((TILES,)),
            dma((TILES,)),
            dma((n_sp, n_tp + 1)),
            dma((n_sp, n_tp)),
            dma((cols // VALUE_DIM, n_tp)),
            dma((cols // VALUE_DIM, n_tp)),
            dma((6, CHUNKS)),
            dma((n_sp, 2, CHUNKS)),
            dma((2, 2)),
            dma((n_tp // 2, 2)),
            dma((TILES,)),
            dma((TILES,)),
        ],
        compiler_params=pltpu.CompilerParams(
            collective_id=0, has_side_effects=True
        ),
    )(
        query_latent, key_latent, rotary_key, query_gain.reshape(-1, LANES), latent_gain[None], out_gain[None],
        table, query_up, key_up, value_up, out_weight,
    )


def fits_fused(mesh):
    n_grp, n_sp, n_tp = (mesh.shape[name] for name in ("grp", "sp", "tp"))
    return n_grp % 2 == 0 and n_sp == LINE and n_sp == n_tp


def solution(mesh):
    in_specs = (
        P(("grp", "sp"), None),
        P(("grp", "sp", "tp"), None),
        P(("grp", "sp", "tp"), None),
        P(),
        P(),
        P(None, "tp"),
        P(None, "tp"),
        P(None, "tp"),
        P("tp"),
        P("sp", "tp"),
    )
    out_specs = P(("grp", "sp"), "tp")
    step = on_device
    if fits_fused(mesh):
        step = functools.partial(on_device_fused, mesh.shape["sp"], mesh.shape["tp"])
    return jax.shard_map(
        step, mesh=mesh, in_specs=in_specs, out_specs=out_specs, check_vma=False
    )
```

```python
import functools

import jax
import jax.numpy as jnp
import numpy as np
from jax import lax
from jax.experimental import pallas as pl
from jax.experimental.pallas import tpu as pltpu
from jax.sharding import PartitionSpec as P

HEADS = 16
NOPE_DIM = 128
ROPE_DIM = 64
VALUE_DIM = 128
KVRANK = 256


norm_eps = 1e-06
rope_theta = 10000.0


def rms_scaled(inputs, gain_vec):
    widened = inputs.astype(jnp.float32)
    return (
        widened
        * lax.rsqrt(jnp.mean(widened * widened, axis=-1, keepdims=True) + norm_eps)
        * gain_vec
    )


def rotate_half(inputs, positions):
    half_width = inputs.shape[-1] // 2
    inverse = rope_theta ** (-jnp.arange(half_width, dtype=jnp.float32) / half_width)
    angles = positions[:, None] * inverse[None, :]
    if inputs.ndim == 3:
        angles = angles[:, None, :]
    cosine = jnp.cos(angles)
    sine = jnp.sin(angles)
    widened = inputs.astype(jnp.float32)
    first = widened[..., :half_width]
    second = widened[..., half_width:]
    return jnp.concatenate(
        [first * cosine - second * sine, second * cosine + first * sine], axis=-1
    )


def on_device(
    query_latent,
    key_latent,
    rotary_key,
    query_gain,
    latent_gain,
    query_up,
    key_up,
    value_up,
    out_gain,
    out_weight,
):
    block_rows = query_latent.shape[0]
    row_count = key_latent.shape[0]
    head_local = key_up.shape[1] // NOPE_DIM
    block_start = lax.axis_index("sp") * block_rows
    own_start = block_start + lax.axis_index("tp") * row_count
    score_scale = (NOPE_DIM + ROPE_DIM) ** (-0.5)
    normed = rms_scaled(query_latent, query_gain).astype(jnp.bfloat16)
    query_full = jnp.dot(normed, query_up, preferred_element_type=jnp.float32).astype(jnp.bfloat16)
    query_full = query_full.reshape(block_rows, head_local, NOPE_DIM + ROPE_DIM)
    query_positions = (block_start + jnp.arange(block_rows, dtype=jnp.int32)).astype(jnp.float32)
    query_plain = query_full[..., :NOPE_DIM]
    query_turned = rotate_half(query_full[..., NOPE_DIM:], query_positions).astype(jnp.bfloat16)
    latent_normed = rms_scaled(key_latent, latent_gain).astype(jnp.bfloat16)
    own_positions = (own_start + jnp.arange(row_count, dtype=jnp.int32)).astype(jnp.float32)
    key_turned = rotate_half(rotary_key, own_positions).astype(jnp.bfloat16)
    running_max = jnp.full((block_rows, head_local), -1e30, jnp.float32)
    running_sum = jnp.zeros((block_rows, head_local), jnp.float32)
    weighted = jnp.zeros((block_rows, head_local, KVRANK), jnp.float32)
    latents = lax.all_gather(latent_normed, ("sp", "tp"), axis=0, tiled=True)
    turned_keys = lax.all_gather(key_turned, ("sp", "tp"), axis=0, tiled=True)
    portion_rows = latents.shape[0]
    step_rows = min(portion_rows, 2048)
    for begin in range(0, portion_rows, step_rows):
        latent_part = latents[begin : begin + step_rows]
        turned_part = turned_keys[begin : begin + step_rows]
        key_plain = jnp.dot(latent_part, key_up, preferred_element_type=jnp.float32).astype(
            jnp.bfloat16
        )
        key_plain = key_plain.reshape(latent_part.shape[0], head_local, NOPE_DIM)
        scores = jnp.einsum(
            "qhd,khd->qhk", query_plain, key_plain, preferred_element_type=jnp.float32
        )
        scores = scores + jnp.einsum(
            "qhd,kd->qhk", query_turned, turned_part, preferred_element_type=jnp.float32
        )
        scores = scores * score_scale
        new_max = jnp.maximum(running_max, jnp.max(scores, axis=-1))
        rescale = jnp.exp(running_max - new_max)
        expo = jnp.exp(scores - new_max[..., None])
        running_sum = running_sum * rescale + jnp.sum(expo, axis=-1)
        weighted = weighted * rescale[..., None] + jnp.einsum(
            "qhk,kc->qhc",
            expo.astype(jnp.bfloat16),
            latent_part,
            preferred_element_type=jnp.float32,
        )
        running_max = new_max
    final_state = (running_max, running_sum, weighted)
    running_max, running_sum, weighted = final_state
    latent_mix = (weighted / running_sum[..., None]).astype(jnp.bfloat16)
    value_heads = value_up.reshape(KVRANK, head_local, VALUE_DIM)
    head_out = jnp.einsum(
        "qhc,chd->qhd", latent_mix, value_heads, preferred_element_type=jnp.float32
    ).astype(jnp.bfloat16)
    head_out = head_out.reshape(block_rows, head_local * VALUE_DIM)
    widened = head_out.astype(jnp.float32)
    square_part = jnp.sum(widened * widened, axis=1)
    gained = (widened * out_gain).astype(jnp.bfloat16)
    all_gained, square_parts = (
        lax.all_gather(gained, "tp", axis=1, tiled=True),
        lax.all_gather(square_part[:, None].astype(jnp.bfloat16), "tp", axis=1, tiled=True).astype(
            jnp.float32
        ),
    )
    all_squares = jnp.sum(square_parts, axis=1)
    own_sums = jnp.dot(
        all_gained,
        lax.all_gather(out_weight, "sp", axis=0, tiled=True),
        preferred_element_type=jnp.float32,
    )
    mean_square = all_squares / (HEADS * VALUE_DIM)
    return (own_sums * lax.rsqrt(mean_square + norm_eps)[:, None]).astype(jnp.bfloat16)


LANES = 128
LINE = 4
TILES = 8
SPLIT = 2
CHUNKS = TILES * SPLIT
TAIL = 3


def rope_table(tokens, width):
    half = width // 2
    inverse = np.float32(rope_theta) ** (-np.arange(half, dtype=np.float32) / np.float32(half))
    angles = np.arange(tokens, dtype=np.float32)[:, None] * inverse.astype(np.float32)[None, :]
    wide = angles.astype(np.float32).astype(np.float64)
    cosine, sine = np.cos(wide), np.sin(wide)
    return np.concatenate([cosine, cosine, -sine, sine], axis=1).astype(np.float32)


def turned(wide, table):
    width = wide.shape[-1]
    half = width // 2
    swapped = jnp.concatenate([wide[:, half:], wide[:, :half]], axis=1)
    return wide * table[:, :width] + swapped * table[:, width:]


def kernel(
    n_sp, n_tp,
    ql_hbm, kl, rk, qg_hbm, lg_hbm, og_hbm, table_hbm, qup, kup, vup, ow, out_hbm,
    ql, qg, lg, og, table,
    lat, wbuf, qbuf, kbuf, vbuf, latn, kturn, qfull, qnorm, gall, squares, acc, asked,
    far_out, far_in, out,
    local, w_local, o_local, l_send, l_recv, g_send, g_recv,
    w_send, w_recv, q_send, q_recv, h_send, h_recv, f_send, f_recv,
):
    z, t, g = lax.axis_index("sp"), lax.axis_index("tp"), lax.axis_index("grp")
    parity = lax.rem(g, 2)
    partner = g + 1 - 2 * parity
    core = lax.rem(t, 2)
    sibling = t + 1 - 2 * core
    block_rows = ql.shape[0]
    depth = ow.shape[0]
    half = depth // 2
    piece = half // SPLIT
    tile = wbuf.shape[3]
    heads = kup.shape[1] // NOPE_DIM
    cols = heads * VALUE_DIM
    head_width = NOPE_DIM + ROPE_DIM
    rank = kl.shape[1]
    width = rk.shape[1]
    keys = n_sp * n_tp * kl.shape[0]

    lower = z < n_sp // 2
    toward = jnp.where(lower, 1, -1)
    centre = z + toward
    outer = z - toward
    beyond = centre + toward
    has_up, has_down = z < n_sp - 1, z > 0
    edge = jnp.logical_or(z == 0, z == n_sp - 1)
    inner = jnp.logical_not(edge)
    far_base = jnp.where(lower, n_tp // 2, 0)
    far_order = [*range(CHUNKS - TAIL, CHUNKS), *range(CHUNKS - TAIL)]

    loads = [
        pltpu.make_async_copy(src, dst, local.at[i])
        for i, (src, dst) in enumerate((
            (kl, lat.at[z, t, :, pl.ds(0, rank)]),
            (rk, lat.at[z, t, :, pl.ds(rank, width)]),
            (ql_hbm, ql),
            (qg_hbm, qg),
            (qup, qbuf),
            (lg_hbm, lg),
            (table_hbm, table),
            (kup, kbuf),
            (vup, vbuf),
            (og_hbm, og),
        ))
    ]
    w_loads = [
        pltpu.make_async_copy(ow.at[:, pl.ds(f * tile, tile)], wbuf.at[z, f], w_local.at[f])
        for f in range(TILES)
    ]
    for load in loads[:2] + w_loads[:1] + loads[2:5] + w_loads[1:] + loads[5:]:
        load.start()

    barrier = pltpu.get_barrier_semaphore()

    @pl.when(has_up)
    def _():
        pl.semaphore_signal(barrier, inc=1, device_id={"sp": z + 1}, device_id_type=MESH)

    @pl.when(has_down)
    def _():
        pl.semaphore_signal(barrier, inc=1, device_id={"sp": z - 1}, device_id_type=MESH)

    pl.semaphore_signal(barrier, inc=1, device_id={"grp": partner}, device_id_type=MESH)
    for d in range(1, n_tp):
        pl.semaphore_signal(barrier, inc=1, device_id={"tp": lax.rem(t + d, n_tp)}, device_id_type=MESH)
    pl.semaphore_wait(barrier, n_tp + jnp.where(edge, 1, 2))

    def remote(src, dst, send, recv, target):
        return pltpu.make_async_remote_copy(
            src_ref=src, dst_ref=dst, send_sem=send, recv_sem=recv,
            device_id=target, device_id_type=MESH,
        )

    def part_along(b, up):
        return remote(
            lat.at[b, t], lat.at[b, t], l_send.at[b, up], l_recv.at[b, t], {"sp": z + 1 if up else z - 1}
        )

    def part_across(b, d):
        return remote(
            lat.at[b, t], lat.at[b, t], l_send.at[b, 1 + d], l_recv.at[b, t], {"tp": lax.rem(t + d, n_tp)}
        )

    def spread(b):
        for d in range(1, n_tp):
            part_across(b, d).start()

    def arrive(d):
        @pl.when(z >= d)
        def _():
            part_along(z - d, 1).wait_recv()

            @pl.when(has_up)
            def _():
                part_along(z - d, 1).start()

            spread(z - d)

        @pl.when(z + d < n_sp)
        def _():
            part_along(z + d, 0).wait_recv()

            @pl.when(has_down)
            def _():
                part_along(z + d, 0).start()

            spread(z + d)

    def rows_of(b, p, i):
        start = pl.multiple_of(p * half + (i % SPLIT) * piece, piece)
        return wbuf.at[b, i // SPLIT, pl.ds(start, piece)]

    def moved(kind, b, p, i, target):
        return remote(rows_of(b, p, i), rows_of(b, p, i), w_send.at[kind, i], w_recv.at[b, p, i], target)

    def inward(i):
        return moved(0, z, parity, i, {"sp": centre})

    def outward(i):
        return moved(1, z, parity, i, {"sp": outer})

    def passed(i):
        return moved(2, outer, parity, i, {"sp": centre})

    def inward_far(i):
        return moved(3, z, 1 - parity, i, {"sp": centre})

    def passed_far(i):
        return moved(6, outer, 1 - parity, i, {"sp": centre})

    def across(b, i):
        return moved(4, b, parity, i, {"grp": partner})

    def across_beyond(i):
        return moved(5, beyond, parity, i, {"grp": partner})

    def landed(b, p, i):
        moved(0, b, p, i, {"sp": centre}).wait_recv()

    def near(i):
        if i % SPLIT == 0:
            w_loads[i // SPLIT].wait()
        inward(i).start()

    def near_out(i):
        @pl.when(inner)
        def _():
            outward(i).start()

    def near_far(some):
        @pl.when(edge)
        def _():
            for i in some:
                inward_far(i).start()

    def to_partner(i):
        landed(centre, parity, i)
        across(centre, i).start()

    def inner_hop(some):
        @pl.when(inner)
        def _():
            for i in some:
                landed(outer, parity, i)
                passed(i).start()
                to_partner(i)

    def edge_hop(some):
        @pl.when(edge)
        def _():
            for i in some:
                to_partner(i)

    def second_hop(i):
        landed(beyond, parity, i)
        if i < CHUNKS - TAIL:
            across_beyond(i).start()

    def first_hop_far():
        for i in range(CHUNKS - TAIL, CHUNKS):
            landed(outer, 1 - parity, i)
            passed_far(i).start()

    def queries():
        for load in loads[2:5]:
            load.wait()
        wide = ql[...].astype(jnp.float32)
        mean = jnp.mean(wide * wide, axis=-1, keepdims=True)
        gain = jnp.concatenate([qg[i : i + 1] for i in range(qg.shape[0])], axis=1)
        qnorm[...] = (wide * lax.rsqrt(mean + norm_eps) * gain).astype(jnp.bfloat16)
        qfull[...] = jnp.dot(qnorm[...], qbuf[...], preferred_element_type=jnp.float32).astype(
            jnp.bfloat16
        )

    def latents():
        for load in loads[5:]:
            load.wait()
        for b in range(n_sp):
            for d in range(1, n_tp):
                p = lax.rem(t + d, n_tp)
                remote(lat.at[b, p], lat.at[b, p], l_send.at[b, 1 + d], l_recv.at[b, p], {"tp": p}).wait_recv()
        whole = lat[...].reshape(keys, rank + width)
        wide = whole[:, :rank].astype(jnp.float32)
        mean = jnp.mean(wide * wide, axis=-1, keepdims=True)
        latn[...] = (wide * lax.rsqrt(mean + norm_eps) * lg[...]).astype(jnp.bfloat16)
        spun = whole[:, rank:].astype(jnp.float32)
        kturn[...] = turned(spun, table[...]).astype(jnp.bfloat16)

    transposed = (((1,), (1,)), ((), ()))

    def attend(h):
        start = h * head_width
        plain = qfull[:, start : start + NOPE_DIM]
        spun = qfull[:, start + NOPE_DIM : start + head_width].astype(jnp.float32)
        own = table[pl.ds(pl.multiple_of(z * block_rows, block_rows), block_rows), :]
        spun = turned(spun, own).astype(jnp.bfloat16)
        key_plain = jnp.dot(
            latn[...], kbuf[:, h * NOPE_DIM : (h + 1) * NOPE_DIM], preferred_element_type=jnp.float32
        ).astype(jnp.bfloat16)
        scores = lax.dot_general(plain, key_plain, transposed, preferred_element_type=jnp.float32)
        scores = scores + lax.dot_general(
            spun, kturn[...], transposed, preferred_element_type=jnp.float32
        )
        scores = scores * (head_width ** (-0.5))
        expo = jnp.exp(scores - jnp.max(scores, axis=-1, keepdims=True))
        total = jnp.sum(expo, axis=-1, keepdims=True)
        mix = jnp.dot(expo.astype(jnp.bfloat16), latn[...], preferred_element_type=jnp.float32)
        mix = (mix / total).astype(jnp.bfloat16)
        head_out = jnp.dot(
            mix, vbuf[:, h * VALUE_DIM : (h + 1) * VALUE_DIM], preferred_element_type=jnp.float32
        ).astype(jnp.bfloat16)
        wide = head_out.astype(jnp.float32)
        gained = wide * og[:, h * VALUE_DIM : (h + 1) * VALUE_DIM]
        gall[t, :, h * VALUE_DIM : (h + 1) * VALUE_DIM] = gained.astype(jnp.bfloat16)
        square = jnp.sum(wide * wide, axis=-1, keepdims=True)
        if h:
            square = square + squares[:, :1]
        squares[...] = jnp.broadcast_to(square, squares.shape)
        if h == heads - 1:
            gall[t, :, cols:] = squares[...].astype(jnp.bfloat16)

    def is_near(p):
        return jnp.logical_or(p < far_base, p >= far_base + n_tp // 2)

    def share_copy(h, d):
        part = gall.at[t, :, pl.ds(h * VALUE_DIM, VALUE_DIM)]
        return remote(part, part, g_send.at[h, d], g_recv.at[h, d], {"tp": lax.rem(t + d, n_tp)})

    def each_share(h, d, p, act):
        @pl.when(jnp.logical_or(inner, is_near(p)) if h < heads else True)
        def _():
            act(share_copy(h, d))

    def share(h):
        for d in range(1, n_tp):
            each_share(h, d, t, lambda copy: copy.start())
        if h < heads:
            @pl.when(asks)
            def _():
                for kind in range(2):
                    ask(h, kind).start()

    def sent(h):
        for d in range(1, n_tp):
            each_share(h, d, t, lambda copy: copy.wait_send())

    def gather(h):
        for d in range(1, n_tp):
            each_share(h, d, lax.rem(t + n_tp - d, n_tp), lambda copy: copy.wait_recv())

    asks = jnp.logical_and(edge, jnp.logical_not(is_near(t)))
    opposite = lax.rem(t + n_tp // 2, n_tp)

    def head_of(h):
        return pl.ds(h * VALUE_DIM, VALUE_DIM)

    def ask(h, kind):
        return remote(
            gall.at[t, :, head_of(h)], asked.at[core, :, head_of(h)],
            q_send.at[kind, h], q_recv.at[h], {"sp": centre, "tp": opposite} if kind else {"sp": centre},
        )

    def pair_of(a):
        return pl.ds(a * (cols // 2), cols // 2)

    def hand(c, a):
        part = asked.at[c, :, pair_of(a)]
        return remote(part, part, h_send.at[a], h_recv.at[a], {"tp": sibling})

    def hand_on(a):
        for h in range(a * heads // 2, (a + 1) * heads // 2):
            ask(h, 0).wait_recv()
        hand(core, a).start()

    def heard(a):
        hand(1 - core, a).wait_recv()

    def answer(f):
        return remote(far_out.at[f], far_in.at[f], f_send.at[f], f_recv.at[f], {"sp": outer})

    def part_of(p):
        return pl.ds(pl.multiple_of(p * half, half), half)

    def wide_of(b, some):
        return jnp.concatenate([wbuf[b, f] for f in some], axis=1)

    def dot(lhs, b, some):
        return jnp.dot(lhs, wide_of(b, some), preferred_element_type=jnp.float32)

    def gained(b):
        return gall[b, :, :cols]

    def keep(some, total, fresh=False):
        for n, f in enumerate(some):
            part = total[:, n * tile : (n + 1) * tile]
            acc[f] = part if fresh else acc[f] + part

    def stored(f):
        return pltpu.make_async_copy(out.at[f], out_hbm.at[:, pl.ds(f * tile, tile)], o_local.at[f])

    def set_scale():
        square = gall[0, :, cols : cols + 1].astype(jnp.float32)
        for p in range(1, n_tp):
            square = square + gall[p, :, cols : cols + 1].astype(jnp.float32)
        squares[...] = jnp.broadcast_to(lax.rsqrt(square / (n_tp * cols) + norm_eps), squares.shape)

    def put(f, total):
        out[f] = (total * squares[...]).astype(out.dtype)
        stored(f).start()

    def run(call, some):
        for i in some:
            call(i)

    tiles = range(TILES)
    pairs = [(f, f + 1) for f in range(0, TILES, 2)]

    def chunks_of(some):
        return range(some[0] * SPLIT, (some[-1] + 1) * SPLIT)

    loads[0].wait()
    loads[1].wait()

    @pl.when(has_up)
    def _():
        part_along(z, 1).start()

    @pl.when(has_down)
    def _():
        part_along(z, 0).start()

    spread(z)
    run(near, range(5))
    queries()
    arrive(1)
    run(near, range(5, CHUNKS))
    run(near_out, range(4))
    arrive(2)
    run(near_out, range(4, CHUNKS))
    inner_hop(range(4))
    arrive(3)
    inner_hop(range(4, 6))
    near_far(far_order[:4])
    latents()
    inner_hop(range(6, 8))
    attend(0)
    inner_hop(range(8, 10))
    edge_hop(range(6))
    near_far(far_order[4:8])
    attend(1)
    share(0)
    inner_hop(range(10, 12))
    edge_hop(range(6, 8))
    attend(2)
    share(1)
    inner_hop(range(12, 14))
    edge_hop(range(8, 9))
    near_far(far_order[8:12])
    attend(3)
    share(2)
    inner_hop(range(14, CHUNKS))
    edge_hop(range(9, 11))

    @pl.when(inner)
    def _():
        first_hop_far()
        run(second_hop, range(2))

    share(3)
    share(heads)

    @pl.when(edge)
    def _():
        run(to_partner, range(11, 13))
        for i in far_order[12:]:
            inward_far(i).start()
        run(to_partner, range(13, CHUNKS))
        for h in range(heads + 1):
            gather(h)
        set_scale()
        for some in pairs:
            keep(some, dot(gained(z), z, some), fresh=True)
        for some in pairs:
            for i in chunks_of(some):
                landed(centre, 1 - parity, i)
            keep(some, dot(gained(centre), centre, some))
        for f in tiles:
            answer(f).wait_recv()
            put(f, acc[f] + far_in[f].astype(jnp.float32))

    @pl.when(inner)
    def _():
        run(second_hop, range(2, 7))
        for h in range(heads + 1):
            gather(h)
        run(second_hop, range(7, 8))
        set_scale()
        for some in pairs:
            keep(some, dot(gained(z), z, some), fresh=True)
        hand_on(0)
        run(second_hop, range(8, 9))
        for i in range(CHUNKS):
            landed(centre, 1 - parity, i)
        for some in pairs:
            keep(some, dot(gained(centre), centre, some))
        hand_on(1)
        run(second_hop, range(9, 11))
        for a in range(2):
            heard(a)
        for some in pairs[:-1] + [(f,) for f in pairs[-1]]:
            run(second_hop, [i for i in chunks_of(some) if i >= 11])
            for i in chunks_of(some):
                landed(beyond, 1 - parity, i)
            both = jnp.concatenate([gained(beyond), asked[beyond - far_base]], axis=0)
            both = dot(both, beyond, some)
            far = both[block_rows:] + dot(asked[centre - far_base], centre, some)
            for n, f in enumerate(some):
                far_out[f] = far[:, n * tile : (n + 1) * tile].astype(far_out.dtype)
            for f in some:
                answer(f).start()
            keep(some, both[:block_rows])
        for i in range(CHUNKS - TAIL):
            landed(outer, 1 - parity, i)
        for some in pairs:
            total = dot(gained(outer), outer, some)
            for n, f in enumerate(some):
                put(f, acc[f] + total[:, n * tile : (n + 1) * tile])

    for b in range(n_sp):
        for d in range(1, n_tp):
            part_across(b, d).wait_send()

        @pl.when(jnp.logical_and(z >= b, has_up))
        def _():
            part_along(b, 1).wait_send()

        @pl.when(jnp.logical_and(z <= b, has_down))
        def _():
            part_along(b, 0).wait_send()

    for h in range(heads + 1):
        sent(h)
    for i in range(CHUNKS):
        inward(i).wait_send()
        across(centre, i).wait_send()

    @pl.when(edge)
    def _():
        for i in range(CHUNKS):
            inward_far(i).wait_send()

    @pl.when(asks)
    def _():
        for h in range(heads):
            for kind in range(2):
                ask(h, kind).wait_send()

    @pl.when(inner)
    def _():
        for i in range(CHUNKS):
            outward(i).wait_send()
            passed(i).wait_send()
            if i < CHUNKS - TAIL:
                across_beyond(i).wait_send()
            else:
                passed_far(i).wait_send()
        for a in range(2):
            hand(core, a).wait_send()
        for f in range(TILES):
            answer(f).wait_send()

    for f in range(TILES):
        stored(f).wait()


MESH = pl.DeviceIdType.MESH


def on_device_fused(
    n_sp, n_tp,
    query_latent, key_latent, rotary_key, query_gain, latent_gain,
    query_up, key_up, value_up, out_gain, out_weight,
):
    block_rows, row_count = query_latent.shape[0], key_latent.shape[0]
    rank, width = key_latent.shape[1], rotary_key.shape[1]
    keys = n_sp * n_tp * row_count
    depth, features = out_weight.shape
    cols = value_up.shape[1]
    vmem, bf16, dma = pltpu.VMEM, jnp.bfloat16, pltpu.SemaphoreType.DMA
    table = jnp.asarray(rope_table(keys, width))
    tiled = (TILES, block_rows, features // TILES)
    in_hbm = pl.BlockSpec(memory_space=pl.ANY)
    return pl.pallas_call(
        functools.partial(kernel, n_sp, n_tp),
        out_shape=jax.ShapeDtypeStruct((block_rows, features), bf16),
        in_specs=[in_hbm] * 11,
        out_specs=in_hbm,
        scratch_shapes=[
            vmem(query_latent.shape, bf16),
            vmem((query_gain.shape[0] // LANES, LANES), jnp.float32),
            vmem((1, rank), jnp.float32),
            vmem((1, cols), jnp.float32),
            vmem(table.shape, jnp.float32),
            vmem((n_sp, n_tp, row_count, rank + width), bf16),
            vmem((n_sp, TILES, depth, features // TILES), bf16),
            vmem(query_up.shape, bf16),
            vmem(key_up.shape, bf16),
            vmem(value_up.shape, bf16),
            vmem((keys, rank), bf16),
            vmem((keys, width), bf16),
            vmem((block_rows, query_up.shape[1]), bf16),
            vmem(query_latent.shape, bf16),
            vmem((n_tp, block_rows, cols + VALUE_DIM), bf16),
            vmem((block_rows, VALUE_DIM), jnp.float32),
            vmem(tiled, jnp.float32),
            vmem((n_tp // 2, block_rows, cols), bf16),
            vmem(tiled, bf16),
            vmem(tiled, bf16),
            vmem(tiled, bf16),
            dma((10,)),
            dma((TILES,)),
            dma((TILES,)),
            dma((n_sp, n_tp + 1)),
            dma((n_sp, n_tp)),
            dma((cols // VALUE_DIM + 1, n_tp)),
            dma((cols // VALUE_DIM + 1, n_tp)),
            dma((7, CHUNKS)),
            dma((n_sp, 2, CHUNKS)),
            dma((2, cols // VALUE_DIM)),
            dma((cols // VALUE_DIM,)),
            dma((2,)),
            dma((2,)),
            dma((TILES,)),
            dma((TILES,)),
        ],
        compiler_params=pltpu.CompilerParams(
            collective_id=0, has_side_effects=True
        ),
    )(
        query_latent, key_latent, rotary_key, query_gain.reshape(-1, LANES), latent_gain[None], out_gain[None],
        table, query_up, key_up, value_up, out_weight,
    )


def fits_fused(mesh):
    n_grp, n_sp, n_tp = (mesh.shape[name] for name in ("grp", "sp", "tp"))
    return n_grp % 2 == 0 and n_sp == LINE and n_sp == n_tp


def solution(mesh):
    in_specs = (
        P(("grp", "sp"), None),
        P(("grp", "sp", "tp"), None),
        P(("grp", "sp", "tp"), None),
        P(),
        P(),
        P(None, "tp"),
        P(None, "tp"),
        P(None, "tp"),
        P("tp"),
        P("sp", "tp"),
    )
    out_specs = P(("grp", "sp"), "tp")
    step = on_device
    if fits_fused(mesh):
        step = functools.partial(on_device_fused, mesh.shape["sp"], mesh.shape["tp"])
    return jax.shard_map(
        step, mesh=mesh, in_specs=in_specs, out_specs=out_specs, check_vma=False
    )
```

```python
import functools

import jax
import jax.numpy as jnp
import numpy as np
from jax import lax
from jax.experimental import pallas as pl
from jax.experimental.pallas import tpu as pltpu
from jax.sharding import PartitionSpec as P

HEADS = 16
NOPE_DIM = 128
ROPE_DIM = 64
VALUE_DIM = 128
KVRANK = 256


norm_eps = 1e-06
rope_theta = 10000.0


def rms_scaled(inputs, gain_vec):
    widened = inputs.astype(jnp.float32)
    return (
        widened
        * lax.rsqrt(jnp.mean(widened * widened, axis=-1, keepdims=True) + norm_eps)
        * gain_vec
    )


def rotate_half(inputs, positions):
    half_width = inputs.shape[-1] // 2
    inverse = rope_theta ** (-jnp.arange(half_width, dtype=jnp.float32) / half_width)
    angles = positions[:, None] * inverse[None, :]
    if inputs.ndim == 3:
        angles = angles[:, None, :]
    cosine = jnp.cos(angles)
    sine = jnp.sin(angles)
    widened = inputs.astype(jnp.float32)
    first = widened[..., :half_width]
    second = widened[..., half_width:]
    return jnp.concatenate(
        [first * cosine - second * sine, second * cosine + first * sine], axis=-1
    )


def on_device(
    query_latent,
    key_latent,
    rotary_key,
    query_gain,
    latent_gain,
    query_up,
    key_up,
    value_up,
    out_gain,
    out_weight,
):
    block_rows = query_latent.shape[0]
    row_count = key_latent.shape[0]
    head_local = key_up.shape[1] // NOPE_DIM
    block_start = lax.axis_index("sp") * block_rows
    own_start = block_start + lax.axis_index("tp") * row_count
    score_scale = (NOPE_DIM + ROPE_DIM) ** (-0.5)
    normed = rms_scaled(query_latent, query_gain).astype(jnp.bfloat16)
    query_full = jnp.dot(normed, query_up, preferred_element_type=jnp.float32).astype(jnp.bfloat16)
    query_full = query_full.reshape(block_rows, head_local, NOPE_DIM + ROPE_DIM)
    query_positions = (block_start + jnp.arange(block_rows, dtype=jnp.int32)).astype(jnp.float32)
    query_plain = query_full[..., :NOPE_DIM]
    query_turned = rotate_half(query_full[..., NOPE_DIM:], query_positions).astype(jnp.bfloat16)
    latent_normed = rms_scaled(key_latent, latent_gain).astype(jnp.bfloat16)
    own_positions = (own_start + jnp.arange(row_count, dtype=jnp.int32)).astype(jnp.float32)
    key_turned = rotate_half(rotary_key, own_positions).astype(jnp.bfloat16)
    running_max = jnp.full((block_rows, head_local), -1e30, jnp.float32)
    running_sum = jnp.zeros((block_rows, head_local), jnp.float32)
    weighted = jnp.zeros((block_rows, head_local, KVRANK), jnp.float32)
    latents = lax.all_gather(latent_normed, ("sp", "tp"), axis=0, tiled=True)
    turned_keys = lax.all_gather(key_turned, ("sp", "tp"), axis=0, tiled=True)
    portion_rows = latents.shape[0]
    step_rows = min(portion_rows, 2048)
    for begin in range(0, portion_rows, step_rows):
        latent_part = latents[begin : begin + step_rows]
        turned_part = turned_keys[begin : begin + step_rows]
        key_plain = jnp.dot(latent_part, key_up, preferred_element_type=jnp.float32).astype(
            jnp.bfloat16
        )
        key_plain = key_plain.reshape(latent_part.shape[0], head_local, NOPE_DIM)
        scores = jnp.einsum(
            "qhd,khd->qhk", query_plain, key_plain, preferred_element_type=jnp.float32
        )
        scores = scores + jnp.einsum(
            "qhd,kd->qhk", query_turned, turned_part, preferred_element_type=jnp.float32
        )
        scores = scores * score_scale
        new_max = jnp.maximum(running_max, jnp.max(scores, axis=-1))
        rescale = jnp.exp(running_max - new_max)
        expo = jnp.exp(scores - new_max[..., None])
        running_sum = running_sum * rescale + jnp.sum(expo, axis=-1)
        weighted = weighted * rescale[..., None] + jnp.einsum(
            "qhk,kc->qhc",
            expo.astype(jnp.bfloat16),
            latent_part,
            preferred_element_type=jnp.float32,
        )
        running_max = new_max
    final_state = (running_max, running_sum, weighted)
    running_max, running_sum, weighted = final_state
    latent_mix = (weighted / running_sum[..., None]).astype(jnp.bfloat16)
    value_heads = value_up.reshape(KVRANK, head_local, VALUE_DIM)
    head_out = jnp.einsum(
        "qhc,chd->qhd", latent_mix, value_heads, preferred_element_type=jnp.float32
    ).astype(jnp.bfloat16)
    head_out = head_out.reshape(block_rows, head_local * VALUE_DIM)
    widened = head_out.astype(jnp.float32)
    square_part = jnp.sum(widened * widened, axis=1)
    gained = (widened * out_gain).astype(jnp.bfloat16)
    all_gained, square_parts = (
        lax.all_gather(gained, "tp", axis=1, tiled=True),
        lax.all_gather(square_part[:, None].astype(jnp.bfloat16), "tp", axis=1, tiled=True).astype(
            jnp.float32
        ),
    )
    all_squares = jnp.sum(square_parts, axis=1)
    own_sums = jnp.dot(
        all_gained,
        lax.all_gather(out_weight, "sp", axis=0, tiled=True),
        preferred_element_type=jnp.float32,
    )
    mean_square = all_squares / (HEADS * VALUE_DIM)
    return (own_sums * lax.rsqrt(mean_square + norm_eps)[:, None]).astype(jnp.bfloat16)


LANES = 128
LINE = 4
TILES = 8


def rope_table(tokens, width):
    half = width // 2
    inverse = np.float32(rope_theta) ** (-np.arange(half, dtype=np.float32) / np.float32(half))
    angles = np.arange(tokens, dtype=np.float32)[:, None] * inverse.astype(np.float32)[None, :]
    wide = angles.astype(np.float32).astype(np.float64)
    cosine, sine = np.cos(wide), np.sin(wide)
    return np.concatenate([cosine, cosine, -sine, sine], axis=1).astype(np.float32)


def turned(wide, table):
    width = wide.shape[-1]
    half = width // 2
    swapped = jnp.concatenate([wide[:, half:], wide[:, :half]], axis=1)
    return wide * table[:, :width] + swapped * table[:, width:]


def kernel(
    n_sp, n_tp,
    ql_hbm, kl, rk, qg_hbm, lg_hbm, og_hbm, table_hbm, qup, kup, vup, ow, out_hbm,
    ql, ql_outer, qg, lg, og, table,
    lat, wbuf, qbuf, kbuf, vbuf, latn, kturn, qfull, qfull_outer, qnorm, gall, squares, squares_outer, tally,
    acc, asked,
    far_out, far_in, out,
    local, w_local, o_local, l_send, l_recv, g_send, g_recv,
    w_send, w_recv, m_recv, q_send, q_recv, h_send, h_recv, f_send, f_recv,
):
    z, t, g = lax.axis_index("sp"), lax.axis_index("tp"), lax.axis_index("grp")
    parity = lax.rem(g, 2)
    partner = g + 1 - 2 * parity
    core = lax.rem(t, 2)
    sibling = t + 1 - 2 * core
    block_rows = ql.shape[0]
    depth = ow.shape[0]
    half = depth // 2
    piece = half // 2
    tile = wbuf.shape[3]
    heads = kup.shape[1] // NOPE_DIM
    cols = heads * VALUE_DIM
    head_width = NOPE_DIM + ROPE_DIM
    rank = kl.shape[1]
    width = rk.shape[1]
    keys = n_sp * n_tp * kl.shape[0]

    lower = z < n_sp // 2
    toward = jnp.where(lower, 1, -1)
    centre = z + toward
    outer = z - toward
    beyond = centre + toward
    has_up, has_down = z < n_sp - 1, z > 0
    edge = jnp.logical_or(z == 0, z == n_sp - 1)
    inner = jnp.logical_not(edge)
    far_base = jnp.where(lower, n_tp // 2, 0)
    far_group = jnp.logical_and(t >= far_base, t < far_base + n_tp // 2)
    helps = jnp.logical_and(inner, far_group)
    helped = jnp.logical_and(edge, far_group)

    loads = [
        pltpu.make_async_copy(src, dst, local.at[i])
        for i, (src, dst) in enumerate((
            (kl, lat.at[z, t, :, pl.ds(0, rank)]),
            (rk, lat.at[z, t, :, pl.ds(rank, width)]),
            (ql_hbm, ql),
            (qg_hbm, qg),
            (qup, qbuf),
            (lg_hbm, lg),
            (table_hbm, table),
            (kup, kbuf),
            (vup, vbuf),
            (og_hbm, og),
        ))
    ]
    def w_load(f):
        return pltpu.make_async_copy(
            ow.at[:, pl.ds(f * tile, tile)], wbuf.at[z, f], w_local.at[min(f, 1)]
        )

    for load in loads[:3]:
        load.start()
    w_load(0).start()
    for load in loads[3:5]:
        load.start()
    for f in range(1, TILES):
        w_load(f).start()
    for load in loads[5:]:
        load.start()

    barrier = pltpu.get_barrier_semaphore()

    @pl.when(has_up)
    def _():
        pl.semaphore_signal(barrier, inc=1, device_id={"sp": z + 1}, device_id_type=MESH)

    @pl.when(has_down)
    def _():
        pl.semaphore_signal(barrier, inc=1, device_id={"sp": z - 1}, device_id_type=MESH)

    pl.semaphore_signal(barrier, inc=1, device_id={"grp": partner}, device_id_type=MESH)
    for d in range(1, n_tp):
        pl.semaphore_signal(barrier, inc=1, device_id={"tp": lax.rem(t + d, n_tp)}, device_id_type=MESH)
    pl.semaphore_wait(barrier, n_tp + jnp.where(edge, 1, 2))

    def remote(src, dst, send, recv, target):
        return pltpu.make_async_remote_copy(
            src_ref=src, dst_ref=dst, send_sem=send, recv_sem=recv,
            device_id=target, device_id_type=MESH,
        )

    opposite = lax.rem(t + n_tp // 2, n_tp)

    def drain(ref, send):
        remote(ref, ref, send, send, {"tp": opposite}).wait_send()

    def expect(ref, recv):
        remote(ref, ref, recv, recv, {"tp": opposite}).wait_recv()

    def part_along(b, up):
        way = jnp.where(lower, 1 - up, up)
        return remote(lat.at[b, t], lat.at[b, t], l_send.at[way], l_recv.at[b], {"sp": z + 1 if up else z - 1})

    def part_across(b, d):
        return remote(
            lat.at[b, t], lat.at[b, t], l_send.at[2], l_recv.at[n_sp], {"tp": lax.rem(t + d, n_tp)}
        )

    def spread(b):
        for d in range(1, n_tp):
            part_across(b, d).start()

    def arrive(d):
        @pl.when(z >= d)
        def _():
            part_along(z - d, 1).wait_recv()

            @pl.when(has_up)
            def _():
                part_along(z - d, 1).start()

            spread(z - d)

        @pl.when(z + d < n_sp)
        def _():
            part_along(z + d, 0).wait_recv()

            @pl.when(has_down)
            def _():
                part_along(z + d, 0).start()

            spread(z + d)

    NEAR_OUTER, NEAR_CENTRE, BEYOND_NEAR, BEYOND_FAR = range(4)
    CENTRE_FAR, TAIL_TILE, TAIL_PIECE, REST_TILES, REST_PIECE = range(5)
    last, split = TILES - 1, TILES - 2

    def rows_of(b, p, f, start=0, rows=None):
        return wbuf.at[b, f, pl.ds(pl.multiple_of(p * half + start, piece), rows or half)]

    def moved(kind, ref, recv, target):
        return remote(ref, ref, w_send.at[kind], recv, target)

    def inward(f):
        role = jnp.where(edge, NEAR_OUTER, NEAR_CENTRE)
        return moved(0, rows_of(z, parity, f), w_recv.at[role, f], {"sp": centre})

    def outward(f):
        return moved(1, rows_of(z, parity, f), w_recv.at[NEAR_CENTRE, f], {"sp": outer})

    def passed(f):
        return moved(2, rows_of(outer, parity, f), w_recv.at[BEYOND_NEAR, f], {"sp": centre})

    def inward_far(ref, part):
        return moved(3, ref, m_recv.at[part], {"sp": centre})

    def across(f):
        return moved(4, rows_of(centre, parity, f), m_recv.at[CENTRE_FAR], {"grp": partner})

    def across_beyond(f):
        return moved(5, rows_of(beyond, parity, f), w_recv.at[BEYOND_FAR, f], {"grp": partner})

    def across_piece():
        return moved(
            6, rows_of(beyond, parity, split, 0, piece), w_recv.at[BEYOND_FAR, split], {"grp": partner}
        )

    def passed_far():
        return (
            moved(7, rows_of(outer, 1 - parity, last), w_recv.at[BEYOND_FAR, last], {"sp": centre}),
            moved(
                7, rows_of(outer, 1 - parity, split, piece, piece), w_recv.at[BEYOND_FAR, split], {"sp": centre}
            ),
        )

    def landed(role, f):
        expect(wbuf.at[0, f, pl.ds(0, half)], w_recv.at[role, f])

    def near(f):
        if f == 0:
            w_load(0).wait()
        if f == 1:
            rest = wbuf.at[z, pl.ds(1, last)]
            pltpu.make_async_copy(rest, rest, w_local.at[1]).wait()
        inward(f).start()

    def near_out(f):
        @pl.when(inner)
        def _():
            outward(f).start()

    def near_far():
        @pl.when(edge)
        def _():
            inward_far(rows_of(z, 1 - parity, last), TAIL_TILE).start()
            inward_far(rows_of(z, 1 - parity, split, piece, piece), TAIL_PIECE).start()
            for f in range(split):
                inward_far(rows_of(z, 1 - parity, f), REST_TILES).start()
            inward_far(rows_of(z, 1 - parity, split, 0, piece), REST_PIECE).start()

    def to_partner(f):
        landed(NEAR_CENTRE, f)
        across(f).start()

    def inner_partner(some):
        @pl.when(inner)
        def _():
            for f in some:
                to_partner(f)

    def inner_pass(some):
        @pl.when(inner)
        def _():
            for f in some:
                landed(NEAR_OUTER, f)
                passed(f).start()

    def edge_partner(some):
        @pl.when(edge)
        def _():
            for f in some:
                to_partner(f)

    def second_hop(f):
        landed(BEYOND_NEAR, f)
        if f < split:
            across_beyond(f).start()
        if f == split:
            across_piece().start()

    def first_hop_far():
        expect(wbuf.at[0, 0, pl.ds(0, half)], m_recv.at[TAIL_TILE])
        expect(wbuf.at[0, 0, pl.ds(0, piece)], m_recv.at[TAIL_PIECE])
        for copy in passed_far():
            copy.start()

    def outer_rest():
        expect(wbuf.at[0, pl.ds(0, split), pl.ds(0, half)], m_recv.at[REST_TILES])
        expect(wbuf.at[0, 0, pl.ds(0, piece)], m_recv.at[REST_PIECE])

    def centre_far():
        expect(wbuf.at[0, :, pl.ds(0, half)], m_recv.at[CENTRE_FAR])

    def project(latent, full):
        wide = latent[...].astype(jnp.float32)
        mean = jnp.mean(wide * wide, axis=-1, keepdims=True)
        gain = jnp.concatenate([qg[i : i + 1] for i in range(qg.shape[0])], axis=1)
        qnorm[...] = (wide * lax.rsqrt(mean + norm_eps) * gain).astype(jnp.bfloat16)
        full[...] = jnp.dot(qnorm[...], qbuf[...], preferred_element_type=jnp.float32).astype(
            jnp.bfloat16
        )

    def lend():
        return remote(ql, ql_outer, h_send.at[1], h_recv.at[1], {"sp": centre})

    def queries():
        for load in loads[3:5]:
            load.wait()
        project(ql, qfull)

    def outer_queries():
        @pl.when(helps)
        def _():
            lend().wait_recv()
            project(ql_outer, qfull_outer)

    def latents():
        for load in loads[5:]:
            load.wait()
        expect(lat.at[:, pl.ds(0, n_tp - 1)], l_recv.at[n_sp])
        whole = lat[...].reshape(keys, rank + width)
        wide = whole[:, :rank].astype(jnp.float32)
        mean = jnp.mean(wide * wide, axis=-1, keepdims=True)
        latn[...] = (wide * lax.rsqrt(mean + norm_eps) * lg[...]).astype(jnp.bfloat16)
        spun = whole[:, rank:].astype(jnp.float32)
        kturn[...] = turned(spun, table[...]).astype(jnp.bfloat16)

    transposed = (((1,), (1,)), ((), ()))

    def attend_with(h, full, block, store, squares):
        start = h * head_width
        plain = full[:, start : start + NOPE_DIM]
        spun = full[:, start + NOPE_DIM : start + head_width].astype(jnp.float32)
        own = table[pl.ds(pl.multiple_of(block * block_rows, block_rows), block_rows), :]
        spun = turned(spun, own).astype(jnp.bfloat16)
        key_plain = jnp.dot(
            latn[...], kbuf[:, h * NOPE_DIM : (h + 1) * NOPE_DIM], preferred_element_type=jnp.float32
        ).astype(jnp.bfloat16)
        scores = lax.dot_general(plain, key_plain, transposed, preferred_element_type=jnp.float32)
        scores = scores + lax.dot_general(
            spun, kturn[...], transposed, preferred_element_type=jnp.float32
        )
        scores = scores * (head_width ** (-0.5))
        expo = jnp.exp(scores - jnp.max(scores, axis=-1, keepdims=True))
        total = jnp.sum(expo, axis=-1, keepdims=True)
        mix = jnp.dot(expo.astype(jnp.bfloat16), latn[...], preferred_element_type=jnp.float32)
        mix = (mix / total).astype(jnp.bfloat16)
        head_out = jnp.dot(
            mix, vbuf[:, h * VALUE_DIM : (h + 1) * VALUE_DIM], preferred_element_type=jnp.float32
        ).astype(jnp.bfloat16)
        wide = head_out.astype(jnp.float32)
        gained = wide * og[:, h * VALUE_DIM : (h + 1) * VALUE_DIM]
        store(gained.astype(jnp.bfloat16))
        square = jnp.sum(wide * wide, axis=-1, keepdims=True)
        if h:
            square = square + squares[:, :1]
        squares[...] = jnp.broadcast_to(square, squares.shape)

    def attend(h):
        def store(value):
            gall[t, :, h * VALUE_DIM : (h + 1) * VALUE_DIM] = value

        attend_with(h, qfull, z, store, squares)
        if h == heads - 1:
            gall[t, :, cols:] = squares[...].astype(jnp.bfloat16)

    def attend_outer(h):
        def store(value):
            asked[core, :, h * VALUE_DIM : (h + 1) * VALUE_DIM] = value

        attend_with(h, qfull_outer, outer, store, squares_outer)
        if h == heads - 1:
            tally[...] = squares_outer[...].astype(jnp.bfloat16)

    def is_near(p):
        return jnp.logical_or(p < far_base, p >= far_base + n_tp // 2)

    def share(h):
        @pl.when(jnp.logical_or(inner, is_near(t)) if h < heads else True)
        def _():
            for d in range(1, n_tp):
                part = gall.at[t, :, pl.ds(h * VALUE_DIM, VALUE_DIM)]
                kind = h // heads
                remote(part, part, g_send.at[kind], g_recv.at[kind], {"tp": lax.rem(t + d, n_tp)}).start()

    def slabs(count, span):
        return gall.at[pl.ds(0, count), :, pl.ds(0, span)]

    def gather():
        for where, count in (
            (inner, n_tp - 1),
            (jnp.logical_and(edge, is_near(t)), n_tp // 2 - 1),
            (helped, n_tp // 2),
        ):
            @pl.when(where)
            def _():
                expect(slabs(count, cols), g_recv.at[0])

        expect(slabs(n_tp - 1, VALUE_DIM), g_recv.at[1])

    def ask(h):
        part = asked.at[core, :, pl.ds(h * VALUE_DIM, VALUE_DIM)]
        return remote(part, part, q_send.at[0], q_recv.at[0], {"tp": opposite})

    def tell():
        return remote(
            tally, gall.at[t, :, pl.ds(cols, VALUE_DIM)], h_send.at[2], h_recv.at[2], {"sp": outer}
        )

    def hand(c):
        return remote(asked.at[c], asked.at[c], h_send.at[0], h_recv.at[0], {"tp": sibling})

    def hand_on():
        @pl.when(jnp.logical_not(helps))
        def _():
            expect(asked.at[0], q_recv.at[0])

        hand(core).start()

    def heard():
        hand(1 - core).wait_recv()

    def answer(f):
        return remote(far_out.at[f], far_in.at[f], f_send.at[0], f_recv.at[f], {"sp": outer})

    def part_of(p):
        return pl.ds(pl.multiple_of(p * half, half), half)

    def wide_of(b, some):
        return jnp.concatenate([wbuf[b, f] for f in some], axis=1)

    def dot(lhs, b, some):
        return jnp.dot(lhs, wide_of(b, some), preferred_element_type=jnp.float32)

    def gained(b):
        return gall[b, :, :cols]

    def keep(some, total, fresh=False):
        for n, f in enumerate(some):
            part = total[:, n * tile : (n + 1) * tile]
            acc[f] = part if fresh else acc[f] + part

    def stored(f):
        return pltpu.make_async_copy(out.at[f], out_hbm.at[:, pl.ds(f * tile, tile)], o_local.at[0])

    def set_scale():
        square = gall[0, :, cols : cols + 1].astype(jnp.float32)
        for p in range(1, n_tp):
            square = square + gall[p, :, cols : cols + 1].astype(jnp.float32)
        squares[...] = jnp.broadcast_to(lax.rsqrt(square / (n_tp * cols) + norm_eps), squares.shape)

    def put(f, total):
        out[f] = (total * squares[...]).astype(out.dtype)
        stored(f).start()

    def run(call, some):
        for i in some:
            call(i)

    tiles = range(TILES)
    pairs = [(f, f + 1) for f in range(0, TILES, 2)]

    loads[0].wait()
    loads[1].wait()

    @pl.when(has_up)
    def _():
        part_along(z, 1).start()

    @pl.when(has_down)
    def _():
        part_along(z, 0).start()

    spread(z)
    loads[2].wait()

    @pl.when(helped)
    def _():
        lend().start()

    run(near, range(2))
    queries()
    arrive(1)
    run(near, range(2, TILES))
    run(near_out, range(2))
    inner_partner(range(2))
    arrive(2)
    run(near_out, range(2, TILES))
    inner_partner(range(2, 3))
    arrive(3)
    near_far()
    outer_queries()
    inner_partner(range(3, 4))
    latents()
    inner_partner(range(4, 5))
    inner_pass(range(2))

    @pl.when(helps)
    def _():
        attend_outer(0)
        run(to_partner, range(5, 6))
        attend_outer(1)
        ask(0).start()
        inner_pass(range(2, 4))
        run(to_partner, range(6, 7))
        attend_outer(2)
        ask(1).start()
        inner_pass(range(4, 5))
        attend_outer(3)
        ask(2).start()
        run(to_partner, range(7, TILES))
        inner_pass(range(5, 6))
        ask(3).start()
        tell().start()
        attend(0)
        hand_on()
        inner_pass(range(6, 7))
        attend(1)
        share(0)
        run(second_hop, range(1))
        attend(2)
        share(1)
        inner_pass(range(7, TILES))
        run(second_hop, range(1, 2))
        attend(3)
        share(2)
        run(second_hop, range(2, 3))
        share(3)

    @pl.when(is_near(t))
    def _():
        attend(0)
        inner_partner(range(5, 6))
        inner_pass(range(2, 4))
        edge_partner(range(5))
        attend(1)
        share(0)
        inner_pass(range(4, 5))
        edge_partner(range(5, 6))
        attend(2)
        share(1)
        inner_partner(range(6, 7))
        inner_pass(range(5, 6))
        edge_partner(range(6, 7))
        attend(3)
        share(2)
        inner_partner(range(7, TILES))
        inner_pass(range(6, TILES))
        edge_partner(range(7, TILES))
        share(3)

        @pl.when(inner)
        def _():
            run(second_hop, range(2))
            hand_on()
            run(second_hop, range(2, 3))

    @pl.when(helped)
    def _():
        run(to_partner, tiles)
        tell().wait_recv()

    share(heads)

    @pl.when(edge)
    def _():
        gather()
        set_scale()
        for some in pairs:
            keep(some, dot(gained(z), z, some), fresh=True)
        centre_far()
        for some in pairs:
            keep(some, dot(gained(centre), centre, some))
        for f in tiles:
            answer(f).wait_recv()
            put(f, acc[f] + far_in[f].astype(jnp.float32))

    def reply(f):
        landed(BEYOND_FAR, f)
        far = dot(asked[beyond - far_base], beyond, (f,)) + dot(asked[centre - far_base], centre, (f,))
        far_out[f] = far.astype(far_out.dtype)
        answer(f).start()

    @pl.when(inner)
    def _():
        first_hop_far()
        run(second_hop, range(3, 4))
        heard()
        centre_far()
        for f in range(4):
            reply(f)
            run(second_hop, range(f + 4, f + 5))
        reply(4)
        gather()
        set_scale()
        for some in pairs[:2]:
            keep(some, dot(gained(z), z, some) + dot(gained(centre), centre, some), fresh=True)
        reply(5)
        for some in pairs[2:]:
            keep(some, dot(gained(z), z, some) + dot(gained(centre), centre, some), fresh=True)
        reply(6)
        reply(7)
        outer_rest()
        for some in pairs:
            total = dot(gained(outer), outer, some) + dot(gained(beyond), beyond, some)
            for n, f in enumerate(some):
                put(f, acc[f] + total[:, n * tile : (n + 1) * tile])

    halves = wbuf.at[0, :, pl.ds(0, half)]
    drain(lat.at[:, pl.ds(0, n_tp - 1)], l_send.at[2])
    drain(slabs(n_tp - 1, VALUE_DIM), g_send.at[1])
    drain(halves, w_send.at[0])
    drain(halves, w_send.at[4])

    @pl.when(jnp.logical_or(inner, is_near(t)))
    def _():
        drain(slabs(n_tp - 1, cols), g_send.at[0])

    @pl.when(edge)
    def _():
        drain(lat.at[0, pl.ds(0, 1)], l_send.at[0])
        drain(halves, w_send.at[3])

    @pl.when(helped)
    def _():
        lend().wait_send()

    @pl.when(helps)
    def _():
        drain(asked.at[0], q_send.at[0])
        tell().wait_send()

    @pl.when(inner)
    def _():
        drain(lat.at[0, pl.ds(0, 2)], l_send.at[0])
        drain(lat.at[0, pl.ds(0, 3)], l_send.at[1])
        drain(halves, w_send.at[1])
        drain(halves, w_send.at[2])
        drain(wbuf.at[0, pl.ds(0, split), pl.ds(0, half)], w_send.at[5])
        across_piece().wait_send()
        drain(wbuf.at[0, 0, pl.ds(0, half + piece)], w_send.at[7])
        hand(core).wait_send()
        drain(far_out, f_send.at[0])

    pltpu.make_async_copy(out, out, o_local.at[0]).wait()


MESH = pl.DeviceIdType.MESH


def on_device_fused(
    n_sp, n_tp,
    query_latent, key_latent, rotary_key, query_gain, latent_gain,
    query_up, key_up, value_up, out_gain, out_weight,
):
    block_rows, row_count = query_latent.shape[0], key_latent.shape[0]
    rank, width = key_latent.shape[1], rotary_key.shape[1]
    keys = n_sp * n_tp * row_count
    depth, features = out_weight.shape
    cols = value_up.shape[1]
    vmem, bf16, dma = pltpu.VMEM, jnp.bfloat16, pltpu.SemaphoreType.DMA
    table = jnp.asarray(rope_table(keys, width))
    tiled = (TILES, block_rows, features // TILES)
    in_hbm = pl.BlockSpec(memory_space=pl.ANY)
    return pl.pallas_call(
        functools.partial(kernel, n_sp, n_tp),
        out_shape=jax.ShapeDtypeStruct((block_rows, features), bf16),
        in_specs=[in_hbm] * 11,
        out_specs=in_hbm,
        scratch_shapes=[
            vmem(query_latent.shape, bf16),
            vmem(query_latent.shape, bf16),
            vmem((query_gain.shape[0] // LANES, LANES), jnp.float32),
            vmem((1, rank), jnp.float32),
            vmem((1, cols), jnp.float32),
            vmem(table.shape, jnp.float32),
            vmem((n_sp, n_tp, row_count, rank + width), bf16),
            vmem((n_sp, TILES, depth, features // TILES), bf16),
            vmem(query_up.shape, bf16),
            vmem(key_up.shape, bf16),
            vmem(value_up.shape, bf16),
            vmem((keys, rank), bf16),
            vmem((keys, width), bf16),
            vmem((block_rows, query_up.shape[1]), bf16),
            vmem((block_rows, query_up.shape[1]), bf16),
            vmem(query_latent.shape, bf16),
            vmem((n_tp, block_rows, cols + VALUE_DIM), bf16),
            vmem((block_rows, VALUE_DIM), jnp.float32),
            vmem((block_rows, VALUE_DIM), jnp.float32),
            vmem((block_rows, VALUE_DIM), bf16),
            vmem(tiled, jnp.float32),
            vmem((n_tp // 2, block_rows, cols), bf16),
            vmem(tiled, bf16),
            vmem(tiled, bf16),
            vmem(tiled, bf16),
            dma((10,)),
            dma((2,)),
            dma((1,)),
            dma((3,)),
            dma((n_sp + 1,)),
            dma((2,)),
            dma((2,)),
            dma((8,)),
            dma((4, TILES)),
            dma((5,)),
            dma((1,)),
            dma((1,)),
            dma((3,)),
            dma((3,)),
            dma((1,)),
            dma((TILES,)),
        ],
        compiler_params=pltpu.CompilerParams(
            collective_id=0, has_side_effects=True
        ),
    )(
        query_latent, key_latent, rotary_key, query_gain.reshape(-1, LANES), latent_gain[None], out_gain[None],
        table, query_up, key_up, value_up, out_weight,
    )


def fits_fused(mesh):
    n_grp, n_sp, n_tp = (mesh.shape[name] for name in ("grp", "sp", "tp"))
    return n_grp % 2 == 0 and n_sp == LINE and n_sp == n_tp


def solution(mesh):
    in_specs = (
        P(("grp", "sp"), None),
        P(("grp", "sp", "tp"), None),
        P(("grp", "sp", "tp"), None),
        P(),
        P(),
        P(None, "tp"),
        P(None, "tp"),
        P(None, "tp"),
        P("tp"),
        P("sp", "tp"),
    )
    out_specs = P(("grp", "sp"), "tp")
    step = on_device
    if fits_fused(mesh):
        step = functools.partial(on_device_fused, mesh.shape["sp"], mesh.shape["tp"])
    return jax.shard_map(
        step, mesh=mesh, in_specs=in_specs, out_specs=out_specs, check_vma=False
    )
```

```python
import functools

import jax
import jax.numpy as jnp
import numpy as np
from jax import lax
from jax.experimental import pallas as pl
from jax.experimental.pallas import tpu as pltpu
from jax.sharding import PartitionSpec as P

HEADS = 16
NOPE_DIM = 128
ROPE_DIM = 64
VALUE_DIM = 128
KVRANK = 256


norm_eps = 1e-06
rope_theta = 10000.0


def rms_scaled(inputs, gain_vec):
    widened = inputs.astype(jnp.float32)
    return (
        widened
        * lax.rsqrt(jnp.mean(widened * widened, axis=-1, keepdims=True) + norm_eps)
        * gain_vec
    )


def rotate_half(inputs, positions):
    half_width = inputs.shape[-1] // 2
    inverse = rope_theta ** (-jnp.arange(half_width, dtype=jnp.float32) / half_width)
    angles = positions[:, None] * inverse[None, :]
    if inputs.ndim == 3:
        angles = angles[:, None, :]
    cosine = jnp.cos(angles)
    sine = jnp.sin(angles)
    widened = inputs.astype(jnp.float32)
    first = widened[..., :half_width]
    second = widened[..., half_width:]
    return jnp.concatenate(
        [first * cosine - second * sine, second * cosine + first * sine], axis=-1
    )


def on_device(
    query_latent,
    key_latent,
    rotary_key,
    query_gain,
    latent_gain,
    query_up,
    key_up,
    value_up,
    out_gain,
    out_weight,
):
    block_rows = query_latent.shape[0]
    row_count = key_latent.shape[0]
    head_local = key_up.shape[1] // NOPE_DIM
    block_start = lax.axis_index("sp") * block_rows
    own_start = block_start + lax.axis_index("tp") * row_count
    score_scale = (NOPE_DIM + ROPE_DIM) ** (-0.5)
    normed = rms_scaled(query_latent, query_gain).astype(jnp.bfloat16)
    query_full = jnp.dot(normed, query_up, preferred_element_type=jnp.float32).astype(jnp.bfloat16)
    query_full = query_full.reshape(block_rows, head_local, NOPE_DIM + ROPE_DIM)
    query_positions = (block_start + jnp.arange(block_rows, dtype=jnp.int32)).astype(jnp.float32)
    query_plain = query_full[..., :NOPE_DIM]
    query_turned = rotate_half(query_full[..., NOPE_DIM:], query_positions).astype(jnp.bfloat16)
    latent_normed = rms_scaled(key_latent, latent_gain).astype(jnp.bfloat16)
    own_positions = (own_start + jnp.arange(row_count, dtype=jnp.int32)).astype(jnp.float32)
    key_turned = rotate_half(rotary_key, own_positions).astype(jnp.bfloat16)
    running_max = jnp.full((block_rows, head_local), -1e30, jnp.float32)
    running_sum = jnp.zeros((block_rows, head_local), jnp.float32)
    weighted = jnp.zeros((block_rows, head_local, KVRANK), jnp.float32)
    latents = lax.all_gather(latent_normed, ("sp", "tp"), axis=0, tiled=True)
    turned_keys = lax.all_gather(key_turned, ("sp", "tp"), axis=0, tiled=True)
    portion_rows = latents.shape[0]
    step_rows = min(portion_rows, 2048)
    for begin in range(0, portion_rows, step_rows):
        latent_part = latents[begin : begin + step_rows]
        turned_part = turned_keys[begin : begin + step_rows]
        key_plain = jnp.dot(latent_part, key_up, preferred_element_type=jnp.float32).astype(
            jnp.bfloat16
        )
        key_plain = key_plain.reshape(latent_part.shape[0], head_local, NOPE_DIM)
        scores = jnp.einsum(
            "qhd,khd->qhk", query_plain, key_plain, preferred_element_type=jnp.float32
        )
        scores = scores + jnp.einsum(
            "qhd,kd->qhk", query_turned, turned_part, preferred_element_type=jnp.float32
        )
        scores = scores * score_scale
        new_max = jnp.maximum(running_max, jnp.max(scores, axis=-1))
        rescale = jnp.exp(running_max - new_max)
        expo = jnp.exp(scores - new_max[..., None])
        running_sum = running_sum * rescale + jnp.sum(expo, axis=-1)
        weighted = weighted * rescale[..., None] + jnp.einsum(
            "qhk,kc->qhc",
            expo.astype(jnp.bfloat16),
            latent_part,
            preferred_element_type=jnp.float32,
        )
        running_max = new_max
    final_state = (running_max, running_sum, weighted)
    running_max, running_sum, weighted = final_state
    latent_mix = (weighted / running_sum[..., None]).astype(jnp.bfloat16)
    value_heads = value_up.reshape(KVRANK, head_local, VALUE_DIM)
    head_out = jnp.einsum(
        "qhc,chd->qhd", latent_mix, value_heads, preferred_element_type=jnp.float32
    ).astype(jnp.bfloat16)
    head_out = head_out.reshape(block_rows, head_local * VALUE_DIM)
    widened = head_out.astype(jnp.float32)
    square_part = jnp.sum(widened * widened, axis=1)
    gained = (widened * out_gain).astype(jnp.bfloat16)
    all_gained, square_parts = (
        lax.all_gather(gained, "tp", axis=1, tiled=True),
        lax.all_gather(square_part[:, None].astype(jnp.bfloat16), "tp", axis=1, tiled=True).astype(
            jnp.float32
        ),
    )
    all_squares = jnp.sum(square_parts, axis=1)
    own_sums = jnp.dot(
        all_gained,
        lax.all_gather(out_weight, "sp", axis=0, tiled=True),
        preferred_element_type=jnp.float32,
    )
    mean_square = all_squares / (HEADS * VALUE_DIM)
    return (own_sums * lax.rsqrt(mean_square + norm_eps)[:, None]).astype(jnp.bfloat16)


LANES = 128
LINE = 4
TILES = 8


def rope_table(tokens, width):
    half = width // 2
    inverse = np.float32(rope_theta) ** (-np.arange(half, dtype=np.float32) / np.float32(half))
    angles = np.arange(tokens, dtype=np.float32)[:, None] * inverse.astype(np.float32)[None, :]
    wide = angles.astype(np.float32).astype(np.float64)
    cosine, sine = np.cos(wide), np.sin(wide)
    return np.concatenate([cosine, cosine, -sine, sine], axis=1).astype(np.float32)


def turned(wide, table):
    width = wide.shape[-1]
    half = width // 2
    swapped = jnp.concatenate([wide[:, half:], wide[:, :half]], axis=1)
    return wide * table[:, :width] + swapped * table[:, width:]


def kernel(
    n_sp, n_tp,
    ql_hbm, kl, rk, qg_hbm, lg_hbm, og_hbm, table_hbm, qup, kup, vup, ow, out_hbm,
    ql, ql_outer, qg, lg, og, table,
    lat, wbuf, qbuf, kbuf, vbuf, latn, kturn, qfull, qfull_outer, qnorm, gall, squares, squares_outer, tally,
    acc, asked,
    far_out, far_in, out,
    local, w_local, o_local, sends, l_recv, g_recv, w_recv, m_recv, q_recv, h_recv, f_recv,
):
    z, t, g = lax.axis_index("sp"), lax.axis_index("tp"), lax.axis_index("grp")
    parity = lax.rem(g, 2)
    partner = g + 1 - 2 * parity
    core = lax.rem(t, 2)
    sibling = t + 1 - 2 * core
    block_rows = ql.shape[0]
    depth = ow.shape[0]
    half = depth // 2
    piece = half // 2
    tile = wbuf.shape[3]
    heads = kup.shape[1] // NOPE_DIM
    cols = heads * VALUE_DIM
    head_width = NOPE_DIM + ROPE_DIM
    rank = kl.shape[1]
    width = rk.shape[1]
    keys = n_sp * n_tp * kl.shape[0]

    lower = z < n_sp // 2
    toward = jnp.where(lower, 1, -1)
    centre = z + toward
    outer = z - toward
    beyond = centre + toward
    has_up, has_down = z < n_sp - 1, z > 0
    edge = jnp.logical_or(z == 0, z == n_sp - 1)
    inner = jnp.logical_not(edge)
    far_base = jnp.where(lower, n_tp // 2, 0)
    far_group = jnp.logical_and(t >= far_base, t < far_base + n_tp // 2)
    helps = jnp.logical_and(inner, far_group)
    helped = jnp.logical_and(edge, far_group)

    loads = [
        pltpu.make_async_copy(src, dst, local.at[i])
        for i, src, dst in (
            (0, kl, lat.at[z, t, :, pl.ds(0, rank)]),
            (0, rk, lat.at[z, t, :, pl.ds(rank, width)]),
            (1, ql_hbm, ql),
            (2, qg_hbm, qg),
            (2, qup, qbuf),
            (3, lg_hbm, lg),
            (3, table_hbm, table),
            (3, kup, kbuf),
            (3, vup, vbuf),
            (3, og_hbm, og),
        )
    ]
    def w_load(f):
        return pltpu.make_async_copy(
            ow.at[:, pl.ds(f * tile, tile)], wbuf.at[z, f], w_local.at[min(f, 1)]
        )

    for load in loads[:3]:
        load.start()
    w_load(0).start()
    for load in loads[3:5]:
        load.start()
    for f in range(1, TILES):
        w_load(f).start()
    for load in loads[5:]:
        load.start()

    barrier = pltpu.get_barrier_semaphore()

    @pl.when(has_up)
    def _():
        pl.semaphore_signal(barrier, inc=1, device_id={"sp": z + 1}, device_id_type=MESH)

    @pl.when(has_down)
    def _():
        pl.semaphore_signal(barrier, inc=1, device_id={"sp": z - 1}, device_id_type=MESH)

    pl.semaphore_signal(barrier, inc=1, device_id={"grp": partner}, device_id_type=MESH)
    for d in range(1, n_tp):
        pl.semaphore_signal(barrier, inc=1, device_id={"tp": lax.rem(t + d, n_tp)}, device_id_type=MESH)
    pl.semaphore_wait(barrier, n_tp + jnp.where(edge, 1, 2))

    def remote(src, dst, recv, target):
        return pltpu.make_async_remote_copy(
            src_ref=src, dst_ref=dst, send_sem=sends.at[0], recv_sem=recv,
            device_id=target, device_id_type=MESH,
        )

    opposite = lax.rem(t + n_tp // 2, n_tp)

    def drain(ref):
        remote(ref, ref, sends.at[0], {"tp": opposite}).wait_send()

    def expect(ref, recv):
        remote(ref, ref, recv, {"tp": opposite}).wait_recv()

    def part_along(b, up):
        return remote(lat.at[b, t], lat.at[b, t], l_recv.at[b], {"sp": z + 1 if up else z - 1})

    def part_across(b, d):
        return remote(lat.at[b, t], lat.at[b, t], l_recv.at[n_sp], {"tp": lax.rem(t + d, n_tp)})

    def spread(b):
        for d in range(1, n_tp):
            part_across(b, d).start()

    def arrive(d):
        @pl.when(z >= d)
        def _():
            part_along(z - d, 1).wait_recv()

            @pl.when(has_up)
            def _():
                part_along(z - d, 1).start()

            spread(z - d)

        @pl.when(z + d < n_sp)
        def _():
            part_along(z + d, 0).wait_recv()

            @pl.when(has_down)
            def _():
                part_along(z + d, 0).start()

            spread(z + d)

    FROM_OUTER = 0
    FROM_CENTRE, BEYOND_NEAR, BEYOND_FAR = (TILES // 2 + TILES * i for i in range(3))
    CENTRE_FAR, TAIL_TILE, TAIL_PIECE, REST_TILES, REST_PIECE = range(5)
    last, split = TILES - 1, TILES - 2

    def rows_of(b, p, f, start=0, rows=None):
        return wbuf.at[b, f, pl.ds(pl.multiple_of(p * half + start, piece), rows or half)]

    def moved(ref, recv, target):
        return remote(ref, ref, recv, target)

    def inward(f):
        role = jnp.where(edge, FROM_OUTER + f // 2, FROM_CENTRE + f)
        return moved(rows_of(z, parity, f), w_recv.at[role], {"sp": centre})

    def outward(f):
        return moved(rows_of(z, parity, f), w_recv.at[FROM_CENTRE + f], {"sp": outer})

    def passed(f):
        return moved(rows_of(outer, parity, f), w_recv.at[BEYOND_NEAR + f], {"sp": centre})

    def inward_far(ref, part):
        return moved(ref, m_recv.at[part], {"sp": centre})

    def across(f):
        return moved(rows_of(centre, parity, f), m_recv.at[CENTRE_FAR], {"grp": partner})

    def across_beyond(f):
        return moved(rows_of(beyond, parity, f), w_recv.at[BEYOND_FAR + f], {"grp": partner})

    def across_piece():
        return moved(
            rows_of(beyond, parity, split, 0, piece), w_recv.at[BEYOND_FAR + split], {"grp": partner}
        )

    def pass_tail(f, start=0, rows=None):
        return moved(
            rows_of(outer, 1 - parity, f, start, rows), w_recv.at[BEYOND_FAR + f], {"sp": centre}
        )

    def landed(role, f):
        expect(wbuf.at[0, f, pl.ds(0, half)], w_recv.at[role + f])

    def near(f):
        if f == 0:
            w_load(0).wait()
        if f == 1:
            rest = wbuf.at[z, pl.ds(1, last)]
            pltpu.make_async_copy(rest, rest, w_local.at[1]).wait()
        inward(f).start()

    def near_out(f):
        @pl.when(inner)
        def _():
            outward(f).start()

    def near_far():
        @pl.when(edge)
        def _():
            inward_far(rows_of(z, 1 - parity, split, piece, piece), TAIL_PIECE).start()
            inward_far(rows_of(z, 1 - parity, split, 0, piece), REST_PIECE).start()
            inward_far(rows_of(z, 1 - parity, last), TAIL_TILE).start()
            for f in range(split):
                inward_far(rows_of(z, 1 - parity, f), REST_TILES).start()

    def to_partner(f):
        landed(FROM_CENTRE, f)
        across(f).start()

    def inner_partner(some):
        @pl.when(inner)
        def _():
            for f in some:
                to_partner(f)

    def inner_pass(pair):
        @pl.when(inner)
        def _():
            expect(wbuf.at[0, pl.ds(0, 2), pl.ds(0, half)], w_recv.at[FROM_OUTER + pair])
            for f in (2 * pair, 2 * pair + 1):
                passed(f).start()

    def edge_partner(some):
        @pl.when(edge)
        def _():
            for f in some:
                to_partner(f)

    def second_hop(f):
        landed(BEYOND_NEAR, f)
        if f < split:
            across_beyond(f).start()
        if f == split:
            @pl.when(core == 1)
            def _():
                across_piece().start()

    def pass_tails():
        expect(wbuf.at[0, 0, pl.ds(0, piece)], m_recv.at[TAIL_PIECE])
        pass_tail(split, piece, piece).start()

        @pl.when(core == 0)
        def _():
            expect(wbuf.at[0, 0, pl.ds(0, piece)], m_recv.at[REST_PIECE])
            pass_tail(split, 0, piece).start()

        expect(wbuf.at[0, 0, pl.ds(0, half)], m_recv.at[TAIL_TILE])
        pass_tail(last).start()

    def outer_rest():
        expect(wbuf.at[0, pl.ds(0, split), pl.ds(0, half)], m_recv.at[REST_TILES])

        @pl.when(core == 1)
        def _():
            expect(wbuf.at[0, 0, pl.ds(0, piece)], m_recv.at[REST_PIECE])

    def centre_far():
        expect(wbuf.at[0, :, pl.ds(0, half)], m_recv.at[CENTRE_FAR])

    def project(latent, full):
        wide = latent[...].astype(jnp.float32)
        mean = jnp.mean(wide * wide, axis=-1, keepdims=True)
        gain = jnp.concatenate([qg[i : i + 1] for i in range(qg.shape[0])], axis=1)
        qnorm[...] = (wide * lax.rsqrt(mean + norm_eps) * gain).astype(jnp.bfloat16)
        full[...] = jnp.dot(qnorm[...], qbuf[...], preferred_element_type=jnp.float32).astype(
            jnp.bfloat16
        )

    def lend():
        return remote(ql, ql_outer, h_recv.at[1], {"sp": centre})

    def queries():
        for load in loads[3:5]:
            load.wait()
        project(ql, qfull)

    def outer_queries():
        @pl.when(helps)
        def _():
            lend().wait_recv()
            project(ql_outer, qfull_outer)

    def latents():
        for load in loads[5:]:
            load.wait()
        expect(lat.at[:, pl.ds(0, n_tp - 1)], l_recv.at[n_sp])
        whole = lat[...].reshape(keys, rank + width)
        wide = whole[:, :rank].astype(jnp.float32)
        mean = jnp.mean(wide * wide, axis=-1, keepdims=True)
        latn[...] = (wide * lax.rsqrt(mean + norm_eps) * lg[...]).astype(jnp.bfloat16)
        spun = whole[:, rank:].astype(jnp.float32)
        kturn[...] = turned(spun, table[...]).astype(jnp.bfloat16)

    transposed = (((1,), (1,)), ((), ()))

    def attend_with(h, full, block, store, squares):
        start = h * head_width
        plain = full[:, start : start + NOPE_DIM]
        spun = full[:, start + NOPE_DIM : start + head_width].astype(jnp.float32)
        own = table[pl.ds(pl.multiple_of(block * block_rows, block_rows), block_rows), :]
        spun = turned(spun, own).astype(jnp.bfloat16)
        key_plain = jnp.dot(
            latn[...], kbuf[:, h * NOPE_DIM : (h + 1) * NOPE_DIM], preferred_element_type=jnp.float32
        ).astype(jnp.bfloat16)
        scores = lax.dot_general(plain, key_plain, transposed, preferred_element_type=jnp.float32)
        scores = scores + lax.dot_general(
            spun, kturn[...], transposed, preferred_element_type=jnp.float32
        )
        scores = scores * (head_width ** (-0.5))
        expo = jnp.exp(scores - jnp.max(scores, axis=-1, keepdims=True))
        total = jnp.sum(expo, axis=-1, keepdims=True)
        mix = jnp.dot(expo.astype(jnp.bfloat16), latn[...], preferred_element_type=jnp.float32)
        mix = (mix / total).astype(jnp.bfloat16)
        head_out = jnp.dot(
            mix, vbuf[:, h * VALUE_DIM : (h + 1) * VALUE_DIM], preferred_element_type=jnp.float32
        ).astype(jnp.bfloat16)
        wide = head_out.astype(jnp.float32)
        gained = wide * og[:, h * VALUE_DIM : (h + 1) * VALUE_DIM]
        store(gained.astype(jnp.bfloat16))
        square = jnp.sum(wide * wide, axis=-1, keepdims=True)
        if h:
            square = square + squares[:, :1]
        squares[...] = jnp.broadcast_to(square, squares.shape)

    def attend(h):
        def store(value):
            gall[t, :, h * VALUE_DIM : (h + 1) * VALUE_DIM] = value

        attend_with(h, qfull, z, store, squares)
        if h == heads - 1:
            gall[t, :, cols:] = squares[...].astype(jnp.bfloat16)

    def attend_outer(h):
        def store(value):
            asked[core, :, h * VALUE_DIM : (h + 1) * VALUE_DIM] = value

        attend_with(h, qfull_outer, outer, store, squares_outer)
        if h == heads - 1:
            tally[...] = squares_outer[...].astype(jnp.bfloat16)

    def is_near(p):
        return jnp.logical_or(p < far_base, p >= far_base + n_tp // 2)

    def share(h):
        @pl.when(jnp.logical_or(inner, is_near(t)) if h < heads else True)
        def _():
            for d in range(1, n_tp):
                part = gall.at[t, :, pl.ds(h * VALUE_DIM, VALUE_DIM)]
                kind = h // heads
                remote(part, part, g_recv.at[kind], {"tp": lax.rem(t + d, n_tp)}).start()

    def slabs(count, span):
        return gall.at[pl.ds(0, count), :, pl.ds(0, span)]

    def gather():
        for where, count in (
            (inner, n_tp - 1),
            (jnp.logical_and(edge, is_near(t)), n_tp // 2 - 1),
            (helped, n_tp // 2),
        ):
            @pl.when(where)
            def _():
                expect(slabs(count, cols), g_recv.at[0])

        expect(slabs(n_tp - 1, VALUE_DIM), g_recv.at[1])

    def ask(h):
        part = asked.at[core, :, pl.ds(h * VALUE_DIM, VALUE_DIM)]
        return remote(part, part, q_recv.at[0], {"tp": opposite})

    def tell():
        return remote(tally, gall.at[t, :, pl.ds(cols, VALUE_DIM)], h_recv.at[2], {"sp": outer})

    def hand(c):
        return remote(asked.at[c], asked.at[c], h_recv.at[0], {"tp": sibling})

    def hand_on():
        @pl.when(jnp.logical_not(helps))
        def _():
            expect(asked.at[0], q_recv.at[0])

        hand(core).start()

    def heard():
        hand(1 - core).wait_recv()

    groups = (tuple(range(split - 2)), (split - 2, split - 1), (split,), (last,))

    def answer(f):
        n = [f in some for some in groups].index(True)
        return remote(far_out.at[f], far_in.at[f], f_recv.at[n], {"sp": outer})

    def wide_of(b, some):
        return jnp.concatenate([wbuf[b, f] for f in some], axis=1)

    def dot(lhs, b, some):
        return jnp.dot(lhs, wide_of(b, some), preferred_element_type=jnp.float32)

    def gained(b):
        return gall[b, :, :cols]

    def keep(some, total, fresh=False):
        for n, f in enumerate(some):
            part = total[:, n * tile : (n + 1) * tile]
            acc[f] = part if fresh else acc[f] + part

    def stored(f):
        return pltpu.make_async_copy(out.at[f], out_hbm.at[:, pl.ds(f * tile, tile)], o_local.at[0])

    def set_scale():
        square = gall[0, :, cols : cols + 1].astype(jnp.float32)
        for p in range(1, n_tp):
            square = square + gall[p, :, cols : cols + 1].astype(jnp.float32)
        squares[...] = jnp.broadcast_to(lax.rsqrt(square / (n_tp * cols) + norm_eps), squares.shape)

    def put(f, total):
        out[f] = (total * squares[...]).astype(out.dtype)
        stored(f).start()

    def run(call, some):
        for i in some:
            call(i)

    tiles = range(TILES)
    pairs = [(f, f + 1) for f in range(0, TILES, 2)]

    loads[0].wait()
    loads[1].wait()

    @pl.when(has_up)
    def _():
        part_along(z, 1).start()

    @pl.when(has_down)
    def _():
        part_along(z, 0).start()

    spread(z)
    loads[2].wait()

    @pl.when(helped)
    def _():
        lend().start()

    run(near, range(3))
    queries()
    arrive(1)
    run(near, range(3, TILES))
    run(near_out, range(2))
    inner_partner(range(2))
    arrive(2)
    run(near_out, range(2, TILES))
    inner_partner(range(2, 3))
    arrive(3)
    near_far()
    outer_queries()
    inner_partner(range(3, 4))
    latents()
    inner_partner(range(4, 5))
    inner_pass(0)

    @pl.when(helps)
    def _():
        attend_outer(0)
        run(to_partner, range(5, 6))
        attend_outer(1)
        ask(0).start()
        inner_pass(1)
        run(to_partner, range(6, 7))
        attend_outer(2)
        ask(1).start()
        run(to_partner, range(7, TILES))
        attend_outer(3)
        ask(2).start()
        inner_pass(2)
        ask(3).start()
        tell().start()
        attend(0)
        hand_on()
        run(second_hop, range(1))
        attend(1)
        share(0)
        attend(2)
        share(1)
        inner_pass(3)
        run(second_hop, range(1, 2))
        attend(3)
        share(2)
        run(second_hop, range(2, 3))
        share(3)

    @pl.when(is_near(t))
    def _():
        attend(0)
        inner_partner(range(5, 6))
        inner_pass(1)
        edge_partner(range(5))
        attend(1)
        share(0)
        edge_partner(range(5, 6))
        attend(2)
        share(1)
        inner_partner(range(6, TILES))
        inner_pass(2)
        edge_partner(range(6, 7))
        attend(3)
        share(2)
        inner_pass(3)
        edge_partner(range(7, TILES))
        share(3)

        @pl.when(inner)
        def _():
            run(second_hop, range(2))
            hand_on()
            run(second_hop, range(2, 3))

    @pl.when(helped)
    def _():
        run(to_partner, tiles)
        tell().wait_recv()

    share(heads)

    @pl.when(edge)
    def _():
        gather()
        set_scale()
        for some in pairs:
            keep(some, dot(gained(z), z, some), fresh=True)
        centre_far()
        for some in pairs:
            keep(some, dot(gained(centre), centre, some))
        for n, some in enumerate(groups):
            expect(far_in.at[pl.ds(0, len(some))], f_recv.at[n])
            for f in some:
                put(f, acc[f] + far_in[f].astype(jnp.float32))

    def reply(f):
        landed(BEYOND_FAR, f)
        far = dot(asked[beyond - far_base], beyond, (f,)) + dot(asked[centre - far_base], centre, (f,))
        far_out[f] = far.astype(far_out.dtype)
        answer(f).start()

    @pl.when(inner)
    def _():
        pl.when(core == 0)(pass_tails)
        run(second_hop, range(3, 4))
        heard()
        centre_far()
        for f in range(4):
            reply(f)
            if f == 2:
                pl.when(core == 1)(pass_tails)
            run(second_hop, range(f + 4, f + 5))
        reply(4)
        gather()
        set_scale()
        for some in pairs[:2]:
            keep(some, dot(gained(z), z, some) + dot(gained(centre), centre, some), fresh=True)
        reply(5)
        reply(6)
        reply(7)
        for some in pairs[2:]:
            keep(some, dot(gained(z), z, some) + dot(gained(centre), centre, some), fresh=True)
        outer_rest()
        for some in pairs:
            total = dot(gained(outer), outer, some) + dot(gained(beyond), beyond, some)
            for n, f in enumerate(some):
                put(f, acc[f] + total[:, n * tile : (n + 1) * tile])

    halves = wbuf.at[0, :, pl.ds(0, half)]
    drain(lat.at[:, pl.ds(0, n_tp - 1)])
    drain(slabs(n_tp - 1, VALUE_DIM))
    for _ in range(2):
        drain(halves)

    @pl.when(jnp.logical_or(inner, is_near(t)))
    def _():
        drain(slabs(n_tp - 1, cols))

    @pl.when(edge)
    def _():
        drain(lat.at[0, pl.ds(0, 1)])
        drain(halves)

    @pl.when(helped)
    def _():
        drain(ql)

    @pl.when(helps)
    def _():
        drain(asked.at[0])
        drain(tally)

    @pl.when(inner)
    def _():
        for count in (2, 3):
            drain(lat.at[0, pl.ds(0, count)])
        for _ in range(3):
            drain(halves)
        drain(asked.at[0])
        drain(far_out)

    pltpu.make_async_copy(out, out, o_local.at[0]).wait()


MESH = pl.DeviceIdType.MESH


def on_device_fused(
    n_sp, n_tp,
    query_latent, key_latent, rotary_key, query_gain, latent_gain,
    query_up, key_up, value_up, out_gain, out_weight,
):
    block_rows, row_count = query_latent.shape[0], key_latent.shape[0]
    rank, width = key_latent.shape[1], rotary_key.shape[1]
    keys = n_sp * n_tp * row_count
    depth, features = out_weight.shape
    cols = value_up.shape[1]
    vmem, bf16, dma = pltpu.VMEM, jnp.bfloat16, pltpu.SemaphoreType.DMA
    table = jnp.asarray(rope_table(keys, width))
    tiled = (TILES, block_rows, features // TILES)
    in_hbm = pl.BlockSpec(memory_space=pl.ANY)
    return pl.pallas_call(
        functools.partial(kernel, n_sp, n_tp),
        out_shape=jax.ShapeDtypeStruct((block_rows, features), bf16),
        in_specs=[in_hbm] * 11,
        out_specs=in_hbm,
        scratch_shapes=[
            vmem(query_latent.shape, bf16),
            vmem(query_latent.shape, bf16),
            vmem((query_gain.shape[0] // LANES, LANES), jnp.float32),
            vmem((1, rank), jnp.float32),
            vmem((1, cols), jnp.float32),
            vmem(table.shape, jnp.float32),
            vmem((n_sp, n_tp, row_count, rank + width), bf16),
            vmem((n_sp, TILES, depth, features // TILES), bf16),
            vmem(query_up.shape, bf16),
            vmem(key_up.shape, bf16),
            vmem(value_up.shape, bf16),
            vmem((keys, rank), bf16),
            vmem((keys, width), bf16),
            vmem((block_rows, query_up.shape[1]), bf16),
            vmem((block_rows, query_up.shape[1]), bf16),
            vmem(query_latent.shape, bf16),
            vmem((n_tp, block_rows, cols + VALUE_DIM), bf16),
            vmem((block_rows, VALUE_DIM), jnp.float32),
            vmem((block_rows, VALUE_DIM), jnp.float32),
            vmem((block_rows, VALUE_DIM), bf16),
            vmem(tiled, jnp.float32),
            vmem((n_tp // 2, block_rows, cols), bf16),
            vmem(tiled, bf16),
            vmem(tiled, bf16),
            vmem(tiled, bf16),
            dma((4,)),
            dma((2,)),
            dma((1,)),
            dma((1,)),
            dma((n_sp + 1,)),
            dma((2,)),
            dma((TILES // 2 + 3 * TILES,)),
            dma((5,)),
            dma((1,)),
            dma((3,)),
            dma((4,)),
        ],
        compiler_params=pltpu.CompilerParams(
            collective_id=0, has_side_effects=True
        ),
    )(
        query_latent, key_latent, rotary_key, query_gain.reshape(-1, LANES), latent_gain[None], out_gain[None],
        table, query_up, key_up, value_up, out_weight,
    )


def fits_fused(mesh):
    n_grp, n_sp, n_tp = (mesh.shape[name] for name in ("grp", "sp", "tp"))
    return n_grp % 2 == 0 and n_sp == LINE and n_sp == n_tp


def solution(mesh):
    in_specs = (
        P(("grp", "sp"), None),
        P(("grp", "sp", "tp"), None),
        P(("grp", "sp", "tp"), None),
        P(),
        P(),
        P(None, "tp"),
        P(None, "tp"),
        P(None, "tp"),
        P("tp"),
        P("sp", "tp"),
    )
    out_specs = P(("grp", "sp"), "tp")
    step = on_device
    if fits_fused(mesh):
        step = functools.partial(on_device_fused, mesh.shape["sp"], mesh.shape["tp"])
    return jax.shard_map(
        step, mesh=mesh, in_specs=in_specs, out_specs=out_specs, check_vma=False
    )
```

```python
import functools

import jax
import jax.numpy as jnp
import numpy as np
from jax import lax
from jax.experimental import pallas as pl
from jax.experimental.pallas import tpu as pltpu
from jax.sharding import PartitionSpec as P

HEADS = 16
NOPE_DIM = 128
ROPE_DIM = 64
VALUE_DIM = 128
KVRANK = 256


norm_eps = 1e-06
rope_theta = 10000.0


def rms_scaled(inputs, gain_vec):
    widened = inputs.astype(jnp.float32)
    return (
        widened
        * lax.rsqrt(jnp.mean(widened * widened, axis=-1, keepdims=True) + norm_eps)
        * gain_vec
    )


def rotate_half(inputs, positions):
    half_width = inputs.shape[-1] // 2
    inverse = rope_theta ** (-jnp.arange(half_width, dtype=jnp.float32) / half_width)
    angles = positions[:, None] * inverse[None, :]
    if inputs.ndim == 3:
        angles = angles[:, None, :]
    cosine = jnp.cos(angles)
    sine = jnp.sin(angles)
    widened = inputs.astype(jnp.float32)
    first = widened[..., :half_width]
    second = widened[..., half_width:]
    return jnp.concatenate(
        [first * cosine - second * sine, second * cosine + first * sine], axis=-1
    )


def on_device(
    query_latent,
    key_latent,
    rotary_key,
    query_gain,
    latent_gain,
    query_up,
    key_up,
    value_up,
    out_gain,
    out_weight,
):
    block_rows = query_latent.shape[0]
    row_count = key_latent.shape[0]
    head_local = key_up.shape[1] // NOPE_DIM
    block_start = lax.axis_index("sp") * block_rows
    own_start = block_start + lax.axis_index("tp") * row_count
    score_scale = (NOPE_DIM + ROPE_DIM) ** (-0.5)
    normed = rms_scaled(query_latent, query_gain).astype(jnp.bfloat16)
    query_full = jnp.dot(normed, query_up, preferred_element_type=jnp.float32).astype(jnp.bfloat16)
    query_full = query_full.reshape(block_rows, head_local, NOPE_DIM + ROPE_DIM)
    query_positions = (block_start + jnp.arange(block_rows, dtype=jnp.int32)).astype(jnp.float32)
    query_plain = query_full[..., :NOPE_DIM]
    query_turned = rotate_half(query_full[..., NOPE_DIM:], query_positions).astype(jnp.bfloat16)
    latent_normed = rms_scaled(key_latent, latent_gain).astype(jnp.bfloat16)
    own_positions = (own_start + jnp.arange(row_count, dtype=jnp.int32)).astype(jnp.float32)
    key_turned = rotate_half(rotary_key, own_positions).astype(jnp.bfloat16)
    running_max = jnp.full((block_rows, head_local), -1e30, jnp.float32)
    running_sum = jnp.zeros((block_rows, head_local), jnp.float32)
    weighted = jnp.zeros((block_rows, head_local, KVRANK), jnp.float32)
    latents = lax.all_gather(latent_normed, ("sp", "tp"), axis=0, tiled=True)
    turned_keys = lax.all_gather(key_turned, ("sp", "tp"), axis=0, tiled=True)
    portion_rows = latents.shape[0]
    step_rows = min(portion_rows, 2048)
    for begin in range(0, portion_rows, step_rows):
        latent_part = latents[begin : begin + step_rows]
        turned_part = turned_keys[begin : begin + step_rows]
        key_plain = jnp.dot(latent_part, key_up, preferred_element_type=jnp.float32).astype(
            jnp.bfloat16
        )
        key_plain = key_plain.reshape(latent_part.shape[0], head_local, NOPE_DIM)
        scores = jnp.einsum(
            "qhd,khd->qhk", query_plain, key_plain, preferred_element_type=jnp.float32
        )
        scores = scores + jnp.einsum(
            "qhd,kd->qhk", query_turned, turned_part, preferred_element_type=jnp.float32
        )
        scores = scores * score_scale
        new_max = jnp.maximum(running_max, jnp.max(scores, axis=-1))
        rescale = jnp.exp(running_max - new_max)
        expo = jnp.exp(scores - new_max[..., None])
        running_sum = running_sum * rescale + jnp.sum(expo, axis=-1)
        weighted = weighted * rescale[..., None] + jnp.einsum(
            "qhk,kc->qhc",
            expo.astype(jnp.bfloat16),
            latent_part,
            preferred_element_type=jnp.float32,
        )
        running_max = new_max
    final_state = (running_max, running_sum, weighted)
    running_max, running_sum, weighted = final_state
    latent_mix = (weighted / running_sum[..., None]).astype(jnp.bfloat16)
    value_heads = value_up.reshape(KVRANK, head_local, VALUE_DIM)
    head_out = jnp.einsum(
        "qhc,chd->qhd", latent_mix, value_heads, preferred_element_type=jnp.float32
    ).astype(jnp.bfloat16)
    head_out = head_out.reshape(block_rows, head_local * VALUE_DIM)
    widened = head_out.astype(jnp.float32)
    square_part = jnp.sum(widened * widened, axis=1)
    gained = (widened * out_gain).astype(jnp.bfloat16)
    all_gained, square_parts = (
        lax.all_gather(gained, "tp", axis=1, tiled=True),
        lax.all_gather(square_part[:, None].astype(jnp.bfloat16), "tp", axis=1, tiled=True).astype(
            jnp.float32
        ),
    )
    all_squares = jnp.sum(square_parts, axis=1)
    own_sums = jnp.dot(
        all_gained,
        lax.all_gather(out_weight, "sp", axis=0, tiled=True),
        preferred_element_type=jnp.float32,
    )
    mean_square = all_squares / (HEADS * VALUE_DIM)
    return (own_sums * lax.rsqrt(mean_square + norm_eps)[:, None]).astype(jnp.bfloat16)


LANES = 128
LINE = 4
TILES = 8
TAILS = (3, 1)
AT_EXIT = 2


def rope_table(tokens, width):
    half = width // 2
    inverse = np.float32(rope_theta) ** (-np.arange(half, dtype=np.float32) / np.float32(half))
    angles = np.arange(tokens, dtype=np.float32)[:, None] * inverse.astype(np.float32)[None, :]
    wide = angles.astype(np.float32).astype(np.float64)
    cosine, sine = np.cos(wide), np.sin(wide)
    return np.concatenate([cosine, cosine, -sine, sine], axis=1).astype(np.float32)


def turned(wide, table):
    width = wide.shape[-1]
    half = width // 2
    swapped = jnp.concatenate([wide[:, half:], wide[:, :half]], axis=1)
    return wide * table[:, :width] + swapped * table[:, width:]


def kernel(
    n_sp, n_tp,
    ql_hbm, kl, rk, qg_hbm, lg_hbm, og_hbm, table_hbm, qup, kup, vup, ow, out_hbm,
    ql, ql_outer, qg, lg, og, table,
    lat, wbuf, qbuf, kbuf, vbuf, latn, kturn, qfull, qfull_outer, qnorm, gall, squares, squares_outer, tally,
    acc, far_acc, asked,
    far_out, far_in, out,
    local, w_local, o_local, sends, l_recv, g_recv, w_recv, m_recv, q_recv, h_recv, f_recv,
):
    z, t, g = lax.axis_index("sp"), lax.axis_index("tp"), lax.axis_index("grp")
    parity = lax.rem(g, 2)
    partner = g + 1 - 2 * parity
    core = lax.rem(t, 2)
    sibling = t + 1 - 2 * core
    block_rows = ql.shape[0]
    depth = ow.shape[0]
    half = depth // 2
    tile = wbuf.shape[3]
    heads = kup.shape[1] // NOPE_DIM
    cols = heads * VALUE_DIM
    head_width = NOPE_DIM + ROPE_DIM
    rank = kl.shape[1]
    width = rk.shape[1]
    keys = n_sp * n_tp * kl.shape[0]

    lower = z < n_sp // 2
    toward = jnp.where(lower, 1, -1)
    centre = z + toward
    outer = z - toward
    beyond = centre + toward
    has_up, has_down = z < n_sp - 1, z > 0
    edge = jnp.logical_or(z == 0, z == n_sp - 1)
    inner = jnp.logical_not(edge)
    far_base = jnp.where(lower, n_tp // 2, 0)
    far_group = jnp.logical_and(t >= far_base, t < far_base + n_tp // 2)
    helps = jnp.logical_and(inner, far_group)
    helped = jnp.logical_and(edge, far_group)

    loads = [
        pltpu.make_async_copy(src, dst, local.at[i])
        for i, src, dst in (
            (0, kl, lat.at[z, t, :, pl.ds(0, rank)]),
            (0, rk, lat.at[z, t, :, pl.ds(rank, width)]),
            (1, ql_hbm, ql),
            (2, qg_hbm, qg),
            (2, qup, qbuf),
            (3, lg_hbm, lg),
            (3, table_hbm, table),
            (3, kup, kbuf),
            (3, vup, vbuf),
            (3, og_hbm, og),
        )
    ]
    def w_load(f):
        return pltpu.make_async_copy(
            ow.at[:, pl.ds(f * tile, tile)], wbuf.at[z, f], w_local.at[min(f, 1)]
        )

    for load in loads[:3]:
        load.start()
    w_load(0).start()
    for load in loads[3:5]:
        load.start()
    for f in range(1, TILES):
        w_load(f).start()
    for load in loads[5:]:
        load.start()

    barrier = pltpu.get_barrier_semaphore()

    @pl.when(has_up)
    def _():
        pl.semaphore_signal(barrier, inc=1, device_id={"sp": z + 1}, device_id_type=MESH)

    @pl.when(has_down)
    def _():
        pl.semaphore_signal(barrier, inc=1, device_id={"sp": z - 1}, device_id_type=MESH)

    pl.semaphore_signal(barrier, inc=1, device_id={"grp": partner}, device_id_type=MESH)
    for d in range(1, n_tp):
        pl.semaphore_signal(barrier, inc=1, device_id={"tp": lax.rem(t + d, n_tp)}, device_id_type=MESH)
    pl.semaphore_wait(barrier, n_tp + jnp.where(edge, 1, 2))

    def remote(src, dst, recv, target):
        return pltpu.make_async_remote_copy(
            src_ref=src, dst_ref=dst, send_sem=sends.at[0], recv_sem=recv,
            device_id=target, device_id_type=MESH,
        )

    opposite = lax.rem(t + n_tp // 2, n_tp)

    def drain(ref):
        remote(ref, ref, sends.at[0], {"tp": opposite}).wait_send()

    def expect(ref, recv):
        remote(ref, ref, recv, {"tp": opposite}).wait_recv()

    def part_along(b, up):
        return remote(lat.at[b, t], lat.at[b, t], l_recv.at[b], {"sp": z + 1 if up else z - 1})

    def part_across(b, d):
        return remote(lat.at[b, t], lat.at[b, t], l_recv.at[n_sp], {"tp": lax.rem(t + d, n_tp)})

    def spread(b):
        for d in range(1, n_tp):
            part_across(b, d).start()

    def arrive(d):
        @pl.when(z >= d)
        def _():
            part_along(z - d, 1).wait_recv()

            @pl.when(has_up)
            def _():
                part_along(z - d, 1).start()

            spread(z - d)

        @pl.when(z + d < n_sp)
        def _():
            part_along(z + d, 0).wait_recv()

            @pl.when(has_down)
            def _():
                part_along(z + d, 0).start()

            spread(z + d)

    FROM_OUTER = 0
    FROM_CENTRE, BEYOND_NEAR, BEYOND_FAR = (TILES // 2 + TILES * i for i in range(3))
    CENTRE_FAR, EARLY_TAIL, LATE_TAIL, REST = range(4)
    last = TILES - 1
    cut_most, cut_least = TILES - max(TAILS), TILES - min(TAILS)
    first_tail = [TILES - count for count in TAILS]

    def rows_of(b, p, f):
        return wbuf.at[b, f, pl.ds(pl.multiple_of(p * half, half), half)]

    def moved(ref, recv, target):
        return remote(ref, ref, recv, target)

    def inward(f):
        role = jnp.where(edge, FROM_OUTER + f // 2, FROM_CENTRE + f)
        return moved(rows_of(z, parity, f), w_recv.at[role], {"sp": centre})

    def outward(f):
        return moved(rows_of(z, parity, f), w_recv.at[FROM_CENTRE + f], {"sp": outer})

    def passed(f):
        return moved(rows_of(outer, parity, f), w_recv.at[BEYOND_NEAR + f], {"sp": centre})

    def inward_far(ref, part):
        return moved(ref, m_recv.at[part], {"sp": centre})

    def across(f):
        return moved(rows_of(centre, parity, f), m_recv.at[CENTRE_FAR], {"grp": partner})

    def across_beyond(f):
        return moved(rows_of(beyond, parity, f), w_recv.at[BEYOND_FAR + f], {"grp": partner})

    def pass_tail(f):
        return moved(rows_of(outer, 1 - parity, f), w_recv.at[BEYOND_FAR + f], {"sp": centre})

    def of_tiles(count):
        return wbuf.at[0, pl.ds(0, count), pl.ds(0, half)]

    def landed(role, f):
        expect(wbuf.at[0, f, pl.ds(0, half)], w_recv.at[role + f])

    def near(f):
        if f == 0:
            w_load(0).wait()
        if f == 1:
            rest = wbuf.at[z, pl.ds(1, last)]
            pltpu.make_async_copy(rest, rest, w_local.at[1]).wait()
        inward(f).start()

    def near_out(f):
        @pl.when(inner)
        def _():
            outward(f).start()

    def near_far():
        @pl.when(edge)
        def _():
            for f in range(cut_most, TILES):
                inward_far(rows_of(z, 1 - parity, f), EARLY_TAIL if f < cut_least else LATE_TAIL).start()
            for f in range(cut_most):
                inward_far(rows_of(z, 1 - parity, f), REST).start()

    def to_partner(f):
        landed(FROM_CENTRE, f)
        across(f).start()

    def inner_partner(some):
        @pl.when(inner)
        def _():
            for f in some:
                to_partner(f)

    def inner_pass(pair):
        @pl.when(inner)
        def _():
            expect(wbuf.at[0, pl.ds(0, 2), pl.ds(0, half)], w_recv.at[FROM_OUTER + pair])
            for f in (2 * pair, 2 * pair + 1):
                passed(f).start()

    def edge_partner(some):
        @pl.when(edge)
        def _():
            for f in some:
                to_partner(f)

    def second_hop(f):
        landed(BEYOND_NEAR, f)
        if f < cut_most:
            across_beyond(f).start()
        else:
            for c, first in enumerate(first_tail):
                if f < first:
                    @pl.when(core == c)
                    def _():
                        across_beyond(f).start()

    def tails(c):
        @pl.when(core == c)
        def _():
            if first_tail[c] == cut_most:
                expect(of_tiles(cut_least - cut_most), m_recv.at[EARLY_TAIL])
            expect(of_tiles(TILES - cut_least), m_recv.at[LATE_TAIL])
            for f in range(first_tail[c], TILES):
                pass_tail(f).start()

    def outer_rest():
        expect(of_tiles(cut_most), m_recv.at[REST])
        for c, first in enumerate(first_tail):
            if first != cut_most:
                @pl.when(core == c)
                def _():
                    expect(of_tiles(cut_least - cut_most), m_recv.at[EARLY_TAIL])

    def centre_far():
        expect(wbuf.at[0, :, pl.ds(0, half)], m_recv.at[CENTRE_FAR])

    def project(latent, full):
        wide = latent[...].astype(jnp.float32)
        mean = jnp.mean(wide * wide, axis=-1, keepdims=True)
        gain = jnp.concatenate([qg[i : i + 1] for i in range(qg.shape[0])], axis=1)
        qnorm[...] = (wide * lax.rsqrt(mean + norm_eps) * gain).astype(jnp.bfloat16)
        full[...] = jnp.dot(qnorm[...], qbuf[...], preferred_element_type=jnp.float32).astype(
            jnp.bfloat16
        )

    def lend():
        return remote(ql, ql_outer, h_recv.at[1], {"sp": centre})

    def queries():
        for load in loads[3:5]:
            load.wait()
        project(ql, qfull)

    def outer_queries():
        @pl.when(helps)
        def _():
            lend().wait_recv()
            project(ql_outer, qfull_outer)

    def latents():
        for load in loads[5:]:
            load.wait()
        expect(lat.at[:, pl.ds(0, n_tp - 1)], l_recv.at[n_sp])
        whole = lat[...].reshape(keys, rank + width)
        wide = whole[:, :rank].astype(jnp.float32)
        mean = jnp.mean(wide * wide, axis=-1, keepdims=True)
        latn[...] = (wide * lax.rsqrt(mean + norm_eps) * lg[...]).astype(jnp.bfloat16)
        spun = whole[:, rank:].astype(jnp.float32)
        kturn[...] = turned(spun, table[...]).astype(jnp.bfloat16)

    transposed = (((1,), (1,)), ((), ()))

    def attend_with(h, full, block, store, squares):
        start = h * head_width
        plain = full[:, start : start + NOPE_DIM]
        spun = full[:, start + NOPE_DIM : start + head_width].astype(jnp.float32)
        own = table[pl.ds(pl.multiple_of(block * block_rows, block_rows), block_rows), :]
        spun = turned(spun, own).astype(jnp.bfloat16)
        key_plain = jnp.dot(
            latn[...], kbuf[:, h * NOPE_DIM : (h + 1) * NOPE_DIM], preferred_element_type=jnp.float32
        ).astype(jnp.bfloat16)
        scores = lax.dot_general(plain, key_plain, transposed, preferred_element_type=jnp.float32)
        scores = scores + lax.dot_general(
            spun, kturn[...], transposed, preferred_element_type=jnp.float32
        )
        scores = scores * (head_width ** (-0.5))
        expo = jnp.exp(scores - jnp.max(scores, axis=-1, keepdims=True))
        total = jnp.sum(expo, axis=-1, keepdims=True)
        mix = jnp.dot(expo.astype(jnp.bfloat16), latn[...], preferred_element_type=jnp.float32)
        mix = (mix / total).astype(jnp.bfloat16)
        head_out = jnp.dot(
            mix, vbuf[:, h * VALUE_DIM : (h + 1) * VALUE_DIM], preferred_element_type=jnp.float32
        ).astype(jnp.bfloat16)
        wide = head_out.astype(jnp.float32)
        gained = wide * og[:, h * VALUE_DIM : (h + 1) * VALUE_DIM]
        store(gained.astype(jnp.bfloat16))
        square = jnp.sum(wide * wide, axis=-1, keepdims=True)
        if h:
            square = square + squares[:, :1]
        squares[...] = jnp.broadcast_to(square, squares.shape)

    def attend(h):
        def store(value):
            gall[t, :, h * VALUE_DIM : (h + 1) * VALUE_DIM] = value

        attend_with(h, qfull, z, store, squares)
        if h == heads - 1:
            gall[t, :, cols:] = squares[...].astype(jnp.bfloat16)

    def attend_outer(h):
        def store(value):
            asked[core, :, h * VALUE_DIM : (h + 1) * VALUE_DIM] = value

        attend_with(h, qfull_outer, outer, store, squares_outer)
        if h == heads - 1:
            tally[...] = squares_outer[...].astype(jnp.bfloat16)

    def is_near(p):
        return jnp.logical_or(p < far_base, p >= far_base + n_tp // 2)

    def share(h):
        @pl.when(jnp.logical_or(inner, is_near(t)) if h < heads else True)
        def _():
            for d in range(1, n_tp):
                part = gall.at[t, :, pl.ds(h * VALUE_DIM, VALUE_DIM)]
                kind = h // heads
                remote(part, part, g_recv.at[kind], {"tp": lax.rem(t + d, n_tp)}).start()

    def slabs(count, span):
        return gall.at[pl.ds(0, count), :, pl.ds(0, span)]

    def gather():
        for where, count in (
            (inner, n_tp - 1),
            (jnp.logical_and(edge, is_near(t)), n_tp // 2 - 1),
            (helped, n_tp // 2),
        ):
            @pl.when(where)
            def _():
                expect(slabs(count, cols), g_recv.at[0])

        expect(slabs(n_tp - 1, VALUE_DIM), g_recv.at[1])

    def ask(h):
        part = asked.at[core, :, pl.ds(h * VALUE_DIM, VALUE_DIM)]
        return remote(part, part, q_recv.at[0], {"tp": opposite})

    def tell():
        return remote(tally, gall.at[t, :, pl.ds(cols, VALUE_DIM)], h_recv.at[2], {"sp": outer})

    def hand(c):
        return remote(asked.at[c], asked.at[c], h_recv.at[0], {"tp": sibling})

    def hand_on():
        @pl.when(jnp.logical_not(helps))
        def _():
            expect(asked.at[0], q_recv.at[0])

        hand(core).start()

    def heard():
        hand(1 - core).wait_recv()

    groups = (tuple(range(last - 3)), (last - 3, last - 2), (last - 1,), (last,))

    def answer(f):
        n = [f in some for some in groups].index(True)
        return remote(far_out.at[f], far_in.at[f], f_recv.at[n], {"sp": outer})

    def wide_of(b, some):
        return jnp.concatenate([wbuf[b, f] for f in some], axis=1)

    def dot(lhs, b, some):
        return jnp.dot(lhs, wide_of(b, some), preferred_element_type=jnp.float32)

    def gained(b):
        return gall[b, :, :cols]

    def keep(some, total, fresh=False):
        for n, f in enumerate(some):
            part = total[:, n * tile : (n + 1) * tile]
            acc[f] = part if fresh else acc[f] + part

    def stored(f):
        return pltpu.make_async_copy(out.at[f], out_hbm.at[:, pl.ds(f * tile, tile)], o_local.at[0])

    def set_scale():
        square = gall[0, :, cols : cols + 1].astype(jnp.float32)
        for p in range(1, n_tp):
            square = square + gall[p, :, cols : cols + 1].astype(jnp.float32)
        squares[...] = jnp.broadcast_to(lax.rsqrt(square / (n_tp * cols) + norm_eps), squares.shape)

    def put(f, total):
        out[f] = (total * squares[...]).astype(out.dtype)
        stored(f).start()

    def run(call, some):
        for i in some:
            call(i)

    tiles = range(TILES)
    late = TILES - far_acc.shape[0]
    pairs = [(f, f + 1) for f in range(0, TILES, 2)]

    loads[0].wait()
    loads[1].wait()

    @pl.when(has_up)
    def _():
        part_along(z, 1).start()

    @pl.when(has_down)
    def _():
        part_along(z, 0).start()

    spread(z)
    loads[2].wait()

    @pl.when(helped)
    def _():
        lend().start()

    run(near, range(AT_EXIT))
    queries()
    arrive(1)
    run(near, range(AT_EXIT, TILES))
    run(near_out, range(2))
    inner_partner(range(2))
    arrive(2)
    run(near_out, range(2, TILES))
    inner_partner(range(2, 3))
    arrive(3)
    near_far()
    outer_queries()
    inner_partner(range(3, 4))
    latents()
    inner_partner(range(4, 5))
    inner_pass(0)

    @pl.when(helps)
    def _():
        attend_outer(0)
        run(to_partner, range(5, 6))
        attend_outer(1)
        ask(0).start()
        inner_pass(1)
        run(to_partner, range(6, 7))
        attend_outer(2)
        ask(1).start()
        run(to_partner, range(7, TILES))
        attend_outer(3)
        ask(2).start()
        inner_pass(2)
        ask(3).start()
        tell().start()
        attend(0)
        hand_on()
        run(second_hop, range(1))
        attend(1)
        share(0)
        attend(2)
        share(1)
        inner_pass(3)
        run(second_hop, range(1, 2))
        attend(3)
        share(2)
        run(second_hop, range(2, 3))
        share(3)

    @pl.when(is_near(t))
    def _():
        attend(0)
        inner_partner(range(5, 6))
        inner_pass(1)
        edge_partner(range(5))
        attend(1)
        share(0)
        edge_partner(range(5, 6))
        attend(2)
        share(1)
        inner_partner(range(6, TILES))
        inner_pass(2)
        edge_partner(range(6, 7))
        attend(3)
        share(2)
        inner_pass(3)
        edge_partner(range(7, TILES))
        share(3)

        @pl.when(inner)
        def _():
            run(second_hop, range(2))
            hand_on()
            run(second_hop, range(2, 3))

    @pl.when(helped)
    def _():
        run(to_partner, tiles)
        tell().wait_recv()

    share(heads)

    @pl.when(edge)
    def _():
        gather()
        set_scale()
        for some in pairs:
            keep(some, dot(gained(z), z, some), fresh=True)
        centre_far()
        for some in pairs:
            keep(some, dot(gained(centre), centre, some))
        for n, some in enumerate(groups):
            expect(far_in.at[pl.ds(0, len(some))], f_recv.at[n])
            for f in some:
                put(f, acc[f] + far_in[f].astype(jnp.float32))

    def part_of(p):
        return pl.ds(pl.multiple_of(p * half, half), half)

    def half_dot(f, p):
        return jnp.dot(
            asked[beyond - far_base, :, part_of(p)], wbuf[beyond, f, part_of(p)],
            preferred_element_type=jnp.float32,
        )

    def prepare(f):
        far_acc[f - late] = half_dot(f, parity) + dot(asked[centre - far_base], centre, (f,))

    def reply(f):
        landed(BEYOND_FAR, f)
        if f < late:
            far = dot(asked[beyond - far_base], beyond, (f,)) + dot(asked[centre - far_base], centre, (f,))
        else:
            far = far_acc[f - late] + half_dot(f, 1 - parity)
        far_out[f] = far.astype(far_out.dtype)
        answer(f).start()

    def own(some):
        keep(some, dot(gained(z), z, some) + dot(gained(centre), centre, some), fresh=True)

    @pl.when(inner)
    def _():
        tails(0)
        run(second_hop, range(3, 4))
        heard()
        centre_far()
        reply(0)
        run(second_hop, range(4, 5))
        reply(1)
        run(second_hop, range(5, 6))
        reply(2)
        tails(1)
        run(second_hop, range(6, 7))
        run(prepare, range(late, late + 1))
        reply(3)
        run(second_hop, range(7, 8))
        run(prepare, range(late + 1, TILES))
        run(reply, range(4, TILES))
        gather()
        set_scale()
        run(own, pairs)
        outer_rest()
        for some in pairs:
            total = dot(gained(outer), outer, some) + dot(gained(beyond), beyond, some)
            for n, f in enumerate(some):
                put(f, acc[f] + total[:, n * tile : (n + 1) * tile])

    halves = wbuf.at[0, :, pl.ds(0, half)]
    drain(lat.at[:, pl.ds(0, n_tp - 1)])
    drain(slabs(n_tp - 1, VALUE_DIM))
    for _ in range(2):
        drain(halves)

    @pl.when(jnp.logical_or(inner, is_near(t)))
    def _():
        drain(slabs(n_tp - 1, cols))

    @pl.when(edge)
    def _():
        drain(lat.at[0, pl.ds(0, 1)])
        drain(halves)

    @pl.when(helped)
    def _():
        drain(ql)

    @pl.when(helps)
    def _():
        drain(asked.at[0])
        drain(tally)

    @pl.when(inner)
    def _():
        for count in (2, 3):
            drain(lat.at[0, pl.ds(0, count)])
        for _ in range(3):
            drain(halves)
        drain(asked.at[0])
        drain(far_out)

    pltpu.make_async_copy(out, out, o_local.at[0]).wait()


MESH = pl.DeviceIdType.MESH


def on_device_fused(
    n_sp, n_tp,
    query_latent, key_latent, rotary_key, query_gain, latent_gain,
    query_up, key_up, value_up, out_gain, out_weight,
):
    block_rows, row_count = query_latent.shape[0], key_latent.shape[0]
    rank, width = key_latent.shape[1], rotary_key.shape[1]
    keys = n_sp * n_tp * row_count
    depth, features = out_weight.shape
    cols = value_up.shape[1]
    vmem, bf16, dma = pltpu.VMEM, jnp.bfloat16, pltpu.SemaphoreType.DMA
    table = jnp.asarray(rope_table(keys, width))
    tiled = (TILES, block_rows, features // TILES)
    in_hbm = pl.BlockSpec(memory_space=pl.ANY)
    return pl.pallas_call(
        functools.partial(kernel, n_sp, n_tp),
        out_shape=jax.ShapeDtypeStruct((block_rows, features), bf16),
        in_specs=[in_hbm] * 11,
        out_specs=in_hbm,
        scratch_shapes=[
            vmem(query_latent.shape, bf16),
            vmem(query_latent.shape, bf16),
            vmem((query_gain.shape[0] // LANES, LANES), jnp.float32),
            vmem((1, rank), jnp.float32),
            vmem((1, cols), jnp.float32),
            vmem(table.shape, jnp.float32),
            vmem((n_sp, n_tp, row_count, rank + width), bf16),
            vmem((n_sp, TILES, depth, features // TILES), bf16),
            vmem(query_up.shape, bf16),
            vmem(key_up.shape, bf16),
            vmem(value_up.shape, bf16),
            vmem((keys, rank), bf16),
            vmem((keys, width), bf16),
            vmem((block_rows, query_up.shape[1]), bf16),
            vmem((block_rows, query_up.shape[1]), bf16),
            vmem(query_latent.shape, bf16),
            vmem((n_tp, block_rows, cols + VALUE_DIM), bf16),
            vmem((block_rows, VALUE_DIM), jnp.float32),
            vmem((block_rows, VALUE_DIM), jnp.float32),
            vmem((block_rows, VALUE_DIM), bf16),
            vmem(tiled, jnp.float32),
            vmem((max(TAILS), *tiled[1:]), jnp.float32),
            vmem((n_tp // 2, block_rows, cols), bf16),
            vmem(tiled, bf16),
            vmem(tiled, bf16),
            vmem(tiled, bf16),
            dma((4,)),
            dma((2,)),
            dma((1,)),
            dma((1,)),
            dma((n_sp + 1,)),
            dma((2,)),
            dma((TILES // 2 + 3 * TILES,)),
            dma((4,)),
            dma((1,)),
            dma((3,)),
            dma((4,)),
        ],
        compiler_params=pltpu.CompilerParams(
            collective_id=0, has_side_effects=True
        ),
    )(
        query_latent, key_latent, rotary_key, query_gain.reshape(-1, LANES), latent_gain[None], out_gain[None],
        table, query_up, key_up, value_up, out_weight,
    )


def fits_fused(mesh):
    n_grp, n_sp, n_tp = (mesh.shape[name] for name in ("grp", "sp", "tp"))
    return n_grp % 2 == 0 and n_sp == LINE and n_sp == n_tp


def solution(mesh):
    in_specs = (
        P(("grp", "sp"), None),
        P(("grp", "sp", "tp"), None),
        P(("grp", "sp", "tp"), None),
        P(),
        P(),
        P(None, "tp"),
        P(None, "tp"),
        P(None, "tp"),
        P("tp"),
        P("sp", "tp"),
    )
    out_specs = P(("grp", "sp"), "tp")
    step = on_device
    if fits_fused(mesh):
        step = functools.partial(on_device_fused, mesh.shape["sp"], mesh.shape["tp"])
    return jax.shard_map(
        step, mesh=mesh, in_specs=in_specs, out_specs=out_specs, check_vma=False
    )
```

```python
import functools

import jax
import jax.numpy as jnp
import numpy as np
from jax import lax
from jax.experimental import pallas as pl
from jax.experimental.pallas import tpu as pltpu
from jax.sharding import PartitionSpec as P

HEADS = 16
NOPE_DIM = 128
ROPE_DIM = 64
VALUE_DIM = 128
KVRANK = 256


norm_eps = 1e-06
rope_theta = 10000.0


def rms_scaled(inputs, gain_vec):
    widened = inputs.astype(jnp.float32)
    return (
        widened
        * lax.rsqrt(jnp.mean(widened * widened, axis=-1, keepdims=True) + norm_eps)
        * gain_vec
    )


def rotate_half(inputs, positions):
    half_width = inputs.shape[-1] // 2
    inverse = rope_theta ** (-jnp.arange(half_width, dtype=jnp.float32) / half_width)
    angles = positions[:, None] * inverse[None, :]
    if inputs.ndim == 3:
        angles = angles[:, None, :]
    cosine = jnp.cos(angles)
    sine = jnp.sin(angles)
    widened = inputs.astype(jnp.float32)
    first = widened[..., :half_width]
    second = widened[..., half_width:]
    return jnp.concatenate(
        [first * cosine - second * sine, second * cosine + first * sine], axis=-1
    )


def on_device(
    query_latent,
    key_latent,
    rotary_key,
    query_gain,
    latent_gain,
    query_up,
    key_up,
    value_up,
    out_gain,
    out_weight,
):
    block_rows = query_latent.shape[0]
    row_count = key_latent.shape[0]
    head_local = key_up.shape[1] // NOPE_DIM
    block_start = lax.axis_index("sp") * block_rows
    own_start = block_start + lax.axis_index("tp") * row_count
    score_scale = (NOPE_DIM + ROPE_DIM) ** (-0.5)
    normed = rms_scaled(query_latent, query_gain).astype(jnp.bfloat16)
    query_full = jnp.dot(normed, query_up, preferred_element_type=jnp.float32).astype(jnp.bfloat16)
    query_full = query_full.reshape(block_rows, head_local, NOPE_DIM + ROPE_DIM)
    query_positions = (block_start + jnp.arange(block_rows, dtype=jnp.int32)).astype(jnp.float32)
    query_plain = query_full[..., :NOPE_DIM]
    query_turned = rotate_half(query_full[..., NOPE_DIM:], query_positions).astype(jnp.bfloat16)
    latent_normed = rms_scaled(key_latent, latent_gain).astype(jnp.bfloat16)
    own_positions = (own_start + jnp.arange(row_count, dtype=jnp.int32)).astype(jnp.float32)
    key_turned = rotate_half(rotary_key, own_positions).astype(jnp.bfloat16)
    running_max = jnp.full((block_rows, head_local), -1e30, jnp.float32)
    running_sum = jnp.zeros((block_rows, head_local), jnp.float32)
    weighted = jnp.zeros((block_rows, head_local, KVRANK), jnp.float32)
    latents = lax.all_gather(latent_normed, ("sp", "tp"), axis=0, tiled=True)
    turned_keys = lax.all_gather(key_turned, ("sp", "tp"), axis=0, tiled=True)
    portion_rows = latents.shape[0]
    step_rows = min(portion_rows, 2048)
    for begin in range(0, portion_rows, step_rows):
        latent_part = latents[begin : begin + step_rows]
        turned_part = turned_keys[begin : begin + step_rows]
        key_plain = jnp.dot(latent_part, key_up, preferred_element_type=jnp.float32).astype(
            jnp.bfloat16
        )
        key_plain = key_plain.reshape(latent_part.shape[0], head_local, NOPE_DIM)
        scores = jnp.einsum(
            "qhd,khd->qhk", query_plain, key_plain, preferred_element_type=jnp.float32
        )
        scores = scores + jnp.einsum(
            "qhd,kd->qhk", query_turned, turned_part, preferred_element_type=jnp.float32
        )
        scores = scores * score_scale
        new_max = jnp.maximum(running_max, jnp.max(scores, axis=-1))
        rescale = jnp.exp(running_max - new_max)
        expo = jnp.exp(scores - new_max[..., None])
        running_sum = running_sum * rescale + jnp.sum(expo, axis=-1)
        weighted = weighted * rescale[..., None] + jnp.einsum(
            "qhk,kc->qhc",
            expo.astype(jnp.bfloat16),
            latent_part,
            preferred_element_type=jnp.float32,
        )
        running_max = new_max
    final_state = (running_max, running_sum, weighted)
    running_max, running_sum, weighted = final_state
    latent_mix = (weighted / running_sum[..., None]).astype(jnp.bfloat16)
    value_heads = value_up.reshape(KVRANK, head_local, VALUE_DIM)
    head_out = jnp.einsum(
        "qhc,chd->qhd", latent_mix, value_heads, preferred_element_type=jnp.float32
    ).astype(jnp.bfloat16)
    head_out = head_out.reshape(block_rows, head_local * VALUE_DIM)
    widened = head_out.astype(jnp.float32)
    square_part = jnp.sum(widened * widened, axis=1)
    gained = (widened * out_gain).astype(jnp.bfloat16)
    all_gained, square_parts = (
        lax.all_gather(gained, "tp", axis=1, tiled=True),
        lax.all_gather(square_part[:, None].astype(jnp.bfloat16), "tp", axis=1, tiled=True).astype(
            jnp.float32
        ),
    )
    all_squares = jnp.sum(square_parts, axis=1)
    own_sums = jnp.dot(
        all_gained,
        lax.all_gather(out_weight, "sp", axis=0, tiled=True),
        preferred_element_type=jnp.float32,
    )
    mean_square = all_squares / (HEADS * VALUE_DIM)
    return (own_sums * lax.rsqrt(mean_square + norm_eps)[:, None]).astype(jnp.bfloat16)


LANES = 128
LINE = 4
TILES = 8
TAILS = (3, 1)
AT_EXIT = 2


def rope_table(tokens, width):
    half = width // 2
    inverse = np.float32(rope_theta) ** (-np.arange(half, dtype=np.float32) / np.float32(half))
    angles = np.arange(tokens, dtype=np.float32)[:, None] * inverse.astype(np.float32)[None, :]
    wide = angles.astype(np.float32).astype(np.float64)
    cosine, sine = np.cos(wide), np.sin(wide)
    return np.concatenate([cosine, cosine, -sine, sine], axis=1).astype(np.float32)


def turned(wide, table):
    width = wide.shape[-1]
    half = width // 2
    swapped = jnp.concatenate([wide[:, half:], wide[:, :half]], axis=1)
    return wide * table[:, :width] + swapped * table[:, width:]


def kernel(
    n_sp, n_tp,
    ql_hbm, kl, rk, qg_hbm, lg_hbm, og_hbm, table_hbm, qup, kup, vup, ow, out,
    ql, ql_outer, qg, lg, og, table,
    lat, wbuf, qbuf, kbuf, vbuf, latn, kturn, qfull, qfull_outer, qnorm, gall, squares, squares_outer, tally,
    acc, far_acc, asked,
    far_out, far_in,
    local, w_local, sends, l_recv, g_recv, w_recv, m_recv, q_recv, h_recv, f_recv,
):
    z, t, g = lax.axis_index("sp"), lax.axis_index("tp"), lax.axis_index("grp")
    parity = lax.rem(g, 2)
    partner = g + 1 - 2 * parity
    core = lax.rem(t, 2)
    sibling = t + 1 - 2 * core
    block_rows = ql.shape[0]
    depth = ow.shape[0]
    half = depth // 2
    tile = wbuf.shape[3]
    heads = kup.shape[1] // NOPE_DIM
    cols = heads * VALUE_DIM
    head_width = NOPE_DIM + ROPE_DIM
    rank = kl.shape[1]
    width = rk.shape[1]
    keys = n_sp * n_tp * kl.shape[0]

    lower = z < n_sp // 2
    toward = jnp.where(lower, 1, -1)
    centre = z + toward
    outer = z - toward
    beyond = centre + toward
    has_up, has_down = z < n_sp - 1, z > 0
    edge = jnp.logical_or(z == 0, z == n_sp - 1)
    inner = jnp.logical_not(edge)
    far_base = jnp.where(lower, n_tp // 2, 0)
    far_group = jnp.logical_and(t >= far_base, t < far_base + n_tp // 2)
    helps = jnp.logical_and(inner, far_group)
    helped = jnp.logical_and(edge, far_group)

    loads = [
        pltpu.make_async_copy(src, dst, local.at[i])
        for i, src, dst in (
            (0, kl, lat.at[z, t, :, pl.ds(0, rank)]),
            (0, rk, lat.at[z, t, :, pl.ds(rank, width)]),
            (1, ql_hbm, ql),
            (2, qg_hbm, qg),
            (2, qup, qbuf),
            (3, lg_hbm, lg),
            (3, table_hbm, table),
            (3, kup, kbuf),
            (3, vup, vbuf),
            (3, og_hbm, og),
        )
    ]
    def w_load(f):
        return pltpu.make_async_copy(
            ow.at[:, pl.ds(f * tile, tile)], wbuf.at[z, f], w_local.at[min(f, 1)]
        )

    for load in loads[:3]:
        load.start()
    w_load(0).start()
    for load in loads[3:5]:
        load.start()
    for f in range(1, TILES):
        w_load(f).start()
    for load in loads[5:]:
        load.start()

    barrier = pltpu.get_barrier_semaphore()

    @pl.when(has_up)
    def _():
        pl.semaphore_signal(barrier, inc=1, device_id={"sp": z + 1}, device_id_type=MESH)

    @pl.when(has_down)
    def _():
        pl.semaphore_signal(barrier, inc=1, device_id={"sp": z - 1}, device_id_type=MESH)

    pl.semaphore_signal(barrier, inc=1, device_id={"grp": partner}, device_id_type=MESH)
    for d in range(1, n_tp):
        pl.semaphore_signal(barrier, inc=1, device_id={"tp": lax.rem(t + d, n_tp)}, device_id_type=MESH)
    pl.semaphore_wait(barrier, n_tp + jnp.where(edge, 1, 2))

    def remote(src, dst, recv, target):
        return pltpu.make_async_remote_copy(
            src_ref=src, dst_ref=dst, send_sem=sends.at[0], recv_sem=recv,
            device_id=target, device_id_type=MESH,
        )

    opposite = lax.rem(t + n_tp // 2, n_tp)

    def drain(ref):
        remote(ref, ref, sends.at[0], {"tp": opposite}).wait_send()

    def expect(ref, recv):
        remote(ref, ref, recv, {"tp": opposite}).wait_recv()

    def part_along(b, up):
        return remote(lat.at[b, t], lat.at[b, t], l_recv.at[b], {"sp": z + 1 if up else z - 1})

    def part_across(b, d):
        return remote(lat.at[b, t], lat.at[b, t], l_recv.at[n_sp], {"tp": lax.rem(t + d, n_tp)})

    def spread(b):
        for d in range(1, n_tp):
            part_across(b, d).start()

    def arrive(d):
        @pl.when(z >= d)
        def _():
            part_along(z - d, 1).wait_recv()

            @pl.when(has_up)
            def _():
                part_along(z - d, 1).start()

            spread(z - d)

        @pl.when(z + d < n_sp)
        def _():
            part_along(z + d, 0).wait_recv()

            @pl.when(has_down)
            def _():
                part_along(z + d, 0).start()

            spread(z + d)

    FROM_OUTER = 0
    FROM_CENTRE, BEYOND_NEAR, BEYOND_FAR = (TILES // 2 + TILES * i for i in range(3))
    CENTRE_FAR, EARLY_TAIL, LATE_TAIL, REST = range(4)
    last = TILES - 1
    cut_most, cut_least = TILES - max(TAILS), TILES - min(TAILS)
    first_tail = [TILES - count for count in TAILS]

    def rows_of(b, p, f):
        return wbuf.at[b, f, pl.ds(pl.multiple_of(p * half, half), half)]

    def moved(ref, recv, target):
        return remote(ref, ref, recv, target)

    def inward(f):
        role = jnp.where(edge, FROM_OUTER + f // 2, FROM_CENTRE + f)
        return moved(rows_of(z, parity, f), w_recv.at[role], {"sp": centre})

    def outward(f):
        return moved(rows_of(z, parity, f), w_recv.at[FROM_CENTRE + f], {"sp": outer})

    def passed(f):
        return moved(rows_of(outer, parity, f), w_recv.at[BEYOND_NEAR + f], {"sp": centre})

    def inward_far(ref, part):
        return moved(ref, m_recv.at[part], {"sp": centre})

    def across(f):
        return moved(rows_of(centre, parity, f), m_recv.at[CENTRE_FAR], {"grp": partner})

    def across_beyond(f):
        return moved(rows_of(beyond, parity, f), w_recv.at[BEYOND_FAR + f], {"grp": partner})

    def pass_tail(f):
        return moved(rows_of(outer, 1 - parity, f), w_recv.at[BEYOND_FAR + f], {"sp": centre})

    def of_tiles(count):
        return wbuf.at[0, pl.ds(0, count), pl.ds(0, half)]

    def landed(role, f):
        expect(wbuf.at[0, f, pl.ds(0, half)], w_recv.at[role + f])

    def near(f):
        if f == 0:
            w_load(0).wait()
        if f == 1:
            rest = wbuf.at[z, pl.ds(1, last)]
            pltpu.make_async_copy(rest, rest, w_local.at[1]).wait()
        inward(f).start()

    def near_out(f):
        @pl.when(inner)
        def _():
            outward(f).start()

    def near_far():
        @pl.when(edge)
        def _():
            for f in range(cut_most, TILES):
                inward_far(rows_of(z, 1 - parity, f), EARLY_TAIL if f < cut_least else LATE_TAIL).start()
            for f in range(cut_most):
                inward_far(rows_of(z, 1 - parity, f), REST).start()

    def to_partner(f):
        landed(FROM_CENTRE, f)
        across(f).start()

    def inner_partner(some):
        @pl.when(inner)
        def _():
            for f in some:
                to_partner(f)

    def inner_pass(pair):
        @pl.when(inner)
        def _():
            expect(wbuf.at[0, pl.ds(0, 2), pl.ds(0, half)], w_recv.at[FROM_OUTER + pair])
            for f in (2 * pair, 2 * pair + 1):
                passed(f).start()

    def edge_partner(some):
        @pl.when(edge)
        def _():
            for f in some:
                to_partner(f)

    def second_hop(f):
        landed(BEYOND_NEAR, f)
        if f < cut_most:
            across_beyond(f).start()
        else:
            for c, first in enumerate(first_tail):
                if f < first:
                    @pl.when(core == c)
                    def _():
                        across_beyond(f).start()

    def tails(c):
        @pl.when(core == c)
        def _():
            if first_tail[c] == cut_most:
                expect(of_tiles(cut_least - cut_most), m_recv.at[EARLY_TAIL])
            expect(of_tiles(TILES - cut_least), m_recv.at[LATE_TAIL])
            for f in range(first_tail[c], TILES):
                pass_tail(f).start()

    def outer_rest():
        expect(of_tiles(cut_most), m_recv.at[REST])
        for c, first in enumerate(first_tail):
            if first != cut_most:
                @pl.when(core == c)
                def _():
                    expect(of_tiles(cut_least - cut_most), m_recv.at[EARLY_TAIL])

    def centre_far():
        expect(wbuf.at[0, :, pl.ds(0, half)], m_recv.at[CENTRE_FAR])

    def project(latent, full):
        wide = latent[...].astype(jnp.float32)
        mean = jnp.mean(wide * wide, axis=-1, keepdims=True)
        gain = jnp.concatenate([qg[i : i + 1] for i in range(qg.shape[0])], axis=1)
        qnorm[...] = (wide * lax.rsqrt(mean + norm_eps) * gain).astype(jnp.bfloat16)
        full[...] = jnp.dot(qnorm[...], qbuf[...], preferred_element_type=jnp.float32).astype(
            jnp.bfloat16
        )

    def lend():
        return remote(ql, ql_outer, h_recv.at[1], {"sp": centre})

    def queries():
        for load in loads[3:5]:
            load.wait()
        project(ql, qfull)

    def outer_queries():
        @pl.when(helps)
        def _():
            lend().wait_recv()
            project(ql_outer, qfull_outer)

    def latents():
        for load in loads[5:]:
            load.wait()
        expect(lat.at[:, pl.ds(0, n_tp - 1)], l_recv.at[n_sp])
        whole = lat[...].reshape(keys, rank + width)
        wide = whole[:, :rank].astype(jnp.float32)
        mean = jnp.mean(wide * wide, axis=-1, keepdims=True)
        latn[...] = (wide * lax.rsqrt(mean + norm_eps) * lg[...]).astype(jnp.bfloat16)
        spun = whole[:, rank:].astype(jnp.float32)
        kturn[...] = turned(spun, table[...]).astype(jnp.bfloat16)

    transposed = (((1,), (1,)), ((), ()))

    def attend_with(h, full, block, store, squares):
        start = h * head_width
        plain = full[:, start : start + NOPE_DIM]
        spun = full[:, start + NOPE_DIM : start + head_width].astype(jnp.float32)
        own = table[pl.ds(pl.multiple_of(block * block_rows, block_rows), block_rows), :]
        spun = turned(spun, own).astype(jnp.bfloat16)
        key_plain = jnp.dot(
            latn[...], kbuf[:, h * NOPE_DIM : (h + 1) * NOPE_DIM], preferred_element_type=jnp.float32
        ).astype(jnp.bfloat16)
        scores = lax.dot_general(plain, key_plain, transposed, preferred_element_type=jnp.float32)
        scores = scores + lax.dot_general(
            spun, kturn[...], transposed, preferred_element_type=jnp.float32
        )
        scores = scores * (head_width ** (-0.5))
        expo = jnp.exp(scores - jnp.max(scores, axis=-1, keepdims=True))
        total = jnp.sum(expo, axis=-1, keepdims=True)
        mix = jnp.dot(expo.astype(jnp.bfloat16), latn[...], preferred_element_type=jnp.float32)
        mix = (mix / total).astype(jnp.bfloat16)
        head_out = jnp.dot(
            mix, vbuf[:, h * VALUE_DIM : (h + 1) * VALUE_DIM], preferred_element_type=jnp.float32
        ).astype(jnp.bfloat16)
        wide = head_out.astype(jnp.float32)
        gained = wide * og[:, h * VALUE_DIM : (h + 1) * VALUE_DIM]
        store(gained.astype(jnp.bfloat16))
        square = jnp.sum(wide * wide, axis=-1, keepdims=True)
        if h:
            square = square + squares[:, :1]
        squares[...] = jnp.broadcast_to(square, squares.shape)

    def attend(h):
        def store(value):
            gall[t, :, h * VALUE_DIM : (h + 1) * VALUE_DIM] = value

        attend_with(h, qfull, z, store, squares)
        if h == heads - 1:
            gall[t, :, cols:] = squares[...].astype(jnp.bfloat16)

    def attend_outer(h):
        def store(value):
            asked[core, :, h * VALUE_DIM : (h + 1) * VALUE_DIM] = value

        attend_with(h, qfull_outer, outer, store, squares_outer)
        if h == heads - 1:
            tally[...] = squares_outer[...].astype(jnp.bfloat16)

    def is_near(p):
        return jnp.logical_or(p < far_base, p >= far_base + n_tp // 2)

    def share(h):
        @pl.when(jnp.logical_or(inner, is_near(t)) if h < heads else True)
        def _():
            for d in range(1, n_tp):
                part = gall.at[t, :, pl.ds(h * VALUE_DIM, VALUE_DIM)]
                kind = h // heads
                remote(part, part, g_recv.at[kind], {"tp": lax.rem(t + d, n_tp)}).start()

    def slabs(count, span):
        return gall.at[pl.ds(0, count), :, pl.ds(0, span)]

    def gather():
        for where, count in (
            (inner, n_tp - 1),
            (jnp.logical_and(edge, is_near(t)), n_tp // 2 - 1),
            (helped, n_tp // 2),
        ):
            @pl.when(where)
            def _():
                expect(slabs(count, cols), g_recv.at[0])

        expect(slabs(n_tp - 1, VALUE_DIM), g_recv.at[1])

    def ask(h):
        part = asked.at[core, :, pl.ds(h * VALUE_DIM, VALUE_DIM)]
        return remote(part, part, q_recv.at[0], {"tp": opposite})

    def tell():
        return remote(tally, gall.at[t, :, pl.ds(cols, VALUE_DIM)], h_recv.at[2], {"sp": outer})

    def hand(c):
        return remote(asked.at[c], asked.at[c], h_recv.at[0], {"tp": sibling})

    def hand_on():
        @pl.when(jnp.logical_not(helps))
        def _():
            expect(asked.at[0], q_recv.at[0])

        hand(core).start()

    def heard():
        hand(1 - core).wait_recv()

    groups = (tuple(range(last - 3)), (last - 3, last - 2), (last - 1,), (last,))

    def answer(f):
        n = [f in some for some in groups].index(True)
        return remote(far_out.at[f], far_in.at[f], f_recv.at[n], {"sp": outer})

    def wide_of(b, some):
        return jnp.concatenate([wbuf[b, f] for f in some], axis=1)

    def dot(lhs, b, some):
        return jnp.dot(lhs, wide_of(b, some), preferred_element_type=jnp.float32)

    def gained(b):
        return gall[b, :, :cols]

    def keep(some, total, fresh=False):
        for n, f in enumerate(some):
            part = total[:, n * tile : (n + 1) * tile]
            acc[f] = part if fresh else acc[f] + part

    def set_scale():
        square = gall[0, :, cols : cols + 1].astype(jnp.float32)
        for p in range(1, n_tp):
            square = square + gall[p, :, cols : cols + 1].astype(jnp.float32)
        squares[...] = jnp.broadcast_to(lax.rsqrt(square / (n_tp * cols) + norm_eps), squares.shape)

    def put(f, total):
        out[:, f * tile : (f + 1) * tile] = (total * squares[...]).astype(out.dtype)

    def run(call, some):
        for i in some:
            call(i)

    tiles = range(TILES)
    late = TILES - far_acc.shape[0]
    pairs = [(f, f + 1) for f in range(0, TILES, 2)]

    loads[0].wait()
    loads[1].wait()

    @pl.when(has_up)
    def _():
        part_along(z, 1).start()

    @pl.when(has_down)
    def _():
        part_along(z, 0).start()

    spread(z)
    loads[2].wait()

    @pl.when(helped)
    def _():
        lend().start()

    run(near, range(AT_EXIT))
    queries()
    arrive(1)
    run(near, range(AT_EXIT, TILES))
    run(near_out, range(2))
    inner_partner(range(2))
    arrive(2)
    run(near_out, range(2, TILES))
    inner_partner(range(2, 3))
    arrive(3)
    near_far()
    outer_queries()
    inner_partner(range(3, 4))
    latents()
    inner_partner(range(4, 5))
    inner_pass(0)

    @pl.when(helps)
    def _():
        attend_outer(0)
        run(to_partner, range(5, 6))
        attend_outer(1)
        ask(0).start()
        inner_pass(1)
        run(to_partner, range(6, 7))
        attend_outer(2)
        ask(1).start()
        run(to_partner, range(7, TILES))
        attend_outer(3)
        ask(2).start()
        inner_pass(2)
        ask(3).start()
        tell().start()
        attend(0)
        hand_on()
        run(second_hop, range(1))
        attend(1)
        share(0)
        attend(2)
        share(1)
        inner_pass(3)
        run(second_hop, range(1, 2))
        attend(3)
        share(2)
        run(second_hop, range(2, 3))
        share(3)

    @pl.when(is_near(t))
    def _():
        attend(0)
        inner_partner(range(5, 6))
        inner_pass(1)
        edge_partner(range(5))
        attend(1)
        share(0)
        edge_partner(range(5, 6))
        attend(2)
        share(1)
        inner_partner(range(6, TILES))
        inner_pass(2)
        edge_partner(range(6, 7))
        attend(3)
        share(2)
        inner_pass(3)
        edge_partner(range(7, TILES))
        share(3)

        @pl.when(inner)
        def _():
            run(second_hop, range(3))
            hand_on()

    @pl.when(helped)
    def _():
        run(to_partner, tiles)
        tell().wait_recv()

    share(heads)

    @pl.when(edge)
    def _():
        gather()
        set_scale()
        for some in pairs:
            keep(some, dot(gained(z), z, some), fresh=True)
        centre_far()
        for some in pairs:
            keep(some, dot(gained(centre), centre, some))
        for n, some in enumerate(groups):
            expect(far_in.at[pl.ds(0, len(some))], f_recv.at[n])
            for f in some:
                put(f, acc[f] + far_in[f].astype(jnp.float32))

    def part_of(p):
        return pl.ds(pl.multiple_of(p * half, half), half)

    def half_dot(f, p):
        return jnp.dot(
            asked[beyond - far_base, :, part_of(p)], wbuf[beyond, f, part_of(p)],
            preferred_element_type=jnp.float32,
        )

    def prepare(f):
        far_acc[f - late] = half_dot(f, parity) + dot(asked[centre - far_base], centre, (f,))

    def reply(f):
        landed(BEYOND_FAR, f)
        if f < late:
            far = dot(asked[beyond - far_base], beyond, (f,)) + dot(asked[centre - far_base], centre, (f,))
        else:
            far = far_acc[f - late] + half_dot(f, 1 - parity)
        far_out[f] = far.astype(far_out.dtype)
        answer(f).start()

    def own(some):
        keep(some, dot(gained(z), z, some) + dot(gained(centre), centre, some), fresh=True)

    @pl.when(inner)
    def _():
        run(second_hop, range(3, 4))
        heard()
        centre_far()
        reply(0)
        run(second_hop, range(4, 5))
        tails(0)
        reply(1)
        run(second_hop, range(5, 6))
        reply(2)
        tails(1)
        run(second_hop, range(6, 7))
        run(prepare, range(late, late + 1))
        reply(3)
        run(second_hop, range(7, 8))
        run(prepare, range(late + 1, TILES))
        run(reply, range(4, TILES))
        gather()
        set_scale()
        run(own, pairs)
        outer_rest()
        for some in pairs:
            total = dot(gained(outer), outer, some) + dot(gained(beyond), beyond, some)
            for n, f in enumerate(some):
                put(f, acc[f] + total[:, n * tile : (n + 1) * tile])

    halves = wbuf.at[0, :, pl.ds(0, half)]
    drain(lat.at[:, pl.ds(0, n_tp - 1)])
    drain(slabs(n_tp - 1, VALUE_DIM))
    for _ in range(2):
        drain(halves)

    @pl.when(jnp.logical_or(inner, is_near(t)))
    def _():
        drain(slabs(n_tp - 1, cols))

    @pl.when(edge)
    def _():
        drain(lat.at[0, pl.ds(0, 1)])
        drain(halves)

    @pl.when(helped)
    def _():
        drain(ql)

    @pl.when(helps)
    def _():
        drain(asked.at[0])
        drain(tally)

    @pl.when(inner)
    def _():
        for count in (2, 3):
            drain(lat.at[0, pl.ds(0, count)])
        for _ in range(3):
            drain(halves)
        drain(asked.at[0])
        drain(far_out)


MESH = pl.DeviceIdType.MESH


def on_device_fused(
    n_sp, n_tp,
    query_latent, key_latent, rotary_key, query_gain, latent_gain,
    query_up, key_up, value_up, out_gain, out_weight,
):
    block_rows, row_count = query_latent.shape[0], key_latent.shape[0]
    rank, width = key_latent.shape[1], rotary_key.shape[1]
    keys = n_sp * n_tp * row_count
    depth, features = out_weight.shape
    cols = value_up.shape[1]
    vmem, bf16, dma = pltpu.VMEM, jnp.bfloat16, pltpu.SemaphoreType.DMA
    table = jnp.asarray(rope_table(keys, width))
    tiled = (TILES, block_rows, features // TILES)
    in_hbm = pl.BlockSpec(memory_space=pl.ANY)
    return pl.pallas_call(
        functools.partial(kernel, n_sp, n_tp),
        out_shape=vmem((block_rows, features), bf16),
        in_specs=[in_hbm] * 11,
        out_specs=pl.BlockSpec(memory_space=pltpu.VMEM),
        scratch_shapes=[
            vmem(query_latent.shape, bf16),
            vmem(query_latent.shape, bf16),
            vmem((query_gain.shape[0] // LANES, LANES), jnp.float32),
            vmem((1, rank), jnp.float32),
            vmem((1, cols), jnp.float32),
            vmem(table.shape, jnp.float32),
            vmem((n_sp, n_tp, row_count, rank + width), bf16),
            vmem((n_sp, TILES, depth, features // TILES), bf16),
            vmem(query_up.shape, bf16),
            vmem(key_up.shape, bf16),
            vmem(value_up.shape, bf16),
            vmem((keys, rank), bf16),
            vmem((keys, width), bf16),
            vmem((block_rows, query_up.shape[1]), bf16),
            vmem((block_rows, query_up.shape[1]), bf16),
            vmem(query_latent.shape, bf16),
            vmem((n_tp, block_rows, cols + VALUE_DIM), bf16),
            vmem((block_rows, VALUE_DIM), jnp.float32),
            vmem((block_rows, VALUE_DIM), jnp.float32),
            vmem((block_rows, VALUE_DIM), bf16),
            vmem(tiled, jnp.float32),
            vmem((max(TAILS), *tiled[1:]), jnp.float32),
            vmem((n_tp // 2, block_rows, cols), bf16),
            vmem(tiled, bf16),
            vmem(tiled, bf16),
            dma((4,)),
            dma((2,)),
            dma((1,)),
            dma((n_sp + 1,)),
            dma((2,)),
            dma((TILES // 2 + 3 * TILES,)),
            dma((4,)),
            dma((1,)),
            dma((3,)),
            dma((4,)),
        ],
        compiler_params=pltpu.CompilerParams(
            collective_id=0, has_side_effects=True
        ),
    )(
        query_latent, key_latent, rotary_key, query_gain.reshape(-1, LANES), latent_gain[None], out_gain[None],
        table, query_up, key_up, value_up, out_weight,
    )


def fits_fused(mesh):
    n_grp, n_sp, n_tp = (mesh.shape[name] for name in ("grp", "sp", "tp"))
    return n_grp % 2 == 0 and n_sp == LINE and n_sp == n_tp


def solution(mesh):
    in_specs = (
        P(("grp", "sp"), None),
        P(("grp", "sp", "tp"), None),
        P(("grp", "sp", "tp"), None),
        P(),
        P(),
        P(None, "tp"),
        P(None, "tp"),
        P(None, "tp"),
        P("tp"),
        P("sp", "tp"),
    )
    out_specs = P(("grp", "sp"), "tp")
    step = on_device
    if fits_fused(mesh):
        step = functools.partial(on_device_fused, mesh.shape["sp"], mesh.shape["tp"])
    return jax.shard_map(
        step, mesh=mesh, in_specs=in_specs, out_specs=out_specs, check_vma=False
    )
```

```python
import functools

import jax
import jax.numpy as jnp
import numpy as np
from jax import lax
from jax.experimental import pallas as pl
from jax.experimental.pallas import tpu as pltpu
from jax.sharding import PartitionSpec as P

HEADS = 16
NOPE_DIM = 128
ROPE_DIM = 64
VALUE_DIM = 128
KVRANK = 256


norm_eps = 1e-06
rope_theta = 10000.0


def rms_scaled(inputs, gain_vec):
    widened = inputs.astype(jnp.float32)
    return (
        widened
        * lax.rsqrt(jnp.mean(widened * widened, axis=-1, keepdims=True) + norm_eps)
        * gain_vec
    )


def rotate_half(inputs, positions):
    half_width = inputs.shape[-1] // 2
    inverse = rope_theta ** (-jnp.arange(half_width, dtype=jnp.float32) / half_width)
    angles = positions[:, None] * inverse[None, :]
    if inputs.ndim == 3:
        angles = angles[:, None, :]
    cosine = jnp.cos(angles)
    sine = jnp.sin(angles)
    widened = inputs.astype(jnp.float32)
    first = widened[..., :half_width]
    second = widened[..., half_width:]
    return jnp.concatenate(
        [first * cosine - second * sine, second * cosine + first * sine], axis=-1
    )


def on_device(
    query_latent,
    key_latent,
    rotary_key,
    query_gain,
    latent_gain,
    query_up,
    key_up,
    value_up,
    out_gain,
    out_weight,
):
    block_rows = query_latent.shape[0]
    row_count = key_latent.shape[0]
    head_local = key_up.shape[1] // NOPE_DIM
    block_start = lax.axis_index("sp") * block_rows
    own_start = block_start + lax.axis_index("tp") * row_count
    score_scale = (NOPE_DIM + ROPE_DIM) ** (-0.5)
    normed = rms_scaled(query_latent, query_gain).astype(jnp.bfloat16)
    query_full = jnp.dot(normed, query_up, preferred_element_type=jnp.float32).astype(jnp.bfloat16)
    query_full = query_full.reshape(block_rows, head_local, NOPE_DIM + ROPE_DIM)
    query_positions = (block_start + jnp.arange(block_rows, dtype=jnp.int32)).astype(jnp.float32)
    query_plain = query_full[..., :NOPE_DIM]
    query_turned = rotate_half(query_full[..., NOPE_DIM:], query_positions).astype(jnp.bfloat16)
    latent_normed = rms_scaled(key_latent, latent_gain).astype(jnp.bfloat16)
    own_positions = (own_start + jnp.arange(row_count, dtype=jnp.int32)).astype(jnp.float32)
    key_turned = rotate_half(rotary_key, own_positions).astype(jnp.bfloat16)
    running_max = jnp.full((block_rows, head_local), -1e30, jnp.float32)
    running_sum = jnp.zeros((block_rows, head_local), jnp.float32)
    weighted = jnp.zeros((block_rows, head_local, KVRANK), jnp.float32)
    latents = lax.all_gather(latent_normed, ("sp", "tp"), axis=0, tiled=True)
    turned_keys = lax.all_gather(key_turned, ("sp", "tp"), axis=0, tiled=True)
    portion_rows = latents.shape[0]
    step_rows = min(portion_rows, 2048)
    for begin in range(0, portion_rows, step_rows):
        latent_part = latents[begin : begin + step_rows]
        turned_part = turned_keys[begin : begin + step_rows]
        key_plain = jnp.dot(latent_part, key_up, preferred_element_type=jnp.float32).astype(
            jnp.bfloat16
        )
        key_plain = key_plain.reshape(latent_part.shape[0], head_local, NOPE_DIM)
        scores = jnp.einsum(
            "qhd,khd->qhk", query_plain, key_plain, preferred_element_type=jnp.float32
        )
        scores = scores + jnp.einsum(
            "qhd,kd->qhk", query_turned, turned_part, preferred_element_type=jnp.float32
        )
        scores = scores * score_scale
        new_max = jnp.maximum(running_max, jnp.max(scores, axis=-1))
        rescale = jnp.exp(running_max - new_max)
        expo = jnp.exp(scores - new_max[..., None])
        running_sum = running_sum * rescale + jnp.sum(expo, axis=-1)
        weighted = weighted * rescale[..., None] + jnp.einsum(
            "qhk,kc->qhc",
            expo.astype(jnp.bfloat16),
            latent_part,
            preferred_element_type=jnp.float32,
        )
        running_max = new_max
    final_state = (running_max, running_sum, weighted)
    running_max, running_sum, weighted = final_state
    latent_mix = (weighted / running_sum[..., None]).astype(jnp.bfloat16)
    value_heads = value_up.reshape(KVRANK, head_local, VALUE_DIM)
    head_out = jnp.einsum(
        "qhc,chd->qhd", latent_mix, value_heads, preferred_element_type=jnp.float32
    ).astype(jnp.bfloat16)
    head_out = head_out.reshape(block_rows, head_local * VALUE_DIM)
    widened = head_out.astype(jnp.float32)
    square_part = jnp.sum(widened * widened, axis=1)
    gained = (widened * out_gain).astype(jnp.bfloat16)
    all_gained, square_parts = (
        lax.all_gather(gained, "tp", axis=1, tiled=True),
        lax.all_gather(square_part[:, None].astype(jnp.bfloat16), "tp", axis=1, tiled=True).astype(
            jnp.float32
        ),
    )
    all_squares = jnp.sum(square_parts, axis=1)
    own_sums = jnp.dot(
        all_gained,
        lax.all_gather(out_weight, "sp", axis=0, tiled=True),
        preferred_element_type=jnp.float32,
    )
    mean_square = all_squares / (HEADS * VALUE_DIM)
    return (own_sums * lax.rsqrt(mean_square + norm_eps)[:, None]).astype(jnp.bfloat16)


LANES = 128
LINE = 4
TILES = 8
TAILS = (2, 2)
AT_EXIT = (3, 1)
ORDERS = ((4, 6, 5, 7), (4, 5, 6, 7))
LATE = 3


def rope_table(tokens, width):
    half = width // 2
    inverse = np.float32(rope_theta) ** (-np.arange(half, dtype=np.float32) / np.float32(half))
    angles = np.arange(tokens, dtype=np.float32)[:, None] * inverse.astype(np.float32)[None, :]
    wide = angles.astype(np.float32).astype(np.float64)
    cosine, sine = np.cos(wide), np.sin(wide)
    return np.concatenate([cosine, cosine, -sine, sine], axis=1).astype(np.float32)


def turned(wide, table):
    width = wide.shape[-1]
    half = width // 2
    swapped = jnp.concatenate([wide[:, half:], wide[:, :half]], axis=1)
    return wide * table[:, :width] + swapped * table[:, width:]


def kernel(
    n_sp, n_tp,
    ql_hbm, kl, rk, qg_hbm, lg_hbm, og_hbm, table_hbm, qup, kup, vup, ow, out,
    ql, ql_outer, qg, lg, og, table,
    lat, wbuf, qbuf, kbuf, vbuf, latn, kturn, qfull, qfull_outer, qnorm, gall, squares, squares_outer, tally,
    acc, far_acc, asked,
    far_out, far_in,
    local, w_local, sends, l_recv, g_recv, w_recv, m_recv, q_recv, h_recv, f_recv,
):
    z, t, g = lax.axis_index("sp"), lax.axis_index("tp"), lax.axis_index("grp")
    parity = lax.rem(g, 2)
    partner = g + 1 - 2 * parity
    core = lax.rem(t, 2)
    sibling = t + 1 - 2 * core
    block_rows = ql.shape[0]
    depth = ow.shape[0]
    half = depth // 2
    tile = wbuf.shape[3]
    heads = kup.shape[1] // NOPE_DIM
    cols = heads * VALUE_DIM
    head_width = NOPE_DIM + ROPE_DIM
    rank = kl.shape[1]
    width = rk.shape[1]
    keys = n_sp * n_tp * kl.shape[0]

    lower = z < n_sp // 2
    toward = jnp.where(lower, 1, -1)
    centre = z + toward
    outer = z - toward
    beyond = centre + toward
    has_up, has_down = z < n_sp - 1, z > 0
    edge = jnp.logical_or(z == 0, z == n_sp - 1)
    inner = jnp.logical_not(edge)
    far_base = jnp.where(lower, n_tp // 2, 0)
    far_group = jnp.logical_and(t >= far_base, t < far_base + n_tp // 2)
    helps = jnp.logical_and(inner, far_group)
    helped = jnp.logical_and(edge, far_group)

    loads = [
        pltpu.make_async_copy(src, dst, local.at[i])
        for i, src, dst in (
            (0, kl, lat.at[z, t, :, pl.ds(0, rank)]),
            (0, rk, lat.at[z, t, :, pl.ds(rank, width)]),
            (1, ql_hbm, ql),
            (2, qg_hbm, qg),
            (2, qup, qbuf),
            (3, lg_hbm, lg),
            (3, table_hbm, table),
            (3, kup, kbuf),
            (3, vup, vbuf),
            (3, og_hbm, og),
        )
    ]
    def w_load(f):
        return pltpu.make_async_copy(
            ow.at[:, pl.ds(f * tile, tile)], wbuf.at[z, f], w_local.at[min(f, 1)]
        )

    for load in loads[:3]:
        load.start()
    w_load(0).start()
    for load in loads[3:5]:
        load.start()
    for f in range(1, TILES):
        w_load(f).start()
    for load in loads[5:]:
        load.start()

    barrier = pltpu.get_barrier_semaphore()

    @pl.when(has_up)
    def _():
        pl.semaphore_signal(barrier, inc=1, device_id={"sp": z + 1}, device_id_type=MESH)

    @pl.when(has_down)
    def _():
        pl.semaphore_signal(barrier, inc=1, device_id={"sp": z - 1}, device_id_type=MESH)

    pl.semaphore_signal(barrier, inc=1, device_id={"grp": partner}, device_id_type=MESH)
    for d in range(1, n_tp):
        pl.semaphore_signal(barrier, inc=1, device_id={"tp": lax.rem(t + d, n_tp)}, device_id_type=MESH)
    pl.semaphore_wait(barrier, n_tp + jnp.where(edge, 1, 2))

    def remote(src, dst, recv, target):
        return pltpu.make_async_remote_copy(
            src_ref=src, dst_ref=dst, send_sem=sends.at[0], recv_sem=recv,
            device_id=target, device_id_type=MESH,
        )

    opposite = lax.rem(t + n_tp // 2, n_tp)

    def drain(ref):
        remote(ref, ref, sends.at[0], {"tp": opposite}).wait_send()

    def expect(ref, recv):
        remote(ref, ref, recv, {"tp": opposite}).wait_recv()

    def part_along(b, up):
        return remote(lat.at[b, t], lat.at[b, t], l_recv.at[b], {"sp": z + 1 if up else z - 1})

    def part_across(b, d):
        return remote(lat.at[b, t], lat.at[b, t], l_recv.at[n_sp], {"tp": lax.rem(t + d, n_tp)})

    def spread(b):
        for d in range(1, n_tp):
            part_across(b, d).start()

    def arrive(d):
        @pl.when(z >= d)
        def _():
            part_along(z - d, 1).wait_recv()

            @pl.when(has_up)
            def _():
                part_along(z - d, 1).start()

            spread(z - d)

        @pl.when(z + d < n_sp)
        def _():
            part_along(z + d, 0).wait_recv()

            @pl.when(has_down)
            def _():
                part_along(z + d, 0).start()

            spread(z + d)

    FROM_OUTER, SECOND_PIECE = 0, TILES // 2 + 3 * TILES
    FROM_CENTRE, BEYOND_NEAR, BEYOND_FAR = (TILES // 2 + TILES * i for i in range(3))
    CENTRE_FAR, EARLY_TAIL, LATE_TAIL, REST = range(4)
    last = TILES - 1
    cut_most, cut_least = TILES - max(TAILS), TILES - min(TAILS)
    first_tail = [TILES - count for count in TAILS]

    def rows_of(b, p, f):
        return wbuf.at[b, f, pl.ds(pl.multiple_of(p * half, half), half)]

    def moved(ref, recv, target):
        return remote(ref, ref, recv, target)

    def pieces(b, f):
        if f:
            return [(rows_of(b, parity, f), FROM_CENTRE + f)]
        rows = half // 2
        return [
            (wbuf.at[b, f, pl.ds(pl.multiple_of(parity * half + n * rows, rows), rows)], role)
            for n, role in enumerate((FROM_CENTRE, SECOND_PIECE))
        ]

    def inward(f):
        return [
            moved(ref, w_recv.at[jnp.where(edge, FROM_OUTER + f // 2, role)], {"sp": centre})
            for ref, role in pieces(z, f)
        ]

    def outward(f):
        return [moved(ref, w_recv.at[role], {"sp": outer}) for ref, role in pieces(z, f)]

    def passed(f):
        return moved(rows_of(outer, parity, f), w_recv.at[BEYOND_NEAR + f], {"sp": centre})

    def inward_far(ref, part):
        return moved(ref, m_recv.at[part], {"sp": centre})


    def across_beyond(f):
        return moved(rows_of(beyond, parity, f), w_recv.at[BEYOND_FAR + f], {"grp": partner})

    def pass_tail(f):
        return moved(rows_of(outer, 1 - parity, f), w_recv.at[BEYOND_FAR + f], {"sp": centre})

    def of_tiles(count):
        return wbuf.at[0, pl.ds(0, count), pl.ds(0, half)]

    def landed(role, f):
        expect(wbuf.at[0, f, pl.ds(0, half)], w_recv.at[role + f])

    def near(f):
        if f == 0:
            w_load(0).wait()
        if f == 1:
            rest = wbuf.at[z, pl.ds(1, last)]
            pltpu.make_async_copy(rest, rest, w_local.at[1]).wait()
        for copy in inward(f):
            copy.start()

    def near_out(f):
        @pl.when(inner)
        def _():
            for copy in outward(f):
                copy.start()

    def near_far():
        @pl.when(edge)
        def _():
            for f in range(cut_most, TILES):
                inward_far(rows_of(z, 1 - parity, f), EARLY_TAIL if f < cut_least else LATE_TAIL).start()
            for f in range(cut_most):
                inward_far(rows_of(z, 1 - parity, f), REST).start()

    def to_partner(f):
        for ref, role in pieces(centre, f):
            expect(ref, w_recv.at[role])
            moved(ref, m_recv.at[CENTRE_FAR], {"grp": partner}).start()

    def inner_partner(some):
        @pl.when(inner)
        def _():
            for f in some:
                to_partner(f)

    def inner_pass(pair):
        @pl.when(inner)
        def _():
            expect(wbuf.at[0, pl.ds(0, 2), pl.ds(0, half)], w_recv.at[FROM_OUTER + pair])
            for f in (2 * pair, 2 * pair + 1):
                passed(f).start()

    def edge_partner(some):
        @pl.when(edge)
        def _():
            for f in some:
                to_partner(f)

    def second_hop(f):
        landed(BEYOND_NEAR, f)
        if f < cut_most:
            across_beyond(f).start()
        else:
            for c, first in enumerate(first_tail):
                if f < first:
                    @pl.when(core == c)
                    def _():
                        across_beyond(f).start()

    def tails(c):
        @pl.when(core == c)
        def _():
            if first_tail[c] < cut_least:
                expect(of_tiles(cut_least - cut_most), m_recv.at[EARLY_TAIL])
                for f in range(cut_most, cut_least):
                    pass_tail(f).start()
            expect(of_tiles(TILES - cut_least), m_recv.at[LATE_TAIL])
            for f in range(cut_least, TILES):
                pass_tail(f).start()

    def outer_rest():
        expect(of_tiles(cut_most), m_recv.at[REST])
        for c, first in enumerate(first_tail):
            if first != cut_most:
                @pl.when(core == c)
                def _():
                    expect(of_tiles(cut_least - cut_most), m_recv.at[EARLY_TAIL])

    def centre_far():
        expect(wbuf.at[0, :, pl.ds(0, half)], m_recv.at[CENTRE_FAR])

    def project(latent, full):
        wide = latent[...].astype(jnp.float32)
        mean = jnp.mean(wide * wide, axis=-1, keepdims=True)
        gain = jnp.concatenate([qg[i : i + 1] for i in range(qg.shape[0])], axis=1)
        qnorm[...] = (wide * lax.rsqrt(mean + norm_eps) * gain).astype(jnp.bfloat16)
        full[...] = jnp.dot(qnorm[...], qbuf[...], preferred_element_type=jnp.float32).astype(
            jnp.bfloat16
        )

    lent_rows = block_rows // 2

    def lent(c):
        return pl.ds(pl.multiple_of(c * lent_rows, lent_rows), lent_rows)

    def lend():
        return remote(ql.at[lent(core)], ql_outer.at[lent(core)], h_recv.at[1], {"sp": centre})

    def swap(c):
        part = ql_outer.at[lent(c)]
        return remote(part, part, h_recv.at[3], {"tp": sibling})

    def lend_on():
        @pl.when(helps)
        def _():
            lend().wait_recv()
            swap(core).start()

    def queries():
        for load in loads[3:5]:
            load.wait()
        project(ql, qfull)

    def outer_queries():
        @pl.when(helps)
        def _():
            swap(1 - core).wait_recv()
            project(ql_outer, qfull_outer)

    def latents():
        for load in loads[5:]:
            load.wait()
        expect(lat.at[:, pl.ds(0, n_tp - 1)], l_recv.at[n_sp])
        whole = lat[...].reshape(keys, rank + width)
        wide = whole[:, :rank].astype(jnp.float32)
        mean = jnp.mean(wide * wide, axis=-1, keepdims=True)
        latn[...] = (wide * lax.rsqrt(mean + norm_eps) * lg[...]).astype(jnp.bfloat16)
        spun = whole[:, rank:].astype(jnp.float32)
        kturn[...] = turned(spun, table[...]).astype(jnp.bfloat16)

    transposed = (((1,), (1,)), ((), ()))

    def attend_with(h, full, block, store, squares):
        start = h * head_width
        plain = full[:, start : start + NOPE_DIM]
        spun = full[:, start + NOPE_DIM : start + head_width].astype(jnp.float32)
        own = table[pl.ds(pl.multiple_of(block * block_rows, block_rows), block_rows), :]
        spun = turned(spun, own).astype(jnp.bfloat16)
        key_plain = jnp.dot(
            latn[...], kbuf[:, h * NOPE_DIM : (h + 1) * NOPE_DIM], preferred_element_type=jnp.float32
        ).astype(jnp.bfloat16)
        scores = lax.dot_general(plain, key_plain, transposed, preferred_element_type=jnp.float32)
        scores = scores + lax.dot_general(
            spun, kturn[...], transposed, preferred_element_type=jnp.float32
        )
        scores = scores * (head_width ** (-0.5))
        expo = jnp.exp(scores - jnp.max(scores, axis=-1, keepdims=True))
        total = jnp.sum(expo, axis=-1, keepdims=True)
        mix = jnp.dot(expo.astype(jnp.bfloat16), latn[...], preferred_element_type=jnp.float32)
        mix = (mix / total).astype(jnp.bfloat16)
        head_out = jnp.dot(
            mix, vbuf[:, h * VALUE_DIM : (h + 1) * VALUE_DIM], preferred_element_type=jnp.float32
        ).astype(jnp.bfloat16)
        wide = head_out.astype(jnp.float32)
        gained = wide * og[:, h * VALUE_DIM : (h + 1) * VALUE_DIM]
        store(gained.astype(jnp.bfloat16))
        square = jnp.sum(wide * wide, axis=-1, keepdims=True)
        if h:
            square = square + squares[:, :1]
        squares[...] = jnp.broadcast_to(square, squares.shape)

    def attend(h):
        def store(value):
            gall[t, :, h * VALUE_DIM : (h + 1) * VALUE_DIM] = value

        attend_with(h, qfull, z, store, squares)
        if h == heads - 1:
            gall[t, :, cols:] = squares[...].astype(jnp.bfloat16)

    def attend_outer(h):
        def store(value):
            asked[core, :, h * VALUE_DIM : (h + 1) * VALUE_DIM] = value

        attend_with(h, qfull_outer, outer, store, squares_outer)
        if h == heads - 1:
            tally[...] = squares_outer[...].astype(jnp.bfloat16)

    def is_near(p):
        return jnp.logical_or(p < far_base, p >= far_base + n_tp // 2)

    def share(h):
        @pl.when(jnp.logical_or(inner, is_near(t)) if h < heads else True)
        def _():
            for d in range(1, n_tp):
                part = gall.at[t, :, pl.ds(h * VALUE_DIM, VALUE_DIM)]
                kind = h // heads
                remote(part, part, g_recv.at[kind], {"tp": lax.rem(t + d, n_tp)}).start()

    def slabs(count, span):
        return gall.at[pl.ds(0, count), :, pl.ds(0, span)]

    def gather():
        for where, count in (
            (inner, n_tp - 1),
            (jnp.logical_and(edge, is_near(t)), n_tp // 2 - 1),
            (helped, n_tp // 2),
        ):
            @pl.when(where)
            def _():
                expect(slabs(count, cols), g_recv.at[0])

        expect(slabs(n_tp - 1, VALUE_DIM), g_recv.at[1])

    def ask(h):
        part = asked.at[core, :, pl.ds(h * VALUE_DIM, VALUE_DIM)]
        return remote(part, part, q_recv.at[0], {"tp": opposite})

    def tell():
        return remote(tally, gall.at[t, :, pl.ds(cols, VALUE_DIM)], h_recv.at[2], {"sp": outer})

    def hand(c):
        return remote(asked.at[c], asked.at[c], h_recv.at[0], {"tp": sibling})

    def hand_on():
        @pl.when(jnp.logical_not(helps))
        def _():
            expect(asked.at[0], q_recv.at[0])

        hand(core).start()

    def heard():
        hand(1 - core).wait_recv()

    early = TILES - LATE

    def answer(f):
        return remote(far_out.at[f], far_in.at[f], f_recv.at[max(0, f - early + 1)], {"sp": outer})

    def wide_of(b, some):
        return jnp.concatenate([wbuf[b, f] for f in some], axis=1)

    def dot(lhs, b, some):
        return jnp.dot(lhs, wide_of(b, some), preferred_element_type=jnp.float32)

    def gained(b):
        return gall[b, :, :cols]

    def keep(some, total, fresh=False):
        for n, f in enumerate(some):
            part = total[:, n * tile : (n + 1) * tile]
            acc[f] = part if fresh else acc[f] + part

    def set_scale():
        square = gall[0, :, cols : cols + 1].astype(jnp.float32)
        for p in range(1, n_tp):
            square = square + gall[p, :, cols : cols + 1].astype(jnp.float32)
        squares[...] = jnp.broadcast_to(lax.rsqrt(square / (n_tp * cols) + norm_eps), squares.shape)

    def put(f, total):
        out[:, f * tile : (f + 1) * tile] = (total * squares[...]).astype(out.dtype)

    def run(call, some):
        for i in some:
            call(i)

    tiles = range(TILES)
    pairs = [(f, f + 1) for f in range(0, TILES, 2)]

    loads[0].wait()
    loads[1].wait()

    @pl.when(has_up)
    def _():
        part_along(z, 1).start()

    @pl.when(has_down)
    def _():
        part_along(z, 0).start()

    spread(z)
    loads[2].wait()

    @pl.when(helped)
    def _():
        lend().start()

    for c, count in enumerate(AT_EXIT):
        pl.when(core == c)(functools.partial(run, near, range(count)))
    queries()
    arrive(1)
    for c, count in enumerate(AT_EXIT):
        pl.when(core == c)(functools.partial(run, near, range(count, TILES)))
    run(near_out, range(2))
    for c, count in enumerate(AT_EXIT):
        pl.when(core == c)(functools.partial(inner_partner, range(max(count, 2))))
    lend_on()
    arrive(2)
    run(near_out, range(2, TILES))
    for c, count in enumerate(AT_EXIT):
        pl.when(core == c)(functools.partial(inner_partner, range(max(count, 2), 3)))
    arrive(3)
    near_far()
    outer_queries()
    inner_partner(range(3, 4))
    latents()
    inner_partner(range(4, 5))
    inner_pass(0)

    @pl.when(helps)
    def _():
        attend_outer(0)
        run(to_partner, range(5, 6))
        attend_outer(1)
        ask(0).start()
        inner_pass(1)
        run(to_partner, range(6, 7))
        attend_outer(2)
        ask(1).start()
        run(to_partner, range(7, TILES))
        attend_outer(3)
        ask(2).start()
        inner_pass(2)
        ask(3).start()
        tell().start()
        attend(0)
        hand_on()
        run(second_hop, range(1))
        attend(1)
        share(0)
        attend(2)
        share(1)
        inner_pass(3)
        run(second_hop, range(1, 2))
        attend(3)
        share(2)
        run(second_hop, range(2, 3))
        share(3)

    @pl.when(is_near(t))
    def _():
        attend(0)
        inner_partner(range(5, 6))
        inner_pass(1)
        edge_partner(range(5))
        attend(1)
        share(0)
        edge_partner(range(5, 6))
        attend(2)
        share(1)
        inner_partner(range(6, TILES))
        inner_pass(2)
        edge_partner(range(6, 7))
        attend(3)
        share(2)
        inner_pass(3)
        edge_partner(range(7, TILES))
        share(3)

        @pl.when(inner)
        def _():
            run(second_hop, range(3))
            hand_on()

    @pl.when(helped)
    def _():
        run(to_partner, tiles)
        tell().wait_recv()

    share(heads)

    @pl.when(edge)
    def _():
        gather()
        set_scale()
        for some in pairs:
            keep(some, dot(gained(z), z, some), fresh=True)
        centre_far()
        for some in pairs:
            keep(some, dot(gained(centre), centre, some))
        def add(f):
            put(f, acc[f] + far_in[f].astype(jnp.float32))

        expect(far_in.at[pl.ds(0, early)], f_recv.at[0])
        run(add, range(early))
        for c, order in enumerate(ORDERS):
            @pl.when(core == c)
            def _():
                for f in order:
                    if f >= early:
                        expect(far_in.at[0], f_recv.at[f - early + 1])
                        add(f)

    def part_of(p):
        return pl.ds(pl.multiple_of(p * half, half), half)

    def half_dot(f, p):
        return jnp.dot(
            asked[beyond - far_base, :, part_of(p)], wbuf[beyond, f, part_of(p)],
            preferred_element_type=jnp.float32,
        )

    def prepare(f):
        far_acc[f - early] = half_dot(f, parity) + dot(asked[centre - far_base], centre, (f,))

    def reply(f):
        landed(BEYOND_FAR, f)
        if f < early:
            far = dot(asked[beyond - far_base], beyond, (f,)) + dot(asked[centre - far_base], centre, (f,))
        else:
            far = far_acc[f - early] + half_dot(f, 1 - parity)
        far_out[f] = far.astype(far_out.dtype)
        answer(f).start()

    def own(some):
        keep(some, dot(gained(z), z, some) + dot(gained(centre), centre, some), fresh=True)

    @pl.when(inner)
    def _():
        run(second_hop, range(3, 4))
        heard()
        centre_far()
        reply(0)
        run(second_hop, range(4, 5))
        tails(0)
        reply(1)
        run(second_hop, range(5, 6))
        reply(2)
        tails(1)
        run(second_hop, range(6, 7))
        reply(3)
        run(second_hop, range(7, 8))
        run(prepare, range(early, TILES))
        for c, order in enumerate(ORDERS):
            pl.when(core == c)(functools.partial(run, reply, order))
        gather()
        set_scale()
        run(own, pairs)
        outer_rest()
        for some in pairs:
            total = dot(gained(outer), outer, some) + dot(gained(beyond), beyond, some)
            for n, f in enumerate(some):
                put(f, acc[f] + total[:, n * tile : (n + 1) * tile])

    halves = wbuf.at[0, :, pl.ds(0, half)]
    drain(lat.at[:, pl.ds(0, n_tp - 1)])
    drain(slabs(n_tp - 1, VALUE_DIM))
    for _ in range(2):
        drain(halves)

    @pl.when(jnp.logical_or(inner, is_near(t)))
    def _():
        drain(slabs(n_tp - 1, cols))

    @pl.when(edge)
    def _():
        drain(lat.at[0, pl.ds(0, 1)])
        drain(halves)

    @pl.when(helped)
    def _():
        drain(ql.at[pl.ds(0, lent_rows)])

    @pl.when(helps)
    def _():
        drain(asked.at[0])
        drain(tally)
        drain(ql.at[pl.ds(0, lent_rows)])

    @pl.when(inner)
    def _():
        for count in (2, 3):
            drain(lat.at[0, pl.ds(0, count)])
        for _ in range(3):
            drain(halves)
        drain(asked.at[0])
        drain(far_out)


MESH = pl.DeviceIdType.MESH


def on_device_fused(
    n_sp, n_tp,
    query_latent, key_latent, rotary_key, query_gain, latent_gain,
    query_up, key_up, value_up, out_gain, out_weight,
):
    block_rows, row_count = query_latent.shape[0], key_latent.shape[0]
    rank, width = key_latent.shape[1], rotary_key.shape[1]
    keys = n_sp * n_tp * row_count
    depth, features = out_weight.shape
    cols = value_up.shape[1]
    vmem, bf16, dma = pltpu.VMEM, jnp.bfloat16, pltpu.SemaphoreType.DMA
    table = jnp.asarray(rope_table(keys, width))
    tiled = (TILES, block_rows, features // TILES)
    in_hbm = pl.BlockSpec(memory_space=pl.ANY)
    return pl.pallas_call(
        functools.partial(kernel, n_sp, n_tp),
        out_shape=vmem((block_rows, features), bf16),
        in_specs=[in_hbm] * 11,
        out_specs=pl.BlockSpec(memory_space=pltpu.VMEM),
        scratch_shapes=[
            vmem(query_latent.shape, bf16),
            vmem(query_latent.shape, bf16),
            vmem((query_gain.shape[0] // LANES, LANES), jnp.float32),
            vmem((1, rank), jnp.float32),
            vmem((1, cols), jnp.float32),
            vmem(table.shape, jnp.float32),
            vmem((n_sp, n_tp, row_count, rank + width), bf16),
            vmem((n_sp, TILES, depth, features // TILES), bf16),
            vmem(query_up.shape, bf16),
            vmem(key_up.shape, bf16),
            vmem(value_up.shape, bf16),
            vmem((keys, rank), bf16),
            vmem((keys, width), bf16),
            vmem((block_rows, query_up.shape[1]), bf16),
            vmem((block_rows, query_up.shape[1]), bf16),
            vmem(query_latent.shape, bf16),
            vmem((n_tp, block_rows, cols + VALUE_DIM), bf16),
            vmem((block_rows, VALUE_DIM), jnp.float32),
            vmem((block_rows, VALUE_DIM), jnp.float32),
            vmem((block_rows, VALUE_DIM), bf16),
            vmem(tiled, jnp.float32),
            vmem((LATE, *tiled[1:]), jnp.float32),
            vmem((n_tp // 2, block_rows, cols), bf16),
            vmem(tiled, bf16),
            vmem(tiled, bf16),
            dma((4,)),
            dma((2,)),
            dma((1,)),
            dma((n_sp + 1,)),
            dma((2,)),
            dma((TILES // 2 + 3 * TILES + 1,)),
            dma((4,)),
            dma((1,)),
            dma((4,)),
            dma((4,)),
        ],
        compiler_params=pltpu.CompilerParams(
            collective_id=0, has_side_effects=True
        ),
    )(
        query_latent, key_latent, rotary_key, query_gain.reshape(-1, LANES), latent_gain[None], out_gain[None],
        table, query_up, key_up, value_up, out_weight,
    )


def fits_fused(mesh):
    n_grp, n_sp, n_tp = (mesh.shape[name] for name in ("grp", "sp", "tp"))
    return n_grp % 2 == 0 and n_sp == LINE and n_sp == n_tp


def solution(mesh):
    in_specs = (
        P(("grp", "sp"), None),
        P(("grp", "sp", "tp"), None),
        P(("grp", "sp", "tp"), None),
        P(),
        P(),
        P(None, "tp"),
        P(None, "tp"),
        P(None, "tp"),
        P("tp"),
        P("sp", "tp"),
    )
    out_specs = P(("grp", "sp"), "tp")
    step = on_device
    if fits_fused(mesh):
        step = functools.partial(on_device_fused, mesh.shape["sp"], mesh.shape["tp"])
    return jax.shard_map(
        step, mesh=mesh, in_specs=in_specs, out_specs=out_specs, check_vma=False
    )
```

```python
import functools

import jax
import jax.numpy as jnp
import numpy as np
from jax import lax
from jax.experimental import pallas as pl
from jax.experimental.pallas import tpu as pltpu
from jax.sharding import PartitionSpec as P

HEADS = 16
NOPE_DIM = 128
ROPE_DIM = 64
VALUE_DIM = 128
KVRANK = 256


norm_eps = 1e-06
rope_theta = 10000.0


def rms_scaled(inputs, gain_vec):
    widened = inputs.astype(jnp.float32)
    return (
        widened
        * lax.rsqrt(jnp.mean(widened * widened, axis=-1, keepdims=True) + norm_eps)
        * gain_vec
    )


def rotate_half(inputs, positions):
    half_width = inputs.shape[-1] // 2
    inverse = rope_theta ** (-jnp.arange(half_width, dtype=jnp.float32) / half_width)
    angles = positions[:, None] * inverse[None, :]
    if inputs.ndim == 3:
        angles = angles[:, None, :]
    cosine = jnp.cos(angles)
    sine = jnp.sin(angles)
    widened = inputs.astype(jnp.float32)
    first = widened[..., :half_width]
    second = widened[..., half_width:]
    return jnp.concatenate(
        [first * cosine - second * sine, second * cosine + first * sine], axis=-1
    )


def on_device(
    query_latent,
    key_latent,
    rotary_key,
    query_gain,
    latent_gain,
    query_up,
    key_up,
    value_up,
    out_gain,
    out_weight,
):
    block_rows = query_latent.shape[0]
    row_count = key_latent.shape[0]
    head_local = key_up.shape[1] // NOPE_DIM
    block_start = lax.axis_index("sp") * block_rows
    own_start = block_start + lax.axis_index("tp") * row_count
    score_scale = (NOPE_DIM + ROPE_DIM) ** (-0.5)
    normed = rms_scaled(query_latent, query_gain).astype(jnp.bfloat16)
    query_full = jnp.dot(normed, query_up, preferred_element_type=jnp.float32).astype(jnp.bfloat16)
    query_full = query_full.reshape(block_rows, head_local, NOPE_DIM + ROPE_DIM)
    query_positions = (block_start + jnp.arange(block_rows, dtype=jnp.int32)).astype(jnp.float32)
    query_plain = query_full[..., :NOPE_DIM]
    query_turned = rotate_half(query_full[..., NOPE_DIM:], query_positions).astype(jnp.bfloat16)
    latent_normed = rms_scaled(key_latent, latent_gain).astype(jnp.bfloat16)
    own_positions = (own_start + jnp.arange(row_count, dtype=jnp.int32)).astype(jnp.float32)
    key_turned = rotate_half(rotary_key, own_positions).astype(jnp.bfloat16)
    running_max = jnp.full((block_rows, head_local), -1e30, jnp.float32)
    running_sum = jnp.zeros((block_rows, head_local), jnp.float32)
    weighted = jnp.zeros((block_rows, head_local, KVRANK), jnp.float32)
    latents = lax.all_gather(latent_normed, ("sp", "tp"), axis=0, tiled=True)
    turned_keys = lax.all_gather(key_turned, ("sp", "tp"), axis=0, tiled=True)
    portion_rows = latents.shape[0]
    step_rows = min(portion_rows, 2048)
    for begin in range(0, portion_rows, step_rows):
        latent_part = latents[begin : begin + step_rows]
        turned_part = turned_keys[begin : begin + step_rows]
        key_plain = jnp.dot(latent_part, key_up, preferred_element_type=jnp.float32).astype(
            jnp.bfloat16
        )
        key_plain = key_plain.reshape(latent_part.shape[0], head_local, NOPE_DIM)
        scores = jnp.einsum(
            "qhd,khd->qhk", query_plain, key_plain, preferred_element_type=jnp.float32
        )
        scores = scores + jnp.einsum(
            "qhd,kd->qhk", query_turned, turned_part, preferred_element_type=jnp.float32
        )
        scores = scores * score_scale
        new_max = jnp.maximum(running_max, jnp.max(scores, axis=-1))
        rescale = jnp.exp(running_max - new_max)
        expo = jnp.exp(scores - new_max[..., None])
        running_sum = running_sum * rescale + jnp.sum(expo, axis=-1)
        weighted = weighted * rescale[..., None] + jnp.einsum(
            "qhk,kc->qhc",
            expo.astype(jnp.bfloat16),
            latent_part,
            preferred_element_type=jnp.float32,
        )
        running_max = new_max
    final_state = (running_max, running_sum, weighted)
    running_max, running_sum, weighted = final_state
    latent_mix = (weighted / running_sum[..., None]).astype(jnp.bfloat16)
    value_heads = value_up.reshape(KVRANK, head_local, VALUE_DIM)
    head_out = jnp.einsum(
        "qhc,chd->qhd", latent_mix, value_heads, preferred_element_type=jnp.float32
    ).astype(jnp.bfloat16)
    head_out = head_out.reshape(block_rows, head_local * VALUE_DIM)
    widened = head_out.astype(jnp.float32)
    square_part = jnp.sum(widened * widened, axis=1)
    gained = (widened * out_gain).astype(jnp.bfloat16)
    all_gained, square_parts = (
        lax.all_gather(gained, "tp", axis=1, tiled=True),
        lax.all_gather(square_part[:, None].astype(jnp.bfloat16), "tp", axis=1, tiled=True).astype(
            jnp.float32
        ),
    )
    all_squares = jnp.sum(square_parts, axis=1)
    own_sums = jnp.dot(
        all_gained,
        lax.all_gather(out_weight, "sp", axis=0, tiled=True),
        preferred_element_type=jnp.float32,
    )
    mean_square = all_squares / (HEADS * VALUE_DIM)
    return (own_sums * lax.rsqrt(mean_square + norm_eps)[:, None]).astype(jnp.bfloat16)


LANES = 128
LINE = 4
TILES = 8
TAILS = (2, 2)
AT_EXIT = (3, 1)
ORDERS = ((4, 6, 5, 7), (4, 5, 6, 7))
LATE = 3


def rope_table(tokens, width):
    half = width // 2
    inverse = np.float32(rope_theta) ** (-np.arange(half, dtype=np.float32) / np.float32(half))
    angles = np.arange(tokens, dtype=np.float32)[:, None] * inverse.astype(np.float32)[None, :]
    wide = angles.astype(np.float32).astype(np.float64)
    cosine, sine = np.cos(wide), np.sin(wide)
    return np.concatenate([cosine, cosine, -sine, sine], axis=1).astype(np.float32)


def turned(wide, table):
    width = wide.shape[-1]
    half = width // 2
    swapped = jnp.concatenate([wide[:, half:], wide[:, :half]], axis=1)
    return wide * table[:, :width] + swapped * table[:, width:]


def kernel(
    n_sp, n_tp,
    ql_hbm, kl, rk, qg_hbm, lg_hbm, og_hbm, table_hbm, qup, kup, vup, ow, out,
    ql, ql_outer, qg, lg, og, table,
    lat, wbuf, qbuf, kbuf, vbuf, latn, kturn, qfull, qfull_outer, qnorm, gall, squares, squares_outer, tally,
    acc, far_acc, asked,
    far_out, far_in,
    local, w_local, sends, l_recv, g_recv, w_recv, m_recv, q_recv, h_recv, f_recv,
):
    z, t, g = lax.axis_index("sp"), lax.axis_index("tp"), lax.axis_index("grp")
    parity = lax.rem(g, 2)
    partner = g + 1 - 2 * parity
    core = lax.rem(t, 2)
    sibling = t + 1 - 2 * core
    block_rows = ql.shape[0]
    depth = ow.shape[0]
    half = depth // 2
    tile = wbuf.shape[3]
    heads = kup.shape[1] // NOPE_DIM
    cols = heads * VALUE_DIM
    head_width = NOPE_DIM + ROPE_DIM
    rank = kl.shape[1]
    width = rk.shape[1]
    keys = n_sp * n_tp * kl.shape[0]

    lower = z < n_sp // 2
    toward = jnp.where(lower, 1, -1)
    centre = z + toward
    outer = z - toward
    beyond = centre + toward
    has_up, has_down = z < n_sp - 1, z > 0
    edge = jnp.logical_or(z == 0, z == n_sp - 1)
    inner = jnp.logical_not(edge)
    far_base = jnp.where(lower, n_tp // 2, 0)
    far_group = jnp.logical_and(t >= far_base, t < far_base + n_tp // 2)
    helps = jnp.logical_and(inner, far_group)
    helped = jnp.logical_and(edge, far_group)

    loads = [
        pltpu.make_async_copy(src, dst, local.at[i])
        for i, src, dst in (
            (0, kl, lat.at[z, t, :, pl.ds(0, rank)]),
            (0, rk, lat.at[z, t, :, pl.ds(rank, width)]),
            (1, ql_hbm, ql),
            (2, qg_hbm, qg),
            (2, qup, qbuf),
            (3, lg_hbm, lg),
            (3, table_hbm, table),
            (3, kup, kbuf),
            (3, vup, vbuf),
            (3, og_hbm, og),
        )
    ]
    def w_load(f):
        return pltpu.make_async_copy(
            ow.at[:, pl.ds(f * tile, tile)], wbuf.at[z, f], w_local.at[min(f, 1)]
        )

    for load in loads[:3]:
        load.start()
    w_load(0).start()
    for load in loads[3:5]:
        load.start()
    for f in range(1, TILES):
        w_load(f).start()
    for load in loads[5:]:
        load.start()

    barrier = pltpu.get_barrier_semaphore()

    @pl.when(has_up)
    def _():
        pl.semaphore_signal(barrier, inc=1, device_id={"sp": z + 1}, device_id_type=MESH)

    @pl.when(has_down)
    def _():
        pl.semaphore_signal(barrier, inc=1, device_id={"sp": z - 1}, device_id_type=MESH)

    pl.semaphore_signal(barrier, inc=1, device_id={"grp": partner}, device_id_type=MESH)
    for d in range(1, n_tp):
        pl.semaphore_signal(barrier, inc=1, device_id={"tp": lax.rem(t + d, n_tp)}, device_id_type=MESH)
    pl.semaphore_wait(barrier, n_tp + jnp.where(edge, 1, 2))

    def remote(src, dst, recv, target):
        return pltpu.make_async_remote_copy(
            src_ref=src, dst_ref=dst, send_sem=sends.at[0], recv_sem=recv,
            device_id=target, device_id_type=MESH,
        )

    opposite = lax.rem(t + n_tp // 2, n_tp)

    def drain(ref):
        remote(ref, ref, sends.at[0], {"tp": opposite}).wait_send()

    def expect(ref, recv):
        remote(ref, ref, recv, {"tp": opposite}).wait_recv()

    def part_along(b, up):
        return remote(lat.at[b, t], lat.at[b, t], l_recv.at[b], {"sp": z + 1 if up else z - 1})

    def part_across(b, d):
        return remote(lat.at[b, t], lat.at[b, t], l_recv.at[n_sp], {"tp": lax.rem(t + d, n_tp)})

    def spread(b):
        for d in range(1, n_tp):
            part_across(b, d).start()

    def arrive(d):
        @pl.when(z >= d)
        def _():
            part_along(z - d, 1).wait_recv()

            @pl.when(has_up)
            def _():
                part_along(z - d, 1).start()

            spread(z - d)

        @pl.when(z + d < n_sp)
        def _():
            part_along(z + d, 0).wait_recv()

            @pl.when(has_down)
            def _():
                part_along(z + d, 0).start()

            spread(z + d)

    FROM_OUTER, SECOND_PIECE = 0, TILES // 2 + 3 * TILES
    FROM_CENTRE, BEYOND_NEAR, BEYOND_FAR = (TILES // 2 + TILES * i for i in range(3))
    CENTRE_FAR, EARLY_TAIL, LATE_TAIL, REST = range(4)
    last = TILES - 1
    cut_most, cut_least = TILES - max(TAILS), TILES - min(TAILS)
    first_tail = [TILES - count for count in TAILS]

    def rows_of(b, p, f):
        return wbuf.at[b, f, pl.ds(pl.multiple_of(p * half, half), half)]

    def moved(ref, recv, target):
        return remote(ref, ref, recv, target)

    def pieces(b, f):
        if f:
            return [(rows_of(b, parity, f), FROM_CENTRE + f)]
        rows = half // 2
        return [
            (wbuf.at[b, f, pl.ds(pl.multiple_of(parity * half + n * rows, rows), rows)], role)
            for n, role in enumerate((FROM_CENTRE, SECOND_PIECE))
        ]

    def inward(f):
        return [
            moved(ref, w_recv.at[jnp.where(edge, FROM_OUTER + f // 2, role)], {"sp": centre})
            for ref, role in pieces(z, f)
        ]

    def outward(f):
        return [moved(ref, w_recv.at[role], {"sp": outer}) for ref, role in pieces(z, f)]

    def passed(f):
        return moved(rows_of(outer, parity, f), w_recv.at[BEYOND_NEAR + f], {"sp": centre})

    def inward_far(ref, part):
        return moved(ref, m_recv.at[part], {"sp": centre})


    def across_beyond(f):
        return moved(rows_of(beyond, parity, f), w_recv.at[BEYOND_FAR + f], {"grp": partner})

    def pass_tail(f):
        return moved(rows_of(outer, 1 - parity, f), w_recv.at[BEYOND_FAR + f], {"sp": centre})

    def of_tiles(count):
        return wbuf.at[0, pl.ds(0, count), pl.ds(0, half)]

    def landed(role, f):
        expect(wbuf.at[0, f, pl.ds(0, half)], w_recv.at[role + f])

    def near(f):
        if f == 0:
            w_load(0).wait()
        if f == 1:
            rest = wbuf.at[z, pl.ds(1, last)]
            pltpu.make_async_copy(rest, rest, w_local.at[1]).wait()
        for copy in inward(f):
            copy.start()

    def near_out(f):
        @pl.when(inner)
        def _():
            for copy in outward(f):
                copy.start()

    def near_far():
        @pl.when(edge)
        def _():
            for f in range(cut_most, TILES):
                inward_far(rows_of(z, 1 - parity, f), EARLY_TAIL if f < cut_least else LATE_TAIL).start()
            for f in range(cut_most):
                inward_far(rows_of(z, 1 - parity, f), REST).start()

    def to_partner(f):
        for ref, role in pieces(centre, f):
            expect(ref, w_recv.at[role])
            moved(ref, m_recv.at[CENTRE_FAR], {"grp": partner}).start()

    def inner_partner(some):
        @pl.when(inner)
        def _():
            for f in some:
                to_partner(f)

    def inner_pass(pair):
        @pl.when(inner)
        def _():
            expect(wbuf.at[0, pl.ds(0, 2), pl.ds(0, half)], w_recv.at[FROM_OUTER + pair])
            for f in (2 * pair, 2 * pair + 1):
                passed(f).start()

    def edge_partner(some):
        @pl.when(edge)
        def _():
            for f in some:
                to_partner(f)

    def second_hop(f):
        landed(BEYOND_NEAR, f)
        if f < cut_most:
            across_beyond(f).start()
        else:
            for c, first in enumerate(first_tail):
                if f < first:
                    @pl.when(core == c)
                    def _():
                        across_beyond(f).start()

    def tails(c):
        @pl.when(core == c)
        def _():
            if first_tail[c] < cut_least:
                expect(of_tiles(cut_least - cut_most), m_recv.at[EARLY_TAIL])
                for f in range(cut_most, cut_least):
                    pass_tail(f).start()
            expect(of_tiles(TILES - cut_least), m_recv.at[LATE_TAIL])
            for f in range(cut_least, TILES):
                pass_tail(f).start()

    def outer_rest():
        expect(of_tiles(cut_most), m_recv.at[REST])
        for c, first in enumerate(first_tail):
            if first != cut_most:
                @pl.when(core == c)
                def _():
                    expect(of_tiles(cut_least - cut_most), m_recv.at[EARLY_TAIL])

    def centre_far():
        expect(wbuf.at[0, :, pl.ds(0, half)], m_recv.at[CENTRE_FAR])

    def project(latent, full):
        wide = latent[...].astype(jnp.float32)
        mean = jnp.mean(wide * wide, axis=-1, keepdims=True)
        gain = jnp.concatenate([qg[i : i + 1] for i in range(qg.shape[0])], axis=1)
        qnorm[...] = (wide * lax.rsqrt(mean + norm_eps) * gain).astype(jnp.bfloat16)
        full[...] = jnp.dot(qnorm[...], qbuf[...], preferred_element_type=jnp.float32).astype(
            jnp.bfloat16
        )

    lent_rows = block_rows // 2

    def lent(c):
        return pl.ds(pl.multiple_of(c * lent_rows, lent_rows), lent_rows)

    def lend():
        return remote(ql.at[lent(core)], ql_outer.at[lent(core)], h_recv.at[1], {"sp": centre})

    def swap(c):
        part = ql_outer.at[lent(c)]
        return remote(part, part, h_recv.at[3], {"tp": sibling})

    def lend_on():
        @pl.when(helps)
        def _():
            lend().wait_recv()
            swap(core).start()

    def queries():
        for load in loads[3:5]:
            load.wait()
        project(ql, qfull)

    def outer_queries():
        @pl.when(helps)
        def _():
            swap(1 - core).wait_recv()
            project(ql_outer, qfull_outer)

    def latents():
        for load in loads[5:]:
            load.wait()
        expect(lat.at[:, pl.ds(0, n_tp - 1)], l_recv.at[n_sp])
        whole = lat[...].reshape(keys, rank + width)
        wide = whole[:, :rank].astype(jnp.float32)
        mean = jnp.mean(wide * wide, axis=-1, keepdims=True)
        latn[...] = (wide * lax.rsqrt(mean + norm_eps) * lg[...]).astype(jnp.bfloat16)
        spun = whole[:, rank:].astype(jnp.float32)
        kturn[...] = turned(spun, table[...]).astype(jnp.bfloat16)

    transposed = (((1,), (1,)), ((), ()))

    def attend_with(h, full, block, store, squares):
        start = h * head_width
        plain = full[:, start : start + NOPE_DIM]
        spun = full[:, start + NOPE_DIM : start + head_width].astype(jnp.float32)
        own = table[pl.ds(pl.multiple_of(block * block_rows, block_rows), block_rows), :]
        spun = turned(spun, own).astype(jnp.bfloat16)
        key_plain = jnp.dot(
            latn[...], kbuf[:, h * NOPE_DIM : (h + 1) * NOPE_DIM], preferred_element_type=jnp.float32
        ).astype(jnp.bfloat16)
        scores = lax.dot_general(plain, key_plain, transposed, preferred_element_type=jnp.float32)
        scores = scores + lax.dot_general(
            spun, kturn[...], transposed, preferred_element_type=jnp.float32
        )
        scores = scores * (head_width ** (-0.5))
        expo = jnp.exp(scores - jnp.max(scores, axis=-1, keepdims=True))
        total = jnp.sum(expo, axis=-1, keepdims=True)
        mix = jnp.dot(expo.astype(jnp.bfloat16), latn[...], preferred_element_type=jnp.float32)
        mix = (mix / total).astype(jnp.bfloat16)
        head_out = jnp.dot(
            mix, vbuf[:, h * VALUE_DIM : (h + 1) * VALUE_DIM], preferred_element_type=jnp.float32
        ).astype(jnp.bfloat16)
        wide = head_out.astype(jnp.float32)
        gained = wide * og[:, h * VALUE_DIM : (h + 1) * VALUE_DIM]
        store(gained.astype(jnp.bfloat16))
        square = jnp.sum(wide * wide, axis=-1, keepdims=True)
        if h:
            square = square + squares[:, :1]
        squares[...] = jnp.broadcast_to(square, squares.shape)

    def attend(h):
        def store(value):
            gall[t, :, h * VALUE_DIM : (h + 1) * VALUE_DIM] = value

        attend_with(h, qfull, z, store, squares)
        if h == heads - 1:
            gall[t, :, cols:] = squares[...].astype(jnp.bfloat16)

    def attend_outer(h):
        def store(value):
            asked[core, :, h * VALUE_DIM : (h + 1) * VALUE_DIM] = value

        attend_with(h, qfull_outer, outer, store, squares_outer)
        if h == heads - 1:
            tally[...] = squares_outer[...].astype(jnp.bfloat16)

    def is_near(p):
        return jnp.logical_or(p < far_base, p >= far_base + n_tp // 2)

    def share(h):
        @pl.when(jnp.logical_or(inner, is_near(t)) if h < heads else True)
        def _():
            for d in range(1, n_tp):
                part = gall.at[t, :, pl.ds(h * VALUE_DIM, VALUE_DIM)]
                kind = h // heads
                remote(part, part, g_recv.at[kind], {"tp": lax.rem(t + d, n_tp)}).start()

    def slabs(count, span):
        return gall.at[pl.ds(0, count), :, pl.ds(0, span)]

    def gather():
        for where, count in (
            (inner, n_tp - 1),
            (jnp.logical_and(edge, is_near(t)), n_tp // 2 - 1),
            (helped, n_tp // 2),
        ):
            @pl.when(where)
            def _():
                expect(slabs(count, cols), g_recv.at[0])

        expect(slabs(n_tp - 1, VALUE_DIM), g_recv.at[1])

    def ask(h):
        part = asked.at[core, :, pl.ds(h * VALUE_DIM, VALUE_DIM)]
        return remote(part, part, q_recv.at[0], {"tp": opposite})

    def tell():
        return remote(tally, gall.at[t, :, pl.ds(cols, VALUE_DIM)], h_recv.at[2], {"sp": outer})

    def hand(c):
        return remote(asked.at[c], asked.at[c], h_recv.at[0], {"tp": sibling})

    def hand_on():
        @pl.when(jnp.logical_not(helps))
        def _():
            expect(asked.at[0], q_recv.at[0])

        hand(core).start()

    def heard():
        hand(1 - core).wait_recv()

    early = TILES - LATE

    def answer(f):
        return remote(far_out.at[f], far_in.at[f], f_recv.at[max(0, f - early + 1)], {"sp": outer})

    def wide_of(b, some):
        return jnp.concatenate([wbuf[b, f] for f in some], axis=1)

    def dot(lhs, b, some):
        return jnp.dot(lhs, wide_of(b, some), preferred_element_type=jnp.float32)

    def gained(b):
        return gall[b, :, :cols]

    def keep(some, total, fresh=False):
        for n, f in enumerate(some):
            part = total[:, n * tile : (n + 1) * tile]
            acc[f] = part if fresh else acc[f] + part

    def set_scale():
        square = gall[0, :, cols : cols + 1].astype(jnp.float32)
        for p in range(1, n_tp):
            square = square + gall[p, :, cols : cols + 1].astype(jnp.float32)
        squares[...] = jnp.broadcast_to(lax.rsqrt(square / (n_tp * cols) + norm_eps), squares.shape)

    def put(f, total):
        out[:, f * tile : (f + 1) * tile] = (total * squares[...]).astype(out.dtype)

    def run(call, some):
        for i in some:
            call(i)

    tiles = range(TILES)
    pairs = [(f, f + 1) for f in range(0, TILES, 2)]

    loads[0].wait()
    loads[1].wait()

    @pl.when(has_up)
    def _():
        part_along(z, 1).start()

    @pl.when(has_down)
    def _():
        part_along(z, 0).start()

    spread(z)
    loads[2].wait()

    @pl.when(helped)
    def _():
        lend().start()

    for c, count in enumerate(AT_EXIT):
        pl.when(core == c)(functools.partial(run, near, range(count)))
    queries()
    arrive(1)
    for c, count in enumerate(AT_EXIT):
        pl.when(core == c)(functools.partial(run, near, range(count, TILES)))
    run(near_out, range(2))
    for c, count in enumerate(AT_EXIT):
        pl.when(core == c)(functools.partial(inner_partner, range(max(count, 2))))
    lend_on()
    arrive(2)
    run(near_out, range(2, TILES))
    for c, count in enumerate(AT_EXIT):
        pl.when(core == c)(functools.partial(inner_partner, range(max(count, 2), 3)))
    arrive(3)
    near_far()
    outer_queries()
    inner_partner(range(3, 4))
    latents()
    inner_partner(range(4, 5))
    inner_pass(0)

    @pl.when(helps)
    def _():
        attend_outer(0)
        run(to_partner, range(5, 6))
        attend_outer(1)
        ask(0).start()
        inner_pass(1)
        run(to_partner, range(6, 7))
        attend_outer(2)
        ask(1).start()
        run(to_partner, range(7, TILES))
        attend_outer(3)
        ask(2).start()
        inner_pass(2)
        ask(3).start()
        tell().start()
        attend(0)
        hand_on()
        run(second_hop, range(1))
        attend(1)
        share(0)
        attend(2)
        share(1)
        inner_pass(3)
        run(second_hop, range(1, 2))
        attend(3)
        share(2)
        run(second_hop, range(2, 3))
        share(3)

    @pl.when(is_near(t))
    def _():
        attend(0)
        inner_partner(range(5, 6))
        inner_pass(1)
        edge_partner(range(5))
        attend(1)
        share(0)
        edge_partner(range(5, 6))
        attend(2)
        share(1)
        inner_partner(range(6, TILES))
        inner_pass(2)
        edge_partner(range(6, 7))
        attend(3)
        share(2)
        inner_pass(3)
        edge_partner(range(7, TILES))
        share(3)

        @pl.when(inner)
        def _():
            run(second_hop, range(3))
            hand_on()

    @pl.when(helped)
    def _():
        run(to_partner, tiles)
        tell().wait_recv()

    share(heads)

    def drain_all():
        halves = wbuf.at[0, :, pl.ds(0, half)]
        drain(lat.at[:, pl.ds(0, n_tp - 1)])
        drain(slabs(n_tp - 1, VALUE_DIM))
        for _ in range(2):
            drain(halves)

        @pl.when(jnp.logical_or(inner, is_near(t)))
        def _():
            drain(slabs(n_tp - 1, cols))

        @pl.when(edge)
        def _():
            drain(lat.at[0, pl.ds(0, 1)])
            drain(halves)

        @pl.when(helped)
        def _():
            drain(ql.at[pl.ds(0, lent_rows)])

        @pl.when(helps)
        def _():
            drain(asked.at[0])
            drain(tally)
            drain(ql.at[pl.ds(0, lent_rows)])

        @pl.when(inner)
        def _():
            for count in (2, 3):
                drain(lat.at[0, pl.ds(0, count)])
            for _ in range(3):
                drain(halves)
            drain(asked.at[0])
            drain(far_out)

    @pl.when(edge)
    def _():
        gather()
        set_scale()
        for some in pairs:
            keep(some, dot(gained(z), z, some), fresh=True)
        centre_far()
        for some in pairs:
            keep(some, dot(gained(centre), centre, some))
        def add(f):
            put(f, acc[f] + far_in[f].astype(jnp.float32))

        drain_all()
        expect(far_in.at[pl.ds(0, early)], f_recv.at[0])
        run(add, range(early))
        for c, order in enumerate(ORDERS):
            @pl.when(core == c)
            def _():
                for f in order:
                    if f >= early:
                        expect(far_in.at[0], f_recv.at[f - early + 1])
                        add(f)

    def part_of(p):
        return pl.ds(pl.multiple_of(p * half, half), half)

    def half_dot(f, p):
        return jnp.dot(
            asked[beyond - far_base, :, part_of(p)], wbuf[beyond, f, part_of(p)],
            preferred_element_type=jnp.float32,
        )

    def prepare(f):
        far_acc[f - early] = half_dot(f, parity) + dot(asked[centre - far_base], centre, (f,))

    def reply(f):
        landed(BEYOND_FAR, f)
        if f < early:
            far = dot(asked[beyond - far_base], beyond, (f,)) + dot(asked[centre - far_base], centre, (f,))
        else:
            far = far_acc[f - early] + half_dot(f, 1 - parity)
        far_out[f] = far.astype(far_out.dtype)
        answer(f).start()

    def own(some):
        keep(some, dot(gained(z), z, some) + dot(gained(centre), centre, some), fresh=True)

    @pl.when(inner)
    def _():
        run(second_hop, range(3, 4))
        heard()
        centre_far()
        reply(0)
        run(second_hop, range(4, 5))
        tails(0)
        reply(1)
        run(second_hop, range(5, 6))
        reply(2)
        tails(1)
        run(second_hop, range(6, 7))
        reply(3)
        run(second_hop, range(7, 8))
        run(prepare, range(early, TILES))
        for c, order in enumerate(ORDERS):
            pl.when(core == c)(functools.partial(run, reply, order))
        gather()
        set_scale()
        run(own, pairs)
        outer_rest()
        for some in pairs:
            total = dot(gained(outer), outer, some) + dot(gained(beyond), beyond, some)
            for n, f in enumerate(some):
                put(f, acc[f] + total[:, n * tile : (n + 1) * tile])

    pl.when(inner)(drain_all)


MESH = pl.DeviceIdType.MESH


def on_device_fused(
    n_sp, n_tp,
    query_latent, key_latent, rotary_key, query_gain, latent_gain,
    query_up, key_up, value_up, out_gain, out_weight,
):
    block_rows, row_count = query_latent.shape[0], key_latent.shape[0]
    rank, width = key_latent.shape[1], rotary_key.shape[1]
    keys = n_sp * n_tp * row_count
    depth, features = out_weight.shape
    cols = value_up.shape[1]
    vmem, bf16, dma = pltpu.VMEM, jnp.bfloat16, pltpu.SemaphoreType.DMA
    table = jnp.asarray(rope_table(keys, width))
    tiled = (TILES, block_rows, features // TILES)
    in_hbm = pl.BlockSpec(memory_space=pl.ANY)
    return pl.pallas_call(
        functools.partial(kernel, n_sp, n_tp),
        out_shape=vmem((block_rows, features), bf16),
        in_specs=[in_hbm] * 11,
        out_specs=pl.BlockSpec(memory_space=pltpu.VMEM),
        scratch_shapes=[
            vmem(query_latent.shape, bf16),
            vmem(query_latent.shape, bf16),
            vmem((query_gain.shape[0] // LANES, LANES), jnp.float32),
            vmem((1, rank), jnp.float32),
            vmem((1, cols), jnp.float32),
            vmem(table.shape, jnp.float32),
            vmem((n_sp, n_tp, row_count, rank + width), bf16),
            vmem((n_sp, TILES, depth, features // TILES), bf16),
            vmem(query_up.shape, bf16),
            vmem(key_up.shape, bf16),
            vmem(value_up.shape, bf16),
            vmem((keys, rank), bf16),
            vmem((keys, width), bf16),
            vmem((block_rows, query_up.shape[1]), bf16),
            vmem((block_rows, query_up.shape[1]), bf16),
            vmem(query_latent.shape, bf16),
            vmem((n_tp, block_rows, cols + VALUE_DIM), bf16),
            vmem((block_rows, VALUE_DIM), jnp.float32),
            vmem((block_rows, VALUE_DIM), jnp.float32),
            vmem((block_rows, VALUE_DIM), bf16),
            vmem(tiled, jnp.float32),
            vmem((LATE, *tiled[1:]), jnp.float32),
            vmem((n_tp // 2, block_rows, cols), bf16),
            vmem(tiled, bf16),
            vmem(tiled, bf16),
            dma((4,)),
            dma((2,)),
            dma((1,)),
            dma((n_sp + 1,)),
            dma((2,)),
            dma((TILES // 2 + 3 * TILES + 1,)),
            dma((4,)),
            dma((1,)),
            dma((4,)),
            dma((4,)),
        ],
        compiler_params=pltpu.CompilerParams(
            collective_id=0, has_side_effects=True
        ),
    )(
        query_latent, key_latent, rotary_key, query_gain.reshape(-1, LANES), latent_gain[None], out_gain[None],
        table, query_up, key_up, value_up, out_weight,
    )


def fits_fused(mesh):
    n_grp, n_sp, n_tp = (mesh.shape[name] for name in ("grp", "sp", "tp"))
    return n_grp % 2 == 0 and n_sp == LINE and n_sp == n_tp


def solution(mesh):
    in_specs = (
        P(("grp", "sp"), None),
        P(("grp", "sp", "tp"), None),
        P(("grp", "sp", "tp"), None),
        P(),
        P(),
        P(None, "tp"),
        P(None, "tp"),
        P(None, "tp"),
        P("tp"),
        P("sp", "tp"),
    )
    out_specs = P(("grp", "sp"), "tp")
    step = on_device
    if fits_fused(mesh):
        step = functools.partial(on_device_fused, mesh.shape["sp"], mesh.shape["tp"])
    return jax.shard_map(
        step, mesh=mesh, in_specs=in_specs, out_specs=out_specs, check_vma=False
    )
```
